32 devices in a mesh: sp: 8 (over z, x), tp: 4 (over y, core).
Axes of the slice: x: 2, y: 2, z: 4, core: 2. Of those that a mesh axis runs over, the one named last changes fastest.
Arguments:
- tokens: bfloat16 [4096, 2048], P(('sp', 'tp')), may hold values from -6 to 6
- input_norm_scale: bfloat16 [2048], replicated, may hold values from 0.099609375 to 1.8984375
- outer_gate_weight: bfloat16 [2048, 1024], P('sp', 'tp'), may hold values from -0.125 to 0.125
- inner_gate_weight: bfloat16 [2048, 1024], P('sp', 'tp'), may hold values from -0.125 to 0.125
- value_weight_matrix: bfloat16 [2048, 1024], P('sp', 'tp'), may hold values from -0.125 to 0.125
- output_gate_weight: bfloat16 [2048, 1024], P('sp', 'tp'), may hold values from -0.125 to 0.125
- state_input_weight: bfloat16 [2048, 1024], P('sp', 'tp'), may hold values from -0.125 to 0.125
- write_key_weight: bfloat16 [2048, 512], P('sp', 'tp'), may hold values from -0.125 to 0.125
- read_key_weight: bfloat16 [2048, 512], P('sp', 'tp'), may hold values from -0.125 to 0.125
- step_size_weight: bfloat16 [2048, 16], P(None, 'tp'), may hold values from -0.125 to 0.125
- gated_conv_weight: bfloat16 [3, 1024], P(None, 'tp'), may hold values from -3.5 to 3.5
- input_conv_weight: bfloat16 [4, 1024], P(None, 'tp'), may hold values from -3 to 3
- write_conv_weight: bfloat16 [4, 512], P(None, 'tp'), may hold values from -3 to 3
- read_conv_weight: bfloat16 [4, 512], P(None, 'tp'), may hold values from -3 to 3
- step_size_bias: float32 [16], P('tp'), may hold values from -1 to 0.5
- log_decay_rate: float32 [16], P('tp'), may hold values from -16 to -2.5, as said below
- decay_spikes: float32 [16, 4096], P('tp', 'sp'), may hold values from -1 to 0, as said below
- direct_path_weight: float32 [16], P('tp'), may hold values from 0.5 to 2
- head_norm_scale: bfloat16 [1024], P('tp'), may hold values from 0.099609375 to 1.8984375
- conv_output_weight: bfloat16 [1024, 2048], P('tp', 'sp'), may hold values from -0.125 to 0.125
- state_output_weight: bfloat16 [1024, 2048], P('tp', 'sp'), may hold values from -0.125 to 0.125
Outputs:
- mixed: bfloat16 [4096, 2048], P(('sp', 'tp'))
The draws below stay inside these ranges and needn't reach their ends.
Inputs may be any that keep to these rules, and one draw needn't show every extreme that they name: `log_decay_rate`: one value a head. `decay_spikes`: never positive.
All inputs are finite; a program needn't handle non-finite values.
Results may differ from the reference program's by a relative error of at most 0.017.
Values may be sent and summed in bfloat16 or wider, within the bound.
A program may use at most 128 MiB of HBM per device.

```python
import math
import jax
import jax.numpy as jnp
from jax import lax

D = 2048
CONV = 1024
MIXER_HEADS = 16
HEAD_DIM = 64
GROUPS = 4
STATE = 128
SHORT_K = 3
SSD_K = 4
BLOCK = 64
TOK_DEV = 512
INNER = 1024
SEQUENCE_TOKENS = 4096
N_TP = 4


def draw_tokens(key, part):
    positions = jnp.arange(SEQUENCE_TOKENS, dtype=jnp.int32)
    segment_ids = positions * 8 // SEQUENCE_TOKENS
    jitter_values = jax.random.truncated_normal(jax.random.fold_in(key, 31), -4.5, 4.5, (SEQUENCE_TOKENS, D), jnp.float32)
    directions = jax.random.uniform(jax.random.fold_in(key, 32), (8, D), jnp.float32, -1.2, 1.2)
    offsets = jnp.take(directions, segment_ids, axis=0)
    return (jitter_values + offsets).astype(jnp.bfloat16)


def draw_log_decay_rate(key, part):
    ranking = jax.random.permutation(jax.random.fold_in(key, 11), MIXER_HEADS)
    quick_heads = ranking < MIXER_HEADS // 2
    fast_rates = jnp.exp(jax.random.uniform(jax.random.fold_in(key, 12), (MIXER_HEADS,), jnp.float32, math.log(0.02), math.log(0.08)))
    slow_rates = jnp.exp(jax.random.uniform(jax.random.fold_in(key, 13), (MIXER_HEADS,), jnp.float32, math.log(0.1), math.log(0.3))) / SEQUENCE_TOKENS
    return jnp.log(jnp.where(quick_heads, fast_rates, slow_rates)).astype(jnp.float32)


def draw_decay_spikes(key, part):
    blocks = SEQUENCE_TOKENS // TOK_DEV
    levels = jnp.exp(jax.random.uniform(jax.random.fold_in(key, 21), (MIXER_HEADS, blocks), jnp.float32, math.log(0.25), math.log(2.0)))
    stable_decay = -0.3 / SEQUENCE_TOKENS * jnp.repeat(levels, TOK_DEV, axis=1)
    spike_positions = jax.random.randint(jax.random.fold_in(key, 22), (3,), 0, SEQUENCE_TOKENS)
    spike_present = jnp.any(jnp.arange(SEQUENCE_TOKENS)[None, :] == spike_positions[:, None], axis=0)
    spike_decrement = jax.random.uniform(jax.random.fold_in(key, 23), (MIXER_HEADS, SEQUENCE_TOKENS), jnp.float32, 0.22, 0.69)
    return (stable_decay - jnp.where(spike_present[None, :], spike_decrement, 0.0)).astype(jnp.float32)


def steps_of(own_key, dims, pieces, least, largest):
    level, own = 1.0, jax.random.fold_in(own_key, 6)
    for dim, parts in pieces:
        draws = jnp.exp(jax.random.uniform(jax.random.fold_in(own, dim), (parts,), jnp.float32, least / len(pieces), largest / len(pieces)))
        level = level * jnp.repeat(draws, dims[dim] // parts).reshape([-1 if axis == dim else 1 for axis in range(len(dims))])
    return level


def gaussian(rng, shape, deviation, limit, pieces=(), kind=jnp.bfloat16):
    drawn = jax.random.normal(rng, shape, jnp.float32) * deviation
    if len(pieces) > 0:
        drawn = steps_of(rng, shape, pieces, -0.22, 0.18) * drawn
    return jnp.clip(drawn, min=-limit, max=limit).astype(kind)


def setup_inputs(seed: int = 0) -> dict:
    streams_of = jax.random.split(jax.random.key(seed), 22)
    return {
        "tokens": draw_tokens(jax.random.fold_in(streams_of[21], 71), 0),
        "input_norm_scale": jnp.clip(1.0 + 0.18 * jax.random.normal(streams_of[1], (D,), jnp.float32), 0.099609375, 1.8984375).astype(jnp.bfloat16),
        "outer_gate_weight": gaussian(streams_of[2], (D, CONV), D ** -0.5, 0.125, ((0, 8), (1, 4))),
        "inner_gate_weight": gaussian(streams_of[3], (D, CONV), D ** -0.5, 0.125, ((0, 8), (1, 4))),
        "value_weight_matrix": gaussian(streams_of[4], (D, CONV), D ** -0.5, 0.125, ((0, 8), (1, 4))),
        "output_gate_weight": gaussian(streams_of[5], (D, INNER), D ** -0.5, 0.125, ((0, 8), (1, 4))),
        "state_input_weight": gaussian(streams_of[6], (D, INNER), D ** -0.5, 0.125, ((0, 8), (1, 4))),
        "write_key_weight": gaussian(streams_of[7], (D, GROUPS * STATE), D ** -0.5, 0.125, ((0, 8), (1, 4))),
        "read_key_weight": gaussian(streams_of[8], (D, GROUPS * STATE), D ** -0.5, 0.125, ((0, 8), (1, 4))),
        "step_size_weight": gaussian(streams_of[9], (D, MIXER_HEADS), D ** -0.5, 0.125, ((1, 4),)),
        "gated_conv_weight": gaussian(streams_of[10], (SHORT_K, CONV), SHORT_K ** -0.5, 3.5, ((1, 4),)),
        "input_conv_weight": gaussian(streams_of[11], (SSD_K, INNER), SSD_K ** -0.5, 3.0, ((1, 4),)),
        "write_conv_weight": gaussian(streams_of[12], (SSD_K, GROUPS * STATE), SSD_K ** -0.5, 3.0, ((1, 4),)),
        "read_conv_weight": gaussian(streams_of[13], (SSD_K, GROUPS * STATE), SSD_K ** -0.5, 3.0, ((1, 4),)),
        "step_size_bias": jnp.clip(-1.0 + 1.5 * jax.random.uniform(streams_of[14], (MIXER_HEADS,), jnp.float32) ** steps_of(streams_of[14], (MIXER_HEADS,), ((0, 4),), -0.2, 0.2), -1.0, 0.5),
        "log_decay_rate": draw_log_decay_rate(jax.random.fold_in(streams_of[21], 71), 0),
        "decay_spikes": draw_decay_spikes(jax.random.fold_in(streams_of[21], 71), 0),
        "direct_path_weight": jnp.clip(0.5 + 1.5 * jax.random.uniform(streams_of[17], (MIXER_HEADS,), jnp.float32) ** steps_of(streams_of[17], (MIXER_HEADS,), ((0, 4),), -0.2, 0.2), 0.5, 2.0),
        "head_norm_scale": jnp.clip(1.0 + 0.18 * jax.random.normal(streams_of[18], (INNER,), jnp.float32), 0.099609375, 1.8984375).astype(jnp.bfloat16),
        "conv_output_weight": gaussian(streams_of[19], (CONV, D), (CONV + INNER) ** -0.5, 0.125, ((0, 4), (1, 8))),
        "state_output_weight": gaussian(streams_of[20], (INNER, D), (CONV + INNER) ** -0.5, 0.125, ((0, 4), (1, 8))),
    }


epsilon = 1e-05
highest = lax.Precision.HIGHEST

def causal_taps(values, tap_weights):
    tap_count = tap_weights.shape[0]
    length = values.shape[0]
    padded = jnp.concatenate([jnp.zeros((tap_count - 1, values.shape[1]), jnp.float32), values], axis=0)
    running = tap_weights[0] * padded[0:length]
    for offset in range(1, tap_count):
        running = running + tap_weights[offset] * padded[offset:offset + length]
    return running

def reference(tokens, input_norm_scale, outer_gate_weight, inner_gate_weight, value_weight_matrix, output_gate_weight, state_input_weight, write_key_weight, read_key_weight, step_size_weight, gated_conv_weight, input_conv_weight, write_conv_weight, read_conv_weight, step_size_bias, log_decay_rate, decay_spikes, direct_path_weight, head_norm_scale, conv_output_weight, state_output_weight):
    token_rows = tokens.astype(jnp.float32)
    scaled = token_rows * lax.rsqrt(lax.optimization_barrier(jnp.mean(token_rows * token_rows, axis=1, keepdims=True)) + epsilon)
    normed = (scaled * input_norm_scale.astype(jnp.float32)).astype(jnp.bfloat16)

    def project(weight):
        return jnp.dot(normed, weight, preferred_element_type=jnp.float32).astype(jnp.bfloat16)
    outer_gate = project(outer_gate_weight)
    inner_gate = project(inner_gate_weight)
    conv_input = project(value_weight_matrix)
    out_gate = project(output_gate_weight)
    state_input = project(state_input_weight)
    write_keys = project(write_key_weight)
    read_keys = project(read_key_weight)
    step_raw = jnp.dot(normed, step_size_weight, preferred_element_type=jnp.float32)
    product = inner_gate.astype(jnp.float32) * conv_input.astype(jnp.float32)
    mixer_part = (outer_gate.astype(jnp.float32) * causal_taps(product, gated_conv_weight.astype(jnp.float32))).astype(jnp.bfloat16)
    seq_input = jax.nn.silu(causal_taps(state_input.astype(jnp.float32), input_conv_weight.astype(jnp.float32)))
    seq_write = jax.nn.silu(causal_taps(write_keys.astype(jnp.float32), write_conv_weight.astype(jnp.float32)))
    seq_read = jax.nn.silu(causal_taps(read_keys.astype(jnp.float32), read_conv_weight.astype(jnp.float32)))
    discrete_step = jax.nn.softplus(step_raw + step_size_bias[None, :])
    step_logarithm = discrete_step * (-jnp.exp(log_decay_rate))[None, :] + decay_spikes.T
    blocks = SEQUENCE_TOKENS // BLOCK
    per_group = MIXER_HEADS // GROUPS
    input_blocks = seq_input.reshape(blocks, BLOCK, MIXER_HEADS, HEAD_DIM)
    weighted = input_blocks * discrete_step.reshape(blocks, BLOCK, MIXER_HEADS, 1)
    write_blocks = seq_write.reshape(blocks, BLOCK, GROUPS, STATE)
    read_blocks = seq_read.reshape(blocks, BLOCK, GROUPS, STATE)
    cumulative = jnp.cumsum(step_logarithm.reshape(blocks, BLOCK, MIXER_HEADS), axis=1)
    causal = lax.broadcasted_iota(jnp.int32, (BLOCK, BLOCK), 0) >= lax.broadcasted_iota(jnp.int32, (BLOCK, BLOCK), 1)

    def one_block(carried_state, inputs):
        block_weighted, block_write, block_read, block_cum = inputs
        write_heads = jnp.repeat(block_write, per_group, axis=1)
        read_heads = jnp.repeat(block_read, per_group, axis=1)
        scores = jnp.einsum('lhm,shm->lsh', read_heads, write_heads, precision=highest)
        damping = jnp.exp(jnp.where(causal[:, :, None], block_cum[:, None, :] - block_cum[None, :, :], -jnp.inf))
        within = jnp.einsum('lsh,shp->lhp', scores * damping, block_weighted, precision=highest)
        from_before = jnp.einsum('lhm,hpm->lhp', read_heads, carried_state, precision=highest) * jnp.exp(block_cum)[:, :, None]
        to_end = jnp.exp(block_cum[-1:, :] - block_cum)
        new_state = jnp.einsum('shm,shp->hpm', write_heads * to_end[:, :, None], block_weighted, precision=highest)
        return (carried_state * jnp.exp(block_cum[-1])[:, None, None] + new_state, within + from_before)
    _, block_outputs = lax.scan(one_block, jnp.zeros((MIXER_HEADS, HEAD_DIM, STATE), jnp.float32), (weighted, write_blocks, read_blocks, cumulative))
    head_out = block_outputs + direct_path_weight[None, None, :, None] * input_blocks
    head_out = head_out.reshape(SEQUENCE_TOKENS, MIXER_HEADS * HEAD_DIM)
    gated_heads = (head_out * jax.nn.silu(out_gate.astype(jnp.float32))).reshape(SEQUENCE_TOKENS, MIXER_HEADS, HEAD_DIM)
    normalized = gated_heads * lax.rsqrt(lax.optimization_barrier(jnp.mean(gated_heads * gated_heads, axis=2, keepdims=True)) + epsilon)
    state_part = (normalized.reshape(SEQUENCE_TOKENS, MIXER_HEADS * HEAD_DIM) * head_norm_scale.astype(jnp.float32)).astype(jnp.bfloat16)
    share_conv = CONV // N_TP
    share_state = MIXER_HEADS * HEAD_DIM // N_TP
    running = jnp.zeros((SEQUENCE_TOKENS, D), jnp.float32)
    for head_block in range(N_TP):
        conv_slice = slice(head_block * share_conv, (head_block + 1) * share_conv)
        state_slice = slice(head_block * share_state, (head_block + 1) * share_state)
        partial_sum = jnp.dot(mixer_part[:, conv_slice], conv_output_weight[conv_slice], preferred_element_type=jnp.float32)
        partial_sum = partial_sum + jnp.dot(state_part[:, state_slice], state_output_weight[state_slice], preferred_element_type=jnp.float32)
        rounded = lax.optimization_barrier(partial_sum.astype(jnp.bfloat16))
        running = running + rounded.astype(jnp.float32)
    return running.astype(jnp.bfloat16)
```

```python
import functools

import jax
import jax.numpy as jnp
from jax import lax
from jax.experimental import pallas as pl
from jax.experimental.pallas import tpu as pltpu
from jax.sharding import PartitionSpec as P

HEAD_DIM = 64
STATE = 128
PLAIN_BLOCK = 64
CHUNK = 128
HALO = 16
PIECES_S = 4
PIECES_R = 8
PIECES_O = 4
PIECES_T = 2
CORES = 2
epsilon = 1e-05
highest = lax.Precision.HIGHEST
f32 = jnp.float32
bf16 = jnp.bfloat16
MESH = pl.DeviceIdType.MESH


def nt(a, b, precision=None):
    return lax.dot_general(
        a, b, (((1,), (1,)), ((), ())), preferred_element_type=f32, precision=precision
    )


def silu(v):
    return v / (1.0 + jnp.exp(-v))


class Ring:
    def __init__(self, n, pieces, buf, send, recv, neighbour):
        self.n, self.pieces, self.buf = n, pieces, buf
        self.send_sem, self.recv_sem, self.neighbour = send, recv, neighbour
        self.rows = buf.shape[1] // pieces
        self.waited = set()

    def copy(self, s, q, way):
        n = self.n
        src, dst = (s, s + 1) if way == 0 else ((n - s) % n, n - 1 - s)
        cut = pl.ds(q * self.rows, self.rows)
        return pltpu.make_async_remote_copy(
            src_ref=self.buf.at[src, cut],
            dst_ref=self.buf.at[dst, cut],
            send_sem=self.send_sem.at[s, q, way],
            recv_sem=self.recv_sem.at[s, q, way],
            device_id={"sp": self.neighbour[way]},
            device_id_type=MESH,
        )

    def ways(self, s, q):
        if s < self.n // 2 - 1:
            return (0, 1)
        return (0,) if q < self.pieces // 2 else (1,)

    def arrive(self, s, q, way):
        if (s, q, way) not in self.waited:
            self.waited.add((s, q, way))
            self.copy(s, q, way).wait_recv()

    def forward(self, s, q):
        for way in self.ways(s, q):
            if s > 0:
                self.arrive(s - 1, q, way)
            self.copy(s, q, way).start()

    def need(self, slot):
        last = self.n // 2
        for q in range(self.pieces):
            if 0 < slot < last:
                self.arrive(slot - 1, q, 0)
            elif slot > last:
                self.arrive(self.n - slot - 1, q, 1)
            elif slot == last:
                self.arrive(last - 1, q, self.ways(last - 1, q)[0])

    def order(self, first):
        return [(s, q) for s in range(first, self.n // 2) for q in range(self.pieces)]

    def drain(self):
        for s, q in self.order(0):
            for way in self.ways(s, q):
                self.copy(s, q, way).wait_send()


def kernel(
    n,
    T,
    tokens_h, in_scale_h, w_outer, w_inner, w_value, w_ogate, w_state, w_write, w_read,
    step_w_h, taps_conv_h, taps_in_h, taps_wr_h, taps_rd_h,
    bias, rate, spikes_h, direct, hscale_h, o_conv, o_state,
    near, far,
    tokens, in_scale, step_w, taps_conv, taps_in, taps_wr, taps_rd, spikes, hscale,
    sbuf, rbuf, obuf, norm, acc_s, acc_r, mixbuf, xbuf, wrbuf, rdbuf, ybuf, cumbuf, stbuf,
    st_send, st_recv, e_send, e_recv, pair_buf, apart, part, r1, p2, nbuf,
    loc_sem, ss_sem, sr_sem, rs_sem, rr_sem, os_sem, or_sem,
    ts_sem, tr_sem, us_sem, ur_sem, h_sem, g_sem, x_sem, e_sem,
    r1s_sem, r1r_sem, r2s_sem, r2r_sem, near_sem,
):
    sp = lax.axis_index("sp")
    tp = lax.axis_index("tp")
    rows, width = tokens.shape
    kdim = w_outer.shape[0]
    cdim = w_outer.shape[1]
    length = rows * T
    heads_width = xbuf.shape[1]
    heads = heads_width // HEAD_DIM
    ocols = obuf.shape[2]
    n_half = n // 2
    Y = T // CORES

    barrier = pltpu.get_barrier_semaphore()
    for d in range(1, n):
        pl.semaphore_signal(
            barrier, inc=1, device_id={"sp": lax.rem(sp + d, n)}, device_id_type=MESH
        )
    for d in range(1, T):
        pl.semaphore_signal(
            barrier, inc=1, device_id={"tp": lax.rem(tp + d, T)}, device_id_type=MESH
        )

    def pack(refs, dst, rows_too=False):
        pairs, at = [], 0
        for ref in refs:
            if rows_too:
                pairs.append((ref, dst.at[0, pl.ds(at, ref.shape[0])]))
                at += ref.shape[0]
            else:
                pairs.append((ref, dst.at[0, :, pl.ds(at, ref.shape[1])]))
                at += ref.shape[1]
        return pairs

    groups = {
        "s": pack((w_state, w_write, w_read), sbuf),
        "t": [(tokens_h, tokens), (in_scale_h, in_scale)],
        "r": pack((w_ogate, w_outer, w_inner, w_value), rbuf),
        "v": [
            (step_w_h, step_w), (taps_conv_h, taps_conv), (taps_in_h, taps_in),
            (taps_wr_h, taps_wr), (taps_rd_h, taps_rd), (spikes_h, spikes), (hscale_h, hscale),
        ],
        "o": pack((o_conv, o_state), obuf, True),
    }
    local, index = {}, 0
    for name, pairs in groups.items():
        local[name] = []
        for src, dst in pairs:
            local[name].append(pltpu.make_async_copy(src, dst, loc_sem.at[index]))
            local[name][-1].start()
            index += 1

    def landed(name):
        for copy in local[name]:
            copy.wait()

    def pos_of(index):
        odd = lax.rem(index, 2)
        low = lax.div(index, 2)
        return (1 - odd) * low + odd * (n - 1 - low)

    def index_of(pos):
        high = lax.div(pos, n_half)
        return (1 - high) * 2 * pos + high * (2 * (n - 1 - pos) + 1)

    pos = pos_of(sp)
    neighbour = (index_of(lax.rem(pos + 1, n)), index_of(lax.rem(pos + n - 1, n)))

    def owner_of(slot):
        return index_of(lax.rem(pos + n - slot, n))

    ring_s = Ring(n, PIECES_S, sbuf, ss_sem, sr_sem, neighbour)
    ring_r = Ring(n, PIECES_R, rbuf, rs_sem, rr_sem, neighbour)
    ring_o = Ring(n, PIECES_O, obuf, os_sem, or_sem, neighbour)

    own_at = pl.multiple_of(HALO + tp * rows, HALO)
    core = lax.rem(tp, CORES)
    chip = lax.div(tp, CORES)
    partner = chip * CORES + 1 - core
    prow = rows // PIECES_T

    def at_rows(block, q):
        return norm.at[pl.ds(pl.multiple_of(HALO + block * rows + q * prow, HALO), prow)]

    def t_copy(d, q):
        device = partner if d == 0 else lax.rem(chip + d, Y) * CORES + core
        return pltpu.make_async_remote_copy(
            src_ref=at_rows(tp, q),
            dst_ref=at_rows(tp, q),
            send_sem=ts_sem.at[d, q],
            recv_sem=tr_sem.at[d, q],
            device_id={"tp": device},
            device_id_type=MESH,
        )

    def u_copy(d, q):
        block = lax.rem(chip + Y - d, Y) * CORES + core
        return pltpu.make_async_remote_copy(
            src_ref=at_rows(block, q),
            dst_ref=at_rows(block, q),
            send_sem=us_sem.at[d, q],
            recv_sem=ur_sem.at[d, q],
            device_id={"tp": partner},
            device_id_type=MESH,
        )

    def h_copy():
        return pltpu.make_async_remote_copy(
            src_ref=norm.at[pl.ds(length, HALO)],
            dst_ref=norm.at[pl.ds(0, HALO)],
            send_sem=h_sem.at[0],
            recv_sem=h_sem.at[1],
            device_id={"sp": lax.rem(sp + 1, n)},
            device_id_type=MESH,
        )

    def g_copy(d):
        return pltpu.make_async_remote_copy(
            src_ref=norm.at[pl.ds(0, HALO)],
            dst_ref=norm.at[pl.ds(0, HALO)],
            send_sem=g_sem.at[0, d],
            recv_sem=g_sem.at[1, d],
            device_id={"tp": d},
            device_id_type=MESH,
        )

    last_tp = tp == T - 1

    landed("s")
    pl.semaphore_wait(barrier, n - 1 + T - 1)
    for q in range(PIECES_S):
        ring_s.forward(0, q)
    landed("t")
    x = tokens[...].astype(f32)
    x = x * lax.rsqrt(jnp.mean(x * x, axis=1, keepdims=True) + epsilon)
    norm[pl.ds(own_at, rows), :] = (x * in_scale[...].astype(f32).reshape(1, width)).astype(bf16)
    for q in range(PIECES_T):
        for d in range(1, Y):
            t_copy(d, q).start()
        t_copy(0, q).start()

    @pl.when(last_tp & (sp < n - 1))
    def _():
        h_copy().start()

    landed("r")
    r_own = [(0, q) for q in range(PIECES_R)]
    ring_r.forward(*r_own.pop(0))

    def t_forward(q):
        for d in range(1, Y):
            t_copy(d, q).wait_recv()
            u_copy(d, q).start()

    s_list = ring_s.order(1)
    hops = [s_list[i : i + PIECES_S] for i in range(0, len(s_list), PIECES_S)]
    for i, hop in enumerate(hops):
        for j, item in enumerate(hop):
            ring_s.forward(*item)
            if i == 1 and j == 0:
                t_forward(0)
            if i == 1 and j == 2:
                for q in range(1, PIECES_T):
                    t_forward(q)
        if i == 0:

            @pl.when(last_tp & (sp > 0))
            def _():
                h_copy().wait_recv()
                for d in range(T - 1):
                    g_copy(d).start()

        if i < len(hops) - 1:
            ring_r.forward(*r_own.pop(0))
    while r_own:
        ring_r.forward(*r_own.pop(0))

    r_list = ring_r.order(1)
    o_list = []

    def pump(count):
        for _ in range(count):
            if r_list:
                ring_r.forward(*r_list.pop(0))
            elif o_list:
                ring_o.forward(*o_list.pop(0))

    for q in range(PIECES_T):
        t_copy(0, q).wait_recv()
        for d in range(1, Y):
            pltpu.make_async_remote_copy(
                src_ref=at_rows(lax.rem(chip + Y - d, Y) * CORES + 1 - core, q),
                dst_ref=at_rows(lax.rem(chip + Y - d, Y) * CORES + 1 - core, q),
                send_sem=us_sem.at[d, q],
                recv_sem=ur_sem.at[d, q],
                device_id={"tp": partner},
                device_id_type=MESH,
            ).wait_recv()
    for d in range(T - 1):

        @pl.when((tp == d) & (sp > 0))
        def _():
            g_copy(d).wait_recv()

    @pl.when(sp == 0)
    def _():
        norm[0:HALO, :] = jnp.zeros((HALO, width), bf16)

    def project(ring, acc, slots, fresh=False):
        total_cols = acc.shape[1]
        for slot in slots:
            ring.need(slot)
        for c in range(0, total_cols, 256):
            total = None
            for slot in slots:
                at = pl.multiple_of(owner_of(slot) * kdim, kdim)
                term = jnp.dot(
                    norm[:, pl.ds(at, kdim)], ring.buf[slot, :, c : c + 256],
                    preferred_element_type=f32,
                )
                total = term if total is None else total + term
            if fresh:
                acc[:, c : c + 256] = total
            else:
                acc[:, c : c + 256] += total

    def pairs_of():
        return [(k, n - k) for k in range(1, n_half)]

    project(ring_s, acc_s, (0,), True)
    for pair in pairs_of():
        project(ring_s, acc_s, pair)
    early = min(2, PIECES_R)
    pump(early)
    project(ring_s, acc_s, (n_half,))

    def column(ref):
        index = lax.broadcasted_iota(jnp.int32, (heads, 1), 0)
        full = jnp.full((heads, 1), ref[0], f32)
        for h in range(1, heads):
            full = jnp.where(index == h, ref[h], full)
        return full

    landed("v")
    step = jax.nn.softplus(nt(step_w[...], norm[HALO:, :]) + column(bias))
    logs = -step * jnp.exp(column(rate)) + spikes[...]
    r_id = lax.broadcasted_iota(jnp.int32, (CHUNK, CHUNK), 0)
    c_id = lax.broadcasted_iota(jnp.int32, (CHUNK, CHUNK), 1)
    causal = r_id >= c_id
    lower = causal.astype(f32)
    eye = (r_id == c_id).astype(f32)
    lane = lax.broadcasted_iota(jnp.int32, (1, heads_width), 1)

    def spread(columns):
        full = jnp.broadcast_to(columns[:, 0:1], (columns.shape[0], heads_width))
        for h in range(1, heads):
            full = jnp.where(lane >= h * HEAD_DIM, columns[:, h : h + 1], full)
        return full

    def taps(u, weights):
        k_taps = weights.shape[0]
        w = weights[...].astype(f32)
        total = w[k_taps - 1 : k_taps] * u[8:]
        for k in range(k_taps - 1):
            total = total + w[k : k + 1] * pltpu.roll(u, k_taps - 1 - k, 0)[8:]
        return total

    blocks = length // CHUNK
    running = jnp.zeros((STATE, heads_width), f32)
    before = jnp.zeros((1, heads_width), f32)
    at_ogate, at_outer, at_inner, at_value = (i * cdim for i in range(4))
    at_state, at_write, at_read = 0, cdim, cdim + STATE

    def spans(b):
        t0 = b * CHUNK
        return (
            slice(t0, t0 + CHUNK),
            slice(t0 + HALO, t0 + HALO + CHUNK),
            slice(t0 + HALO - 8, t0 + HALO + CHUNK),
        )

    def field(acc, begin, size, span):
        return acc[span, begin : begin + size].astype(bf16).astype(f32)

    for b in range(blocks):
        span, own, take = spans(b)
        xs = silu(taps(field(acc_s, at_state, cdim, take), taps_in))
        wr = silu(taps(field(acc_s, at_write, STATE, take), taps_wr))
        rd = silu(taps(field(acc_s, at_read, STATE, take), taps_rd))
        cum = nt(lower, logs[:, span], highest)
        steps = nt(eye, step[:, span], highest)
        cum_wide = spread(cum)
        weighted = xs * spread(steps)
        xbuf[span, :] = xs
        mixbuf[span, :] = weighted.astype(bf16)
        wrbuf[span, :] = wr.astype(bf16)
        rdbuf[span, :] = rd.astype(bf16)
        cumbuf[span, :] = cum_wide
        last = cum_wide[CHUNK - 1 : CHUNK]
        scaled = (weighted * jnp.exp(last - cum_wide)).astype(bf16)
        stbuf[b] = running
        running = running * jnp.exp(last) + jnp.dot(
            wr.T.astype(bf16), scaled, preferred_element_type=f32
        )
        before = before + last
        pump(1)
    st_send[0:STATE, :] = running.astype(bf16)
    st_send[STATE:, :] = jnp.broadcast_to(jnp.exp(before), (HALO, heads_width)).astype(bf16)

    z = lax.div(sp, 2)
    second = lax.rem(sp, 2)
    depth = n_half

    def x_copy():
        return pltpu.make_async_remote_copy(
            src_ref=st_send,
            dst_ref=st_recv,
            send_sem=x_sem.at[0],
            recv_sem=x_sem.at[1],
            device_id={"sp": sp + 1 - 2 * second},
            device_id_type=MESH,
        )

    def e_copy():
        return pltpu.make_async_remote_copy(
            src_ref=e_send,
            dst_ref=e_recv,
            send_sem=e_sem.at[0],
            recv_sem=e_sem.at[1],
            device_id={"sp": lax.rem(sp + 2, n)},
            device_id_type=MESH,
        )

    x_copy().start()

    def within(b):
        span, _, _ = spans(b)
        scores = nt(rdbuf[span, :], wrbuf[span, :])
        cum_t = lax.dot_general(
            logs[:, span], lower, (((1,), (1,)), ((), ())),
            preferred_element_type=f32, precision=highest,
        )
        for pair in range(0, heads_width, 128):
            both = []
            for h in range(pair // HEAD_DIM, (pair + 128) // HEAD_DIM):
                diff = cumbuf[span, h * HEAD_DIM : h * HEAD_DIM + 1] - cum_t[h : h + 1, :]
                damped = scores * jnp.exp(jnp.where(causal, diff, -1e30))
                both.append(
                    jnp.dot(
                        damped.astype(bf16), mixbuf[span, pair : pair + 128],
                        preferred_element_type=f32,
                    )
                )
            first = lax.broadcasted_iota(jnp.int32, (1, 128), 1) < HEAD_DIM
            ybuf[span, pair : pair + 128] = jnp.where(first, both[0], both[1])

    for b in range(blocks):
        within(b)
        if b % 2 == 1:
            pump(1)
    x_copy().wait_recv()
    other = st_recv[0:STATE, :].astype(f32)
    other_decay = st_recv[STATE : STATE + 1, :].astype(f32)
    own_decay = jnp.exp(before)
    is_second = jnp.broadcast_to(second, (1, heads_width)) == 1
    pair_buf[0] = jnp.where(
        is_second, other * own_decay + running, running * other_decay + other
    )
    pair_buf[1] = jnp.where(is_second, other, jnp.zeros_like(other))
    pair_decay = own_decay * other_decay
    first_decay = jnp.where(is_second, other_decay, jnp.ones_like(other_decay))

    def link(j):
        @pl.when(z == j)
        def _():
            if j == 0:
                pair_buf[2] = jnp.zeros_like(pair_buf[2])
            else:
                e_copy().wait_recv()
                pair_buf[2] = e_recv[...].astype(f32)
            if j < depth - 1:
                e_send[...] = (pair_buf[2] * pair_decay + pair_buf[0]).astype(bf16)
                e_copy().start()

    link(0)
    project(ring_r, acc_r, (0,), True)
    landed("o")
    for k, pair in enumerate(pairs_of()):
        if k < n_half - 2:
            pump(PIECES_R // 2)
            project(ring_r, acc_r, pair)
            link(k + 1)
            pump(PIECES_R // 2)
        else:
            pump(len(r_list))
            for q in range(PIECES_O):
                ring_o.forward(0, q)
            o_list += ring_o.order(1)
            project(ring_r, acc_r, pair)
            for j in range(k + 1, depth):
                link(j)

    group = (
        lax.div(lax.broadcasted_iota(jnp.int32, (heads_width, heads_width), 0), HEAD_DIM)
        == lax.div(lax.broadcasted_iota(jnp.int32, (heads_width, heads_width), 1), HEAD_DIM)
    ).astype(bf16)
    direct_wide = jnp.full((1, heads_width), direct[0], f32)
    for h in range(1, heads):
        direct_wide = jnp.where(lane >= h * HEAD_DIM, direct[h], direct_wide)

    arriving = pair_buf[1] + first_decay * pair_buf[2]
    so_far = jnp.zeros((1, heads_width), f32)
    for b in range(blocks):
        span, _, _ = spans(b)
        cum_wide = cumbuf[span, :]
        entering = (stbuf[b] + jnp.exp(so_far) * arriving).astype(bf16)
        so_far = so_far + cum_wide[CHUNK - 1 : CHUNK]
        ybuf[span, :] = (
            ybuf[span, :]
            + jnp.dot(rdbuf[span, :], entering, preferred_element_type=f32) * jnp.exp(cum_wide)
            + direct_wide * xbuf[span, :]
        )

    project(ring_r, acc_r, (n_half,))

    for b in range(blocks):
        span, own, take = spans(b)
        product = field(acc_r, at_inner, cdim, take) * field(acc_r, at_value, cdim, take)
        mix = field(acc_r, at_outer, cdim, own) * taps(product, taps_conv)
        apart[span, 0:cdim] = mix.astype(bf16)
        gated = ybuf[span, :] * silu(field(acc_r, at_ogate, cdim, own))
        square = jnp.dot((gated * gated).astype(bf16), group, preferred_element_type=f32)
        normalized = gated * lax.rsqrt(square * (1.0 / HEAD_DIM) + epsilon)
        apart[span, cdim:] = (
            normalized * hscale[...].astype(f32).reshape(1, heads_width)
        ).astype(bf16)

    def block_rows(y, c):
        return pl.ds(pl.multiple_of((y * CORES + c) * rows, rows), rows)

    def columns_of(slot):
        return pl.ds(pl.multiple_of(owner_of(slot) * ocols, ocols), ocols)

    def r1_copy(d, s):
        return pltpu.make_async_remote_copy(
            src_ref=part.at[s, block_rows(lax.rem(chip + d, Y), 1 - core)],
            dst_ref=r1.at[d, s],
            send_sem=r1s_sem.at[d, s],
            recv_sem=r1r_sem.at[d, s],
            device_id={"tp": partner},
            device_id_type=MESH,
        )

    def r2_copy(d, s):
        return pltpu.make_async_remote_copy(
            src_ref=p2.at[d - 1, s],
            dst_ref=far.at[d - 1, :, columns_of(s)],
            send_sem=r2s_sem.at[d, s],
            recv_sem=r2r_sem.at[d, s],
            device_id={"tp": lax.rem(chip + d, Y) * CORES + core},
            device_id_type=MESH,
        )

    def near_copy(s):
        return pltpu.make_async_copy(nbuf.at[s], near.at[:, columns_of(s)], near_sem.at[s])

    def project_out(s):
        ring_o.need(s)
        part[s] = jnp.dot(apart[...], obuf[s], preferred_element_type=f32).astype(bf16)
        for d in range(1, Y):
            r1_copy(d, s).start()
        r1_copy(0, s).start()

    def reduce(s):
        for d in range(1, Y):
            r1_copy(d, s).wait_recv()
            mine = part[s, block_rows(lax.rem(chip + d, Y), core), :]
            p2[d - 1, s] = (mine.astype(f32) + r1[d, s].astype(f32)).astype(bf16)
            r2_copy(d, s).start()
        r1_copy(0, s).wait_recv()
        mine = part[s, block_rows(chip, core), :]
        nbuf[s] = (mine.astype(f32) + r1[0, s].astype(f32)).astype(bf16)
        near_copy(s).start()

    order = [0]
    for pair in pairs_of():
        order += list(pair)
    order.append(n_half)
    previous = None
    for i, slot in enumerate(order):
        if slot and slot < n_half:
            pump(PIECES_O)
        project_out(slot)
        if previous is not None:
            reduce(previous)
        previous = slot
    reduce(previous)

    ring_s.drain()
    ring_r.drain()
    ring_o.drain()
    for q in range(PIECES_T):
        for d in range(Y):
            t_copy(d, q).wait_send()
        for d in range(1, Y):
            u_copy(d, q).wait_send()

    @pl.when(last_tp & (sp < n - 1))
    def _():
        h_copy().wait_send()

    @pl.when(last_tp & (sp > 0))
    def _():
        for d in range(T - 1):
            g_copy(d).wait_send()

    x_copy().wait_send()

    @pl.when(z < depth - 1)
    def _():
        e_copy().wait_send()

    for s in range(n):
        for d in range(Y):
            r1_copy(d, s).wait_send()
        for d in range(1, Y):
            r2_copy(d, s).wait_send()
        near_copy(s).wait()
    for s in order:
        for d in range(1, Y):
            r2_copy(d, s).wait_recv()


def shifted(shard, axis, by):
    devices = lax.axis_size(axis)
    pairs = [(i, i + by) for i in range(devices) if 0 <= i + by < devices]
    return lax.ppermute(shard, axis, pairs)


def prefix(shard, axis, combine, identity):
    devices, index = (lax.axis_size(axis), lax.axis_index(axis))
    everything = jax.tree.map(
        lambda part, kind: lax.all_gather(part.astype(kind), axis),
        shard,
        (jnp.bfloat16, jnp.bfloat16),
    )
    start = jax.tree.map(
        lambda part, zero: jnp.broadcast_to(jnp.asarray(zero, part.dtype), part.shape),
        shard,
        identity,
    )

    def turn(k, before):
        reached = k < index
        new = combine(
            before, jax.tree.map(lambda part, own: part[k].astype(own.dtype), everything, shard)
        )
        return jax.tree.map(lambda a, b: jnp.where(reached, a, b), new, before)

    return lax.fori_loop(0, devices, turn, start)


def causal_taps(values, rim_rows, tap_weights):
    tap_count = tap_weights.shape[0]
    length = values.shape[0]
    padded = jnp.concatenate([rim_rows, values], axis=0)
    running = tap_weights[0] * padded[0:length]
    for offset in range(1, tap_count):
        running = running + tap_weights[offset] * padded[offset : offset + length]
    return running


def combine_states(earlier, later):
    return (earlier[0] * later[0], earlier[1] * later[0][:, None, None] + later[1])


def plain_path(
    tokens,
    input_norm_scale,
    outer_gate_weight,
    inner_gate_weight,
    value_weight_matrix,
    output_gate_weight,
    state_input_weight,
    write_key_weight,
    read_key_weight,
    step_size_weight,
    gated_conv_weight,
    input_conv_weight,
    write_conv_weight,
    read_conv_weight,
    step_size_bias,
    log_decay_rate,
    decay_spikes,
    direct_path_weight,
    head_norm_scale,
    conv_output_weight,
    state_output_weight,
):
    token_rows = tokens.astype(jnp.float32)
    scaled = token_rows * lax.rsqrt(
        jnp.mean(token_rows * token_rows, axis=1, keepdims=True) + epsilon
    )
    normed_own = (scaled * input_norm_scale.astype(jnp.float32)).astype(jnp.bfloat16)
    normed = lax.all_gather(normed_own, "tp", axis=0, tiled=True)
    length = normed.shape[0]
    pieces = (
        lax.all_gather(outer_gate_weight, "sp", axis=0, tiled=True),
        lax.all_gather(inner_gate_weight, "sp", axis=0, tiled=True),
        lax.all_gather(value_weight_matrix, "sp", axis=0, tiled=True),
        lax.all_gather(output_gate_weight, "sp", axis=0, tiled=True),
        lax.all_gather(state_input_weight, "sp", axis=0, tiled=True),
        lax.all_gather(write_key_weight, "sp", axis=0, tiled=True),
        lax.all_gather(read_key_weight, "sp", axis=0, tiled=True),
    )
    projected = tuple(
        (jnp.dot(normed, weight_rows, preferred_element_type=jnp.float32) for weight_rows in pieces)
    )
    outer_gate, inner_gate, conv_input, out_gate, state_input, write_keys, read_keys = [
        member.astype(jnp.bfloat16) for member in projected
    ]
    step_raw = jnp.dot(normed, step_size_weight, preferred_element_type=jnp.float32)
    short_rim = gated_conv_weight.shape[0] - 1
    state_rim = input_conv_weight.shape[0] - 1
    rim_rows = shifted(
        (
            inner_gate[length - short_rim :],
            conv_input[length - short_rim :],
            state_input[length - state_rim :],
            write_keys[length - state_rim :],
            read_keys[length - state_rim :],
        ),
        "sp",
        1,
    )
    product = inner_gate.astype(jnp.float32) * conv_input.astype(jnp.float32)
    rim_product = rim_rows[0].astype(jnp.float32) * rim_rows[1].astype(jnp.float32)
    mixer_part = (
        outer_gate.astype(jnp.float32)
        * causal_taps(product, rim_product, gated_conv_weight.astype(jnp.float32))
    ).astype(jnp.bfloat16)
    seq_input = jax.nn.silu(
        causal_taps(
            state_input.astype(jnp.float32),
            rim_rows[2].astype(jnp.float32),
            input_conv_weight.astype(jnp.float32),
        )
    )
    seq_write = jax.nn.silu(
        causal_taps(
            write_keys.astype(jnp.float32),
            rim_rows[3].astype(jnp.float32),
            write_conv_weight.astype(jnp.float32),
        )
    )
    seq_read = jax.nn.silu(
        causal_taps(
            read_keys.astype(jnp.float32),
            rim_rows[4].astype(jnp.float32),
            read_conv_weight.astype(jnp.float32),
        )
    )
    discrete_step = jax.nn.softplus(step_raw + step_size_bias[None, :])
    step_logarithm = discrete_step * (-jnp.exp(log_decay_rate))[None, :] + decay_spikes.T
    heads_here = discrete_step.shape[1]
    groups_here = seq_write.shape[1] // STATE
    per_group = heads_here // groups_here
    blocks = length // PLAIN_BLOCK
    input_blocks = seq_input.reshape(blocks, PLAIN_BLOCK, heads_here, HEAD_DIM)
    weighted = input_blocks * discrete_step.reshape(blocks, PLAIN_BLOCK, heads_here, 1)
    write_blocks = jnp.repeat(
        seq_write.reshape(blocks, PLAIN_BLOCK, groups_here, STATE), per_group, axis=2
    )
    read_blocks = jnp.repeat(seq_read.reshape(blocks, PLAIN_BLOCK, groups_here, STATE), per_group, axis=2)
    cumulative = jnp.cumsum(step_logarithm.reshape(blocks, PLAIN_BLOCK, heads_here), axis=1)
    causal = lax.broadcasted_iota(jnp.int32, (PLAIN_BLOCK, PLAIN_BLOCK), 0) >= lax.broadcasted_iota(
        jnp.int32, (PLAIN_BLOCK, PLAIN_BLOCK), 1
    )
    scores = jnp.einsum("clhm,cshm->clsh", read_blocks, write_blocks, precision=highest)
    damping = jnp.exp(
        jnp.where(
            causal[None, :, :, None],
            cumulative[:, :, None, :] - cumulative[:, None, :, :],
            -jnp.inf,
        )
    )
    within_block = jnp.einsum("clsh,cshp->clhp", scores * damping, weighted, precision=highest)
    to_end = jnp.exp(cumulative[:, -1:, :] - cumulative)
    block_states = jnp.einsum(
        "cshm,cshp->chpm", write_blocks * to_end[..., None], weighted, precision=highest
    )
    block_logs = cumulative[:, -1, :]

    def advance(carried_state, inputs):
        contribution, block_log = inputs
        return (carried_state * jnp.exp(block_log)[:, None, None] + contribution, carried_state)

    own_total, own_before = lax.scan(
        advance, jnp.zeros(block_states.shape[1:], jnp.float32), (block_states, block_logs)
    )
    total_log = jnp.sum(block_logs, axis=0)
    arriving = prefix(
        (jnp.exp(total_log), own_total),
        "sp",
        combine_states,
        (jnp.ones_like(total_log), jnp.zeros_like(own_total)),
    )[1]
    before_logs = jnp.cumsum(block_logs, axis=0) - block_logs
    entering = own_before + jnp.exp(before_logs)[:, :, None, None] * arriving[None]
    from_before = (
        jnp.einsum("clhm,chpm->clhp", read_blocks, entering, precision=highest)
        * jnp.exp(cumulative)[..., None]
    )
    head_out = within_block + from_before + direct_path_weight[None, None, :, None] * input_blocks
    head_out = head_out.reshape(length, heads_here * HEAD_DIM)
    gated_heads = (head_out * jax.nn.silu(out_gate.astype(jnp.float32))).reshape(
        length, heads_here, HEAD_DIM
    )
    normalized = gated_heads * lax.rsqrt(
        jnp.mean(gated_heads * gated_heads, axis=2, keepdims=True) + epsilon
    )
    state_part = (
        normalized.reshape(length, heads_here * HEAD_DIM) * head_norm_scale.astype(jnp.float32)
    ).astype(jnp.bfloat16)
    wide_mixer, wide_state = (
        lax.all_gather(conv_output_weight, "sp", axis=1, tiled=True),
        lax.all_gather(state_output_weight, "sp", axis=1, tiled=True),
    )
    return lax.psum_scatter(
        (
            jnp.dot(mixer_part, wide_mixer, preferred_element_type=jnp.float32)
            + jnp.dot(state_part, wide_state, preferred_element_type=jnp.float32)
        ).astype(jnp.bfloat16),
        "tp",
        scatter_dimension=0,
        tiled=True,
    )


def per_device(
    tokens, input_norm_scale, outer_gate_weight, inner_gate_weight, value_weight_matrix,
    output_gate_weight, state_input_weight, write_key_weight, read_key_weight, step_size_weight,
    gated_conv_weight, input_conv_weight, write_conv_weight, read_conv_weight, step_size_bias,
    log_decay_rate, decay_spikes, direct_path_weight, head_norm_scale, conv_output_weight,
    state_output_weight,
):
    n, T = lax.axis_size("sp"), lax.axis_size("tp")
    rows, width = tokens.shape
    kdim, cdim = outer_gate_weight.shape
    heads = step_size_bias.shape[0]
    hw = heads * HEAD_DIM
    length = rows * T
    ocols = conv_output_weight.shape[1]
    if (
        kdim % 128 or ocols % 256 or n % 2 or n < 4 or n > 16 or T % CORES
        or T < 2 * CORES
        or write_key_weight.shape[1] != STATE
    ):
        return plain_path(
            tokens, input_norm_scale, outer_gate_weight, inner_gate_weight,
            value_weight_matrix, output_gate_weight, state_input_weight, write_key_weight,
            read_key_weight, step_size_weight, gated_conv_weight, input_conv_weight,
            write_conv_weight, read_conv_weight, step_size_bias, log_decay_rate, decay_spikes,
            direct_path_weight, head_norm_scale, conv_output_weight, state_output_weight,
        )
    Y = T // CORES
    sm = pl.BlockSpec(memory_space=pltpu.SMEM)
    hbm = pl.BlockSpec(memory_space=pl.ANY)
    dma = pltpu.SemaphoreType.DMA
    s_cols, r_cols = cdim + 2 * STATE, 4 * cdim

    def like(array):
        return pltpu.VMEM(array.shape, array.dtype)

    step_t = step_size_weight.T
    near, far = pl.pallas_call(
        functools.partial(kernel, n, T),
        out_shape=(
            jax.ShapeDtypeStruct((rows, width), bf16),
            jax.ShapeDtypeStruct((Y - 1, rows, width), bf16),
        ),
        in_specs=[hbm] * 14 + [sm] * 2 + [hbm, sm, hbm] + [hbm] * 2,
        out_specs=(hbm, hbm),
        scratch_shapes=[
            like(tokens),
            like(input_norm_scale),
            like(step_t),
            like(gated_conv_weight),
            like(input_conv_weight),
            like(write_conv_weight),
            like(read_conv_weight),
            like(decay_spikes),
            like(head_norm_scale),
            pltpu.VMEM((n, kdim, s_cols), bf16),
            pltpu.VMEM((n, kdim, r_cols), bf16),
            pltpu.VMEM((n, cdim + hw, ocols), bf16),
            pltpu.VMEM((HALO + length, width), bf16),
            pltpu.VMEM((HALO + length, s_cols), f32),
            pltpu.VMEM((HALO + length, r_cols), f32),
            pltpu.VMEM((length, hw), bf16),
            pltpu.VMEM((length, hw), f32),
            pltpu.VMEM((length, STATE), bf16),
            pltpu.VMEM((length, STATE), bf16),
            pltpu.VMEM((length, hw), f32),
            pltpu.VMEM((length, hw), f32),
            pltpu.VMEM((length // CHUNK, STATE, hw), f32),
            pltpu.VMEM((STATE + HALO, hw), bf16),
            pltpu.VMEM((STATE + HALO, hw), bf16),
            pltpu.VMEM((STATE, hw), bf16),
            pltpu.VMEM((STATE, hw), bf16),
            pltpu.VMEM((3, STATE, hw), f32),
            pltpu.VMEM((length, cdim + hw), bf16),
            pltpu.VMEM((n, length, ocols), bf16),
            pltpu.VMEM((Y, n, rows, ocols), bf16),
            pltpu.VMEM((Y - 1, n, rows, ocols), bf16),
            pltpu.VMEM((n, rows, ocols), bf16),
            dma((18,)),
            dma((n // 2, PIECES_S, 2)),
            dma((n // 2, PIECES_S, 2)),
            dma((n // 2, PIECES_R, 2)),
            dma((n // 2, PIECES_R, 2)),
            dma((n // 2, PIECES_O, 2)),
            dma((n // 2, PIECES_O, 2)),
            dma((Y, PIECES_T)),
            dma((Y, PIECES_T)),
            dma((Y, PIECES_T)),
            dma((Y, PIECES_T)),
            dma((2,)),
            dma((2, T)),
            dma((2,)),
            dma((2,)),
            dma((Y, n)),
            dma((Y, n)),
            dma((Y, n)),
            dma((Y, n)),
            dma((n,)),
        ],
        compiler_params=pltpu.CompilerParams(
            collective_id=0, has_side_effects=True, vmem_limit_bytes=62 * 1024 * 1024
        ),
    )(
        tokens, input_norm_scale, outer_gate_weight, inner_gate_weight,
        value_weight_matrix, output_gate_weight, state_input_weight, write_key_weight,
        read_key_weight, step_t, gated_conv_weight, input_conv_weight, write_conv_weight,
        read_conv_weight, step_size_bias, log_decay_rate, decay_spikes, direct_path_weight,
        head_norm_scale,
        conv_output_weight, state_output_weight,
    )
    total = near.astype(f32)
    for d in range(Y - 1):
        total = total + far[d].astype(f32)
    return total.astype(bf16)


def solution(mesh):
    placed = (
        (P(("sp", "tp"), None), P())
        + (P("sp", "tp"),) * 7
        + (P(None, "tp"),) * 5
        + (P("tp"), P("tp"), P("tp", "sp"), P("tp"), P("tp"), P("tp", "sp"), P("tp", "sp"))
    )
    return jax.shard_map(
        per_device, mesh=mesh, in_specs=placed, out_specs=P(("sp", "tp"), None), check_vma=False
    )
```

```python
import functools

import jax
import jax.numpy as jnp
from jax import lax
from jax.experimental import pallas as pl
from jax.experimental.pallas import tpu as pltpu
from jax.sharding import PartitionSpec as P

HEAD_DIM = 64
STATE = 128
PLAIN_BLOCK = 64
CHUNK = 128
HALO = 16
PIECES_S = 4
PIECES_R = 8
PIECES_O = 4
PIECES_T = 2
CORES = 2
epsilon = 1e-05
highest = lax.Precision.HIGHEST
f32 = jnp.float32
bf16 = jnp.bfloat16
MESH = pl.DeviceIdType.MESH


def nt(a, b, precision=None):
    return lax.dot_general(
        a, b, (((1,), (1,)), ((), ())), preferred_element_type=f32, precision=precision
    )


def silu(v):
    return v / (1.0 + jnp.exp(-v))


class Ring:
    def __init__(self, n, pieces, buf, send, recv, neighbour):
        self.n, self.pieces, self.buf = n, pieces, buf
        self.send_sem, self.recv_sem, self.neighbour = send, recv, neighbour
        self.rows = buf.shape[1] // pieces
        self.waited = set()

    def copy(self, s, q, way):
        n = self.n
        src, dst = (s, s + 1) if way == 0 else ((n - s) % n, n - 1 - s)
        cut = pl.ds(q * self.rows, self.rows)
        return pltpu.make_async_remote_copy(
            src_ref=self.buf.at[src, cut],
            dst_ref=self.buf.at[dst, cut],
            send_sem=self.send_sem,
            recv_sem=self.recv_sem.at[self.flat(s, q, way)],
            device_id={"sp": self.neighbour[way]},
            device_id_type=MESH,
        )

    def flat(self, s, q, way):
        last = self.n // 2 - 1
        return (s * self.pieces + q) * 2 + way if s < last else last * self.pieces * 2 + q

    def ways(self, s, q):
        if s < self.n // 2 - 1:
            return (0, 1)
        return (0,) if q < self.pieces // 2 else (1,)

    def arrive(self, s, q, way):
        if (s, q, way) not in self.waited:
            self.waited.add((s, q, way))
            self.copy(s, q, way).wait_recv()

    def forward(self, s, q):
        for way in self.ways(s, q):
            if s > 0:
                self.arrive(s - 1, q, way)
            self.copy(s, q, way).start()

    def need(self, slot):
        last = self.n // 2
        for q in range(self.pieces):
            if 0 < slot < last:
                self.arrive(slot - 1, q, 0)
            elif slot > last:
                self.arrive(self.n - slot - 1, q, 1)
            elif slot == last:
                self.arrive(last - 1, q, self.ways(last - 1, q)[0])

    def order(self, first):
        return [(s, q) for s in range(first, self.n // 2) for q in range(self.pieces)]

    def drain(self):
        every = self.buf.at[pl.ds(0, self.n - 1)]
        pltpu.make_async_remote_copy(
            src_ref=every,
            dst_ref=every,
            send_sem=self.send_sem,
            recv_sem=self.recv_sem.at[0],
            device_id={"sp": self.neighbour[0]},
            device_id_type=MESH,
        ).wait_send()


def kernel(
    n,
    T,
    tokens_h, in_scale_h, w_outer, w_inner, w_value, w_ogate, w_state, w_write, w_read,
    step_w_h, taps_conv_h, taps_in_h, taps_wr_h, taps_rd_h,
    bias, rate, spikes_h, direct, hscale_h, o_conv, o_state,
    near, far,
    tokens, in_scale, step_w, taps_conv, taps_in, taps_wr, taps_rd, spikes, hscale,
    sbuf, rbuf, obuf, norm, acc_s, acc_r, mixbuf, xbuf, wrbuf, rdbuf, ybuf, cumbuf, stbuf,
    st_send, st_recv, e_send, e_recv, pair_buf, apart, part, r1, p2, nbuf,
    loc_sem, ss_sem, sr_sem, rs_sem, rr_sem, os_sem, or_sem,
    ts_sem, tr_sem, us_sem, ur_sem, h_sem, g_sem, x_sem, e_sem,
    r1s_sem, r1r_sem, r2s_sem, r2r_sem, near_sem,
):
    sp = lax.axis_index("sp")
    tp = lax.axis_index("tp")
    rows, width = tokens.shape
    kdim = w_outer.shape[0]
    cdim = w_outer.shape[1]
    length = rows * T
    heads_width = xbuf.shape[1]
    heads = heads_width // HEAD_DIM
    ocols = obuf.shape[2]
    n_half = n // 2
    Y = T // CORES

    barrier = pltpu.get_barrier_semaphore()
    for d in range(1, n):
        pl.semaphore_signal(
            barrier, inc=1, device_id={"sp": lax.rem(sp + d, n)}, device_id_type=MESH
        )
    for d in range(1, T):
        pl.semaphore_signal(
            barrier, inc=1, device_id={"tp": lax.rem(tp + d, T)}, device_id_type=MESH
        )

    def pack(refs, dst, rows_too=False):
        pairs, at = [], 0
        for ref in refs:
            if rows_too:
                pairs.append((ref, dst.at[0, pl.ds(at, ref.shape[0])]))
                at += ref.shape[0]
            else:
                pairs.append((ref, dst.at[0, :, pl.ds(at, ref.shape[1])]))
                at += ref.shape[1]
        return pairs

    groups = {
        "s": pack((w_state, w_write, w_read), sbuf),
        "t": [(tokens_h, tokens), (in_scale_h, in_scale)],
        "r": pack((w_ogate, w_outer, w_inner, w_value), rbuf),
        "v": [
            (step_w_h, step_w), (taps_conv_h, taps_conv), (taps_in_h, taps_in),
            (taps_wr_h, taps_wr), (taps_rd_h, taps_rd), (spikes_h, spikes), (hscale_h, hscale),
        ],
        "o": pack((o_conv, o_state), obuf, True),
    }
    whole = {"s": sbuf.at[0], "r": rbuf.at[0], "o": obuf.at[0]}
    local, index = {}, 0
    for name, pairs in groups.items():
        local[name] = []
        for src, dst in pairs:
            pltpu.make_async_copy(src, dst, loc_sem.at[index]).start()
            if name not in whole:
                local[name].append(pltpu.make_async_copy(src, dst, loc_sem.at[index]))
                index += 1
        if name in whole:
            local[name].append(
                pltpu.make_async_copy(whole[name], whole[name], loc_sem.at[index])
            )
            index += 1

    def landed(name):
        for copy in local[name]:
            copy.wait()

    def pos_of(index):
        odd = lax.rem(index, 2)
        low = lax.div(index, 2)
        return (1 - odd) * low + odd * (n - 1 - low)

    def index_of(pos):
        high = lax.div(pos, n_half)
        return (1 - high) * 2 * pos + high * (2 * (n - 1 - pos) + 1)

    pos = pos_of(sp)
    neighbour = (index_of(lax.rem(pos + 1, n)), index_of(lax.rem(pos + n - 1, n)))

    def owner_of(slot):
        return index_of(lax.rem(pos + n - slot, n))

    ring_s = Ring(n, PIECES_S, sbuf, ss_sem, sr_sem, neighbour)
    ring_r = Ring(n, PIECES_R, rbuf, rs_sem, rr_sem, neighbour)
    ring_o = Ring(n, PIECES_O, obuf, os_sem, or_sem, neighbour)

    own_at = pl.multiple_of(HALO + tp * rows, HALO)
    core = lax.rem(tp, CORES)
    chip = lax.div(tp, CORES)
    partner = chip * CORES + 1 - core
    prow = rows // PIECES_T

    def at_rows(block, q):
        return norm.at[pl.ds(pl.multiple_of(HALO + block * rows + q * prow, HALO), prow)]

    def t_copy(d, q):
        device = partner if d == 0 else lax.rem(chip + d, Y) * CORES + core
        return pltpu.make_async_remote_copy(
            src_ref=at_rows(tp, q),
            dst_ref=at_rows(tp, q),
            send_sem=ts_sem,
            recv_sem=tr_sem.at[d, q],
            device_id={"tp": device},
            device_id_type=MESH,
        )

    def u_copy(d, q):
        block = lax.rem(chip + Y - d, Y) * CORES + core
        return pltpu.make_async_remote_copy(
            src_ref=at_rows(block, q),
            dst_ref=at_rows(block, q),
            send_sem=us_sem,
            recv_sem=ur_sem.at[d, q],
            device_id={"tp": partner},
            device_id_type=MESH,
        )

    def h_copy():
        return pltpu.make_async_remote_copy(
            src_ref=norm.at[pl.ds(length, HALO)],
            dst_ref=norm.at[pl.ds(0, HALO)],
            send_sem=h_sem.at[0],
            recv_sem=h_sem.at[1],
            device_id={"sp": lax.rem(sp + 1, n)},
            device_id_type=MESH,
        )

    def g_copy(d):
        return pltpu.make_async_remote_copy(
            src_ref=norm.at[pl.ds(0, HALO)],
            dst_ref=norm.at[pl.ds(0, HALO)],
            send_sem=g_sem.at[0],
            recv_sem=g_sem.at[1],
            device_id={"tp": d},
            device_id_type=MESH,
        )

    last_tp = tp == T - 1

    landed("s")
    pl.semaphore_wait(barrier, n - 1 + T - 1)
    for q in range(PIECES_S):
        ring_s.forward(0, q)
    landed("t")
    x = tokens[...].astype(f32)
    x = x * lax.rsqrt(jnp.mean(x * x, axis=1, keepdims=True) + epsilon)
    norm[pl.ds(own_at, rows), :] = (x * in_scale[...].astype(f32).reshape(1, width)).astype(bf16)
    for q in range(PIECES_T):
        for d in range(1, Y):
            t_copy(d, q).start()
        t_copy(0, q).start()

    @pl.when(last_tp & (sp < n - 1))
    def _():
        h_copy().start()

    landed("r")
    r_own = [(0, q) for q in range(PIECES_R)]
    ring_r.forward(*r_own.pop(0))

    def t_forward(q):
        for d in range(1, Y):
            t_copy(d, q).wait_recv()
            u_copy(d, q).start()

    s_list = ring_s.order(1)
    hops = [s_list[i : i + PIECES_S] for i in range(0, len(s_list), PIECES_S)]
    for i, hop in enumerate(hops):
        for j, item in enumerate(hop):
            ring_s.forward(*item)
            if i == 1 and j == 0:
                t_forward(0)
            if i == 1 and j == 2:
                for q in range(1, PIECES_T):
                    t_forward(q)
        if i == 0:

            @pl.when(last_tp & (sp > 0))
            def _():
                h_copy().wait_recv()
                for d in range(T - 1):
                    g_copy(d).start()

        if i < len(hops) - 1:
            ring_r.forward(*r_own.pop(0))
    while r_own:
        ring_r.forward(*r_own.pop(0))

    r_list = ring_r.order(1)
    o_list = []

    def pump(count):
        for _ in range(count):
            if r_list:
                ring_r.forward(*r_list.pop(0))
            elif o_list:
                ring_o.forward(*o_list.pop(0))

    for q in range(PIECES_T):
        t_copy(0, q).wait_recv()
        for d in range(1, Y):
            pltpu.make_async_remote_copy(
                src_ref=at_rows(lax.rem(chip + Y - d, Y) * CORES + 1 - core, q),
                dst_ref=at_rows(lax.rem(chip + Y - d, Y) * CORES + 1 - core, q),
                send_sem=us_sem,
                recv_sem=ur_sem.at[d, q],
                device_id={"tp": partner},
                device_id_type=MESH,
            ).wait_recv()
    for d in range(T - 1):

        @pl.when((tp == d) & (sp > 0))
        def _():
            g_copy(d).wait_recv()

    @pl.when(sp == 0)
    def _():
        norm[0:HALO, :] = jnp.zeros((HALO, width), bf16)

    def project(ring, acc, slots, fresh=False):
        total_cols = acc.shape[1]
        for slot in slots:
            ring.need(slot)
        for c in range(0, total_cols, 256):
            total = None
            for slot in slots:
                at = pl.multiple_of(owner_of(slot) * kdim, kdim)
                term = jnp.dot(
                    norm[:, pl.ds(at, kdim)], ring.buf[slot, :, c : c + 256],
                    preferred_element_type=f32,
                )
                total = term if total is None else total + term
            if fresh:
                acc[:, c : c + 256] = total
            else:
                acc[:, c : c + 256] += total

    def pairs_of():
        return [(k, n - k) for k in range(1, n_half)]

    project(ring_s, acc_s, (0,), True)
    for pair in pairs_of():
        project(ring_s, acc_s, pair)
    early = min(2, PIECES_R)
    pump(early)
    project(ring_s, acc_s, (n_half,))

    def column(ref):
        index = lax.broadcasted_iota(jnp.int32, (heads, 1), 0)
        full = jnp.full((heads, 1), ref[0], f32)
        for h in range(1, heads):
            full = jnp.where(index == h, ref[h], full)
        return full

    landed("v")
    step = jax.nn.softplus(nt(step_w[...], norm[HALO:, :]) + column(bias))
    logs = -step * jnp.exp(column(rate)) + spikes[...]
    r_id = lax.broadcasted_iota(jnp.int32, (CHUNK, CHUNK), 0)
    c_id = lax.broadcasted_iota(jnp.int32, (CHUNK, CHUNK), 1)
    causal = r_id >= c_id
    lower = causal.astype(f32)
    eye = (r_id == c_id).astype(f32)
    lane = lax.broadcasted_iota(jnp.int32, (1, heads_width), 1)

    def spread(columns):
        full = jnp.broadcast_to(columns[:, 0:1], (columns.shape[0], heads_width))
        for h in range(1, heads):
            full = jnp.where(lane >= h * HEAD_DIM, columns[:, h : h + 1], full)
        return full

    def taps(u, weights):
        k_taps = weights.shape[0]
        w = weights[...].astype(f32)
        total = w[k_taps - 1 : k_taps] * u[8:]
        for k in range(k_taps - 1):
            total = total + w[k : k + 1] * pltpu.roll(u, k_taps - 1 - k, 0)[8:]
        return total

    blocks = length // CHUNK
    running = jnp.zeros((STATE, heads_width), f32)
    before = jnp.zeros((1, heads_width), f32)
    at_ogate, at_outer, at_inner, at_value = (i * cdim for i in range(4))
    at_state, at_write, at_read = 0, cdim, cdim + STATE

    def spans(b):
        t0 = b * CHUNK
        return (
            slice(t0, t0 + CHUNK),
            slice(t0 + HALO, t0 + HALO + CHUNK),
            slice(t0 + HALO - 8, t0 + HALO + CHUNK),
        )

    def field(acc, begin, size, span):
        return acc[span, begin : begin + size].astype(bf16).astype(f32)

    for b in range(blocks):
        span, own, take = spans(b)
        xs = silu(taps(field(acc_s, at_state, cdim, take), taps_in))
        wr = silu(taps(field(acc_s, at_write, STATE, take), taps_wr))
        rd = silu(taps(field(acc_s, at_read, STATE, take), taps_rd))
        cum = nt(lower, logs[:, span], highest)
        steps = nt(eye, step[:, span], highest)
        cum_wide = spread(cum)
        weighted = xs * spread(steps)
        xbuf[span, :] = xs
        mixbuf[span, :] = weighted.astype(bf16)
        wrbuf[span, :] = wr.astype(bf16)
        rdbuf[span, :] = rd.astype(bf16)
        cumbuf[span, :] = cum_wide
        last = cum_wide[CHUNK - 1 : CHUNK]
        scaled = (weighted * jnp.exp(last - cum_wide)).astype(bf16)
        stbuf[b] = running
        running = running * jnp.exp(last) + jnp.dot(
            wr.T.astype(bf16), scaled, preferred_element_type=f32
        )
        before = before + last
    st_send[0:STATE, :] = running.astype(bf16)
    st_send[STATE:, :] = jnp.broadcast_to(jnp.exp(before), (HALO, heads_width)).astype(bf16)

    z = lax.div(sp, 2)
    second = lax.rem(sp, 2)
    depth = n_half

    def x_copy():
        return pltpu.make_async_remote_copy(
            src_ref=st_send,
            dst_ref=st_recv,
            send_sem=x_sem.at[0],
            recv_sem=x_sem.at[1],
            device_id={"sp": sp + 1 - 2 * second},
            device_id_type=MESH,
        )

    def e_copy():
        return pltpu.make_async_remote_copy(
            src_ref=e_send,
            dst_ref=e_recv,
            send_sem=e_sem.at[0],
            recv_sem=e_sem.at[1],
            device_id={"sp": lax.rem(sp + 2, n)},
            device_id_type=MESH,
        )

    x_copy().start()
    pump(4)

    def within(b):
        span, _, _ = spans(b)
        scores = nt(rdbuf[span, :], wrbuf[span, :])
        cum_t = lax.dot_general(
            logs[:, span], lower, (((1,), (1,)), ((), ())),
            preferred_element_type=f32, precision=highest,
        )
        for pair in range(0, heads_width, 128):
            both = []
            for h in range(pair // HEAD_DIM, (pair + 128) // HEAD_DIM):
                diff = cumbuf[span, h * HEAD_DIM : h * HEAD_DIM + 1] - cum_t[h : h + 1, :]
                damped = scores * jnp.exp(jnp.where(causal, diff, -1e30))
                both.append(
                    jnp.dot(
                        damped.astype(bf16), mixbuf[span, pair : pair + 128],
                        preferred_element_type=f32,
                    )
                )
            first = lax.broadcasted_iota(jnp.int32, (1, 128), 1) < HEAD_DIM
            ybuf[span, pair : pair + 128] = jnp.where(first, both[0], both[1])

    for b in range(blocks):
        within(b)
        if b % 2 == 1:
            pump(1)
    x_copy().wait_recv()
    other = st_recv[0:STATE, :].astype(f32)
    other_decay = st_recv[STATE : STATE + 1, :].astype(f32)
    own_decay = jnp.exp(before)
    is_second = jnp.broadcast_to(second, (1, heads_width)) == 1
    pair_buf[0] = jnp.where(
        is_second, other * own_decay + running, running * other_decay + other
    )
    pair_buf[1] = jnp.where(is_second, other, jnp.zeros_like(other))
    pair_decay = own_decay * other_decay
    first_decay = jnp.where(is_second, other_decay, jnp.ones_like(other_decay))

    def link(j):
        @pl.when(z == j)
        def _():
            if j == 0:
                pair_buf[2] = jnp.zeros_like(pair_buf[2])
            else:
                e_copy().wait_recv()
                pair_buf[2] = e_recv[...].astype(f32)
            if j < depth - 1:
                e_send[...] = (pair_buf[2] * pair_decay + pair_buf[0]).astype(bf16)
                e_copy().start()

    link(0)
    project(ring_r, acc_r, (0,), True)
    landed("o")
    for k, pair in enumerate(pairs_of()):
        if k < n_half - 2:
            pump(PIECES_R // 2)
            project(ring_r, acc_r, pair)
            link(k + 1)
            pump(PIECES_R // 2)
        else:
            pump(len(r_list))
            for q in range(PIECES_O):
                ring_o.forward(0, q)
            o_list += ring_o.order(1)
            project(ring_r, acc_r, pair)
            for j in range(k + 1, depth):
                link(j)

    group = (
        lax.div(lax.broadcasted_iota(jnp.int32, (heads_width, heads_width), 0), HEAD_DIM)
        == lax.div(lax.broadcasted_iota(jnp.int32, (heads_width, heads_width), 1), HEAD_DIM)
    ).astype(bf16)
    direct_wide = jnp.full((1, heads_width), direct[0], f32)
    for h in range(1, heads):
        direct_wide = jnp.where(lane >= h * HEAD_DIM, direct[h], direct_wide)

    arriving = pair_buf[1] + first_decay * pair_buf[2]
    so_far = jnp.zeros((1, heads_width), f32)
    for b in range(blocks):
        span, _, _ = spans(b)
        cum_wide = cumbuf[span, :]
        entering = (stbuf[b] + jnp.exp(so_far) * arriving).astype(bf16)
        so_far = so_far + cum_wide[CHUNK - 1 : CHUNK]
        ybuf[span, :] = (
            ybuf[span, :]
            + jnp.dot(rdbuf[span, :], entering, preferred_element_type=f32) * jnp.exp(cum_wide)
            + direct_wide * xbuf[span, :]
        )

    project(ring_r, acc_r, (n_half,))

    for b in range(blocks):
        span, own, take = spans(b)
        product = field(acc_r, at_inner, cdim, take) * field(acc_r, at_value, cdim, take)
        mix = field(acc_r, at_outer, cdim, own) * taps(product, taps_conv)
        apart[span, 0:cdim] = mix.astype(bf16)
        gated = ybuf[span, :] * silu(field(acc_r, at_ogate, cdim, own))
        square = jnp.dot((gated * gated).astype(bf16), group, preferred_element_type=f32)
        normalized = gated * lax.rsqrt(square * (1.0 / HEAD_DIM) + epsilon)
        apart[span, cdim:] = (
            normalized * hscale[...].astype(f32).reshape(1, heads_width)
        ).astype(bf16)

    def block_rows(y, c):
        return pl.ds(pl.multiple_of((y * CORES + c) * rows, rows), rows)

    def columns_of(slot):
        return pl.ds(pl.multiple_of(owner_of(slot) * ocols, ocols), ocols)

    def r1_copy(d, s):
        return pltpu.make_async_remote_copy(
            src_ref=part.at[s, block_rows(lax.rem(chip + d, Y), 1 - core)],
            dst_ref=r1.at[s, d],
            send_sem=r1s_sem,
            recv_sem=r1r_sem.at[s],
            device_id={"tp": partner},
            device_id_type=MESH,
        )

    def bulk(ref, send, recv, device):
        return pltpu.make_async_remote_copy(
            src_ref=ref, dst_ref=ref, send_sem=send, recv_sem=recv, device_id={"tp": device},
            device_id_type=MESH,
        )

    def r1_all(ref, recv):
        return bulk(ref, r1s_sem, recv, partner)

    def r2_copy(d, s):
        return pltpu.make_async_remote_copy(
            src_ref=p2.at[d - 1, s],
            dst_ref=far.at[d - 1, :, columns_of(s)],
            send_sem=r2s_sem,
            recv_sem=r2r_sem,
            device_id={"tp": lax.rem(chip + d, Y) * CORES + core},
            device_id_type=MESH,
        )

    def near_copy(s):
        return pltpu.make_async_copy(nbuf.at[s], near.at[:, columns_of(s)], near_sem)

    def project_out(s):
        ring_o.need(s)
        part[s] = jnp.dot(apart[...], obuf[s], preferred_element_type=f32).astype(bf16)
        for d in range(1, Y):
            r1_copy(d, s).start()
        r1_copy(0, s).start()

    def reduce(s):
        r1_all(r1.at[s], r1r_sem.at[s]).wait_recv()
        for d in range(1, Y):
            mine = part[s, block_rows(lax.rem(chip + d, Y), core), :]
            p2[d - 1, s] = (mine.astype(f32) + r1[s, d].astype(f32)).astype(bf16)
            r2_copy(d, s).start()
        mine = part[s, block_rows(chip, core), :]
        nbuf[s] = (mine.astype(f32) + r1[s, 0].astype(f32)).astype(bf16)
        near_copy(s).start()

    order = [0]
    for pair in pairs_of():
        order += list(pair)
    order.append(n_half)
    previous = None
    for i, slot in enumerate(order):
        if slot and slot < n_half:
            pump(PIECES_O)
        if slot == n_half:
            reduce(previous)
        project_out(slot)
        if slot != n_half and previous is not None:
            reduce(previous)
        previous = slot
    reduce(previous)

    ring_s.drain()
    ring_r.drain()
    ring_o.drain()
    bulk(norm.at[pl.ds(0, Y * rows)], ts_sem, tr_sem.at[0, 0], partner).wait_send()
    bulk(norm.at[pl.ds(0, (Y - 1) * rows)], us_sem, ur_sem.at[0, 0], partner).wait_send()

    @pl.when(last_tp & (sp < n - 1))
    def _():
        h_copy().wait_send()

    @pl.when(last_tp & (sp > 0))
    def _():
        bulk(norm.at[pl.ds(0, (T - 1) * HALO)], g_sem.at[0], g_sem.at[1], partner).wait_send()

    x_copy().wait_send()

    @pl.when(z < depth - 1)
    def _():
        e_copy().wait_send()

    r1_all(r1, r1r_sem.at[0]).wait_send()
    bulk(p2, r2s_sem, r2r_sem, partner).wait_send()
    pltpu.make_async_copy(far.at[0], near, near_sem).wait()
    bulk(far, r2s_sem, r2r_sem, partner).wait_recv()


def shifted(shard, axis, by):
    devices = lax.axis_size(axis)
    pairs = [(i, i + by) for i in range(devices) if 0 <= i + by < devices]
    return lax.ppermute(shard, axis, pairs)


def prefix(shard, axis, combine, identity):
    devices, index = (lax.axis_size(axis), lax.axis_index(axis))
    everything = jax.tree.map(
        lambda part, kind: lax.all_gather(part.astype(kind), axis),
        shard,
        (jnp.bfloat16, jnp.bfloat16),
    )
    start = jax.tree.map(
        lambda part, zero: jnp.broadcast_to(jnp.asarray(zero, part.dtype), part.shape),
        shard,
        identity,
    )

    def turn(k, before):
        reached = k < index
        new = combine(
            before, jax.tree.map(lambda part, own: part[k].astype(own.dtype), everything, shard)
        )
        return jax.tree.map(lambda a, b: jnp.where(reached, a, b), new, before)

    return lax.fori_loop(0, devices, turn, start)


def causal_taps(values, rim_rows, tap_weights):
    tap_count = tap_weights.shape[0]
    length = values.shape[0]
    padded = jnp.concatenate([rim_rows, values], axis=0)
    running = tap_weights[0] * padded[0:length]
    for offset in range(1, tap_count):
        running = running + tap_weights[offset] * padded[offset : offset + length]
    return running


def combine_states(earlier, later):
    return (earlier[0] * later[0], earlier[1] * later[0][:, None, None] + later[1])


def plain_path(
    tokens,
    input_norm_scale,
    outer_gate_weight,
    inner_gate_weight,
    value_weight_matrix,
    output_gate_weight,
    state_input_weight,
    write_key_weight,
    read_key_weight,
    step_size_weight,
    gated_conv_weight,
    input_conv_weight,
    write_conv_weight,
    read_conv_weight,
    step_size_bias,
    log_decay_rate,
    decay_spikes,
    direct_path_weight,
    head_norm_scale,
    conv_output_weight,
    state_output_weight,
):
    token_rows = tokens.astype(jnp.float32)
    scaled = token_rows * lax.rsqrt(
        jnp.mean(token_rows * token_rows, axis=1, keepdims=True) + epsilon
    )
    normed_own = (scaled * input_norm_scale.astype(jnp.float32)).astype(jnp.bfloat16)
    normed = lax.all_gather(normed_own, "tp", axis=0, tiled=True)
    length = normed.shape[0]
    pieces = (
        lax.all_gather(outer_gate_weight, "sp", axis=0, tiled=True),
        lax.all_gather(inner_gate_weight, "sp", axis=0, tiled=True),
        lax.all_gather(value_weight_matrix, "sp", axis=0, tiled=True),
        lax.all_gather(output_gate_weight, "sp", axis=0, tiled=True),
        lax.all_gather(state_input_weight, "sp", axis=0, tiled=True),
        lax.all_gather(write_key_weight, "sp", axis=0, tiled=True),
        lax.all_gather(read_key_weight, "sp", axis=0, tiled=True),
    )
    projected = tuple(
        (jnp.dot(normed, weight_rows, preferred_element_type=jnp.float32) for weight_rows in pieces)
    )
    outer_gate, inner_gate, conv_input, out_gate, state_input, write_keys, read_keys = [
        member.astype(jnp.bfloat16) for member in projected
    ]
    step_raw = jnp.dot(normed, step_size_weight, preferred_element_type=jnp.float32)
    short_rim = gated_conv_weight.shape[0] - 1
    state_rim = input_conv_weight.shape[0] - 1
    rim_rows = shifted(
        (
            inner_gate[length - short_rim :],
            conv_input[length - short_rim :],
            state_input[length - state_rim :],
            write_keys[length - state_rim :],
            read_keys[length - state_rim :],
        ),
        "sp",
        1,
    )
    product = inner_gate.astype(jnp.float32) * conv_input.astype(jnp.float32)
    rim_product = rim_rows[0].astype(jnp.float32) * rim_rows[1].astype(jnp.float32)
    mixer_part = (
        outer_gate.astype(jnp.float32)
        * causal_taps(product, rim_product, gated_conv_weight.astype(jnp.float32))
    ).astype(jnp.bfloat16)
    seq_input = jax.nn.silu(
        causal_taps(
            state_input.astype(jnp.float32),
            rim_rows[2].astype(jnp.float32),
            input_conv_weight.astype(jnp.float32),
        )
    )
    seq_write = jax.nn.silu(
        causal_taps(
            write_keys.astype(jnp.float32),
            rim_rows[3].astype(jnp.float32),
            write_conv_weight.astype(jnp.float32),
        )
    )
    seq_read = jax.nn.silu(
        causal_taps(
            read_keys.astype(jnp.float32),
            rim_rows[4].astype(jnp.float32),
            read_conv_weight.astype(jnp.float32),
        )
    )
    discrete_step = jax.nn.softplus(step_raw + step_size_bias[None, :])
    step_logarithm = discrete_step * (-jnp.exp(log_decay_rate))[None, :] + decay_spikes.T
    heads_here = discrete_step.shape[1]
    groups_here = seq_write.shape[1] // STATE
    per_group = heads_here // groups_here
    blocks = length // PLAIN_BLOCK
    input_blocks = seq_input.reshape(blocks, PLAIN_BLOCK, heads_here, HEAD_DIM)
    weighted = input_blocks * discrete_step.reshape(blocks, PLAIN_BLOCK, heads_here, 1)
    write_blocks = jnp.repeat(
        seq_write.reshape(blocks, PLAIN_BLOCK, groups_here, STATE), per_group, axis=2
    )
    read_blocks = jnp.repeat(seq_read.reshape(blocks, PLAIN_BLOCK, groups_here, STATE), per_group, axis=2)
    cumulative = jnp.cumsum(step_logarithm.reshape(blocks, PLAIN_BLOCK, heads_here), axis=1)
    causal = lax.broadcasted_iota(jnp.int32, (PLAIN_BLOCK, PLAIN_BLOCK), 0) >= lax.broadcasted_iota(
        jnp.int32, (PLAIN_BLOCK, PLAIN_BLOCK), 1
    )
    scores = jnp.einsum("clhm,cshm->clsh", read_blocks, write_blocks, precision=highest)
    damping = jnp.exp(
        jnp.where(
            causal[None, :, :, None],
            cumulative[:, :, None, :] - cumulative[:, None, :, :],
            -jnp.inf,
        )
    )
    within_block = jnp.einsum("clsh,cshp->clhp", scores * damping, weighted, precision=highest)
    to_end = jnp.exp(cumulative[:, -1:, :] - cumulative)
    block_states = jnp.einsum(
        "cshm,cshp->chpm", write_blocks * to_end[..., None], weighted, precision=highest
    )
    block_logs = cumulative[:, -1, :]

    def advance(carried_state, inputs):
        contribution, block_log = inputs
        return (carried_state * jnp.exp(block_log)[:, None, None] + contribution, carried_state)

    own_total, own_before = lax.scan(
        advance, jnp.zeros(block_states.shape[1:], jnp.float32), (block_states, block_logs)
    )
    total_log = jnp.sum(block_logs, axis=0)
    arriving = prefix(
        (jnp.exp(total_log), own_total),
        "sp",
        combine_states,
        (jnp.ones_like(total_log), jnp.zeros_like(own_total)),
    )[1]
    before_logs = jnp.cumsum(block_logs, axis=0) - block_logs
    entering = own_before + jnp.exp(before_logs)[:, :, None, None] * arriving[None]
    from_before = (
        jnp.einsum("clhm,chpm->clhp", read_blocks, entering, precision=highest)
        * jnp.exp(cumulative)[..., None]
    )
    head_out = within_block + from_before + direct_path_weight[None, None, :, None] * input_blocks
    head_out = head_out.reshape(length, heads_here * HEAD_DIM)
    gated_heads = (head_out * jax.nn.silu(out_gate.astype(jnp.float32))).reshape(
        length, heads_here, HEAD_DIM
    )
    normalized = gated_heads * lax.rsqrt(
        jnp.mean(gated_heads * gated_heads, axis=2, keepdims=True) + epsilon
    )
    state_part = (
        normalized.reshape(length, heads_here * HEAD_DIM) * head_norm_scale.astype(jnp.float32)
    ).astype(jnp.bfloat16)
    wide_mixer, wide_state = (
        lax.all_gather(conv_output_weight, "sp", axis=1, tiled=True),
        lax.all_gather(state_output_weight, "sp", axis=1, tiled=True),
    )
    return lax.psum_scatter(
        (
            jnp.dot(mixer_part, wide_mixer, preferred_element_type=jnp.float32)
            + jnp.dot(state_part, wide_state, preferred_element_type=jnp.float32)
        ).astype(jnp.bfloat16),
        "tp",
        scatter_dimension=0,
        tiled=True,
    )


def per_device(
    tokens, input_norm_scale, outer_gate_weight, inner_gate_weight, value_weight_matrix,
    output_gate_weight, state_input_weight, write_key_weight, read_key_weight, step_size_weight,
    gated_conv_weight, input_conv_weight, write_conv_weight, read_conv_weight, step_size_bias,
    log_decay_rate, decay_spikes, direct_path_weight, head_norm_scale, conv_output_weight,
    state_output_weight,
):
    n, T = lax.axis_size("sp"), lax.axis_size("tp")
    rows, width = tokens.shape
    kdim, cdim = outer_gate_weight.shape
    heads = step_size_bias.shape[0]
    hw = heads * HEAD_DIM
    length = rows * T
    ocols = conv_output_weight.shape[1]
    if (
        kdim % 128 or ocols % 256 or n % 2 or n < 4 or n > 16 or T % CORES
        or T < 2 * CORES
        or write_key_weight.shape[1] != STATE
    ):
        return plain_path(
            tokens, input_norm_scale, outer_gate_weight, inner_gate_weight,
            value_weight_matrix, output_gate_weight, state_input_weight, write_key_weight,
            read_key_weight, step_size_weight, gated_conv_weight, input_conv_weight,
            write_conv_weight, read_conv_weight, step_size_bias, log_decay_rate, decay_spikes,
            direct_path_weight, head_norm_scale, conv_output_weight, state_output_weight,
        )
    Y = T // CORES
    sm = pl.BlockSpec(memory_space=pltpu.SMEM)
    hbm = pl.BlockSpec(memory_space=pl.ANY)
    dma = pltpu.SemaphoreType.DMA
    s_cols, r_cols = cdim + 2 * STATE, 4 * cdim

    def like(array):
        return pltpu.VMEM(array.shape, array.dtype)

    step_t = step_size_weight.T
    near, far = pl.pallas_call(
        functools.partial(kernel, n, T),
        out_shape=(
            jax.ShapeDtypeStruct((rows, width), bf16),
            jax.ShapeDtypeStruct((Y - 1, rows, width), bf16),
        ),
        in_specs=[hbm] * 14 + [sm] * 2 + [hbm, sm, hbm] + [hbm] * 2,
        out_specs=(hbm, hbm),
        scratch_shapes=[
            like(tokens),
            like(input_norm_scale),
            like(step_t),
            like(gated_conv_weight),
            like(input_conv_weight),
            like(write_conv_weight),
            like(read_conv_weight),
            like(decay_spikes),
            like(head_norm_scale),
            pltpu.VMEM((n, kdim, s_cols), bf16),
            pltpu.VMEM((n, kdim, r_cols), bf16),
            pltpu.VMEM((n, cdim + hw, ocols), bf16),
            pltpu.VMEM((HALO + length, width), bf16),
            pltpu.VMEM((HALO + length, s_cols), f32),
            pltpu.VMEM((HALO + length, r_cols), f32),
            pltpu.VMEM((length, hw), bf16),
            pltpu.VMEM((length, hw), f32),
            pltpu.VMEM((length, STATE), bf16),
            pltpu.VMEM((length, STATE), bf16),
            pltpu.VMEM((length, hw), f32),
            pltpu.VMEM((length, hw), f32),
            pltpu.VMEM((length // CHUNK, STATE, hw), f32),
            pltpu.VMEM((STATE + HALO, hw), bf16),
            pltpu.VMEM((STATE + HALO, hw), bf16),
            pltpu.VMEM((STATE, hw), bf16),
            pltpu.VMEM((STATE, hw), bf16),
            pltpu.VMEM((3, STATE, hw), f32),
            pltpu.VMEM((length, cdim + hw), bf16),
            pltpu.VMEM((n, length, ocols), bf16),
            pltpu.VMEM((n, Y, rows, ocols), bf16),
            pltpu.VMEM((Y - 1, n, rows, ocols), bf16),
            pltpu.VMEM((n, rows, ocols), bf16),
            dma((12,)),
            dma,
            dma(((n - 1) * PIECES_S,)),
            dma,
            dma(((n - 1) * PIECES_R,)),
            dma,
            dma(((n - 1) * PIECES_O,)),
            dma,
            dma((Y, PIECES_T)),
            dma,
            dma((Y, PIECES_T)),
            dma((2,)),
            dma((2,)),
            dma((2,)),
            dma((2,)),
            dma,
            dma((n,)),
            dma,
            dma,
            dma,
        ],
        compiler_params=pltpu.CompilerParams(
            collective_id=0, has_side_effects=True, vmem_limit_bytes=62 * 1024 * 1024
        ),
    )(
        tokens, input_norm_scale, outer_gate_weight, inner_gate_weight,
        value_weight_matrix, output_gate_weight, state_input_weight, write_key_weight,
        read_key_weight, step_t, gated_conv_weight, input_conv_weight, write_conv_weight,
        read_conv_weight, step_size_bias, log_decay_rate, decay_spikes, direct_path_weight,
        head_norm_scale,
        conv_output_weight, state_output_weight,
    )
    total = near.astype(f32)
    for d in range(Y - 1):
        total = total + far[d].astype(f32)
    return total.astype(bf16)


def solution(mesh):
    placed = (
        (P(("sp", "tp"), None), P())
        + (P("sp", "tp"),) * 7
        + (P(None, "tp"),) * 5
        + (P("tp"), P("tp"), P("tp", "sp"), P("tp"), P("tp"), P("tp", "sp"), P("tp", "sp"))
    )
    return jax.shard_map(
        per_device, mesh=mesh, in_specs=placed, out_specs=P(("sp", "tp"), None), check_vma=False
    )
```

```python
import functools

import jax
import jax.numpy as jnp
from jax import lax
from jax.experimental import pallas as pl
from jax.experimental.pallas import tpu as pltpu
from jax.sharding import PartitionSpec as P

HEAD_DIM = 64
STATE = 128
PLAIN_BLOCK = 64
CHUNK = 128
HALO = 16
PIECES_S = 4
PIECES_G = 2
PIECES_C = 4
PIECES_O = 2
PIECES_T = 2
PIECES_U = 4
PLANES = 4
CORES = 2
epsilon = 1e-05
highest = lax.Precision.HIGHEST
f32 = jnp.float32
bf16 = jnp.bfloat16
MESH = pl.DeviceIdType.MESH


def nt(a, b, precision=None):
    return lax.dot_general(
        a, b, (((1,), (1,)), ((), ())), preferred_element_type=f32, precision=precision
    )


def silu(v):
    return v / (1.0 + jnp.exp(-v))


def remote(src, dst, send, recv, device):
    return pltpu.make_async_remote_copy(
        src_ref=src, dst_ref=dst, send_sem=send, recv_sem=recv, device_id=device,
        device_id_type=MESH,
    )


class Slots:
    def __init__(self, buf, pieces, recv):
        self.buf, self.pieces, self.recv = buf, pieces, recv
        self.rows = buf.shape[1] // pieces
        self.waited = set()

    def piece(self, slot, q):
        return self.buf.at[slot, pl.ds(q * self.rows, self.rows)]

    def send(self, src, dst, q, sem, device):
        remote(
            self.piece(src, q), self.piece(dst, q), sem,
            self.recv.at[(dst - 1) * self.pieces + q], {"sp": device},
        ).start()

    def arrive(self, slot, q, sem, device):
        if (slot, q) not in self.waited:
            self.waited.add((slot, q))
            remote(
                self.piece(slot, q), self.piece(slot, q), sem,
                self.recv.at[(slot - 1) * self.pieces + q], {"sp": device},
            ).wait_recv()


def kernel(
    n,
    T,
    tokens_h, in_scale_h, w_outer, w_inner, w_value, w_ogate, w_state, w_write, w_read,
    step_w_h, taps_conv_h, taps_in_h, taps_wr_h, taps_rd_h,
    bias, rate, spikes_h, direct, hscale_h, o_conv, o_state,
    near, far,
    tokens, in_scale, step_w, taps_conv, taps_in, taps_wr, taps_rd, spikes, hscale,
    sbuf, gbuf, cbuf, obuf, norm, norm2, spikes2, acc_s, acc_g, acc_c,
    mixbuf, xbuf, wrbuf, rdbuf, ybuf, cumbuf, stbuf, runbuf, decbuf,
    st_send, st_recv, e_send, e_recv, mbuf, apart, part, r1, p2, nbuf,
    loc_sem, ss_sem, sr_sem, gs_sem, gr_sem, cs_sem, cr_sem, os_sem, ox_sem, or_sem,
    ts_sem, tr_sem, us_sem, ur_sem, vs_sem, vr_sem, t2s_sem, t2r_sem, u2s_sem, u2r_sem,
    h_sem, g_sem, k_sem, l_sem, x_sem, e_sem, ms_sem, mr_sem,
    r1s_sem, r1r_sem, r2s_sem, r2r_sem, near_sem,
):
    sp = lax.axis_index("sp")
    tp = lax.axis_index("tp")
    rows, width = tokens.shape
    kdim = w_outer.shape[0]
    cdim = w_outer.shape[1]
    length = rows * T
    heads_width = mbuf.shape[1]
    heads = heads_width // HEAD_DIM
    ocols = obuf.shape[2]
    Y = T // CORES

    barrier = pltpu.get_barrier_semaphore()
    for d in range(1, n):
        pl.semaphore_signal(
            barrier, inc=1, device_id={"sp": lax.rem(sp + d, n)}, device_id_type=MESH
        )
    for d in range(1, T):
        pl.semaphore_signal(
            barrier, inc=1, device_id={"tp": lax.rem(tp + d, T)}, device_id_type=MESH
        )

    def pack(refs, dst, rows_too=False):
        pairs, at = [], 0
        for ref in refs:
            if rows_too:
                pairs.append((ref, dst.at[0, pl.ds(at, ref.shape[0])]))
                at += ref.shape[0]
            else:
                pairs.append((ref, dst.at[0, :, pl.ds(at, ref.shape[1])]))
                at += ref.shape[1]
        return pairs

    groups = {
        "s": pack((w_state, w_write, w_read), sbuf),
        "t": [(tokens_h, tokens), (in_scale_h, in_scale)],
        "c": pack((w_outer, w_inner, w_value), cbuf),
        "g": pack((w_ogate,), gbuf),
        "v": [
            (spikes_h, spikes), (step_w_h, step_w), (taps_conv_h, taps_conv),
            (taps_in_h, taps_in), (taps_wr_h, taps_wr), (taps_rd_h, taps_rd), (hscale_h, hscale),
        ],
        "o": pack((o_conv, o_state), obuf, True),
    }
    whole = {"s": sbuf.at[0], "c": cbuf.at[0], "g": gbuf.at[0], "o": obuf.at[0]}
    local, index = {}, 0
    for name, pairs in groups.items():
        local[name] = []
        for src, dst in pairs:
            pltpu.make_async_copy(src, dst, loc_sem.at[index]).start()
            if name not in whole:
                local[name].append(pltpu.make_async_copy(src, dst, loc_sem.at[index]))
                index += 1
        if name in whole:
            local[name].append(
                pltpu.make_async_copy(whole[name], whole[name], loc_sem.at[index])
            )
            index += 1

    def landed(name):
        for copy in local[name]:
            copy.wait()

    z = lax.div(sp, 2)
    x = lax.rem(sp, 2)
    last_z = PLANES - 1
    odd_z = lax.rem(z, 2)
    pz = z + 1 - 2 * odd_z
    upper = lax.div(z, 2)
    inner_z = 1 + upper
    end_z = upper * last_z
    is_inner = z == inner_z
    inner = (1 - upper) * odd_z + upper * (1 - odd_z)
    mate = pz * 2 + x
    side = z * 2 + 1 - x
    cross = (last_z - z) * 2 + x
    beyond = inner * cross + (1 - inner) * side

    def pos_of(index):
        odd = lax.rem(index, 2)
        low = lax.div(index, 2)
        return (1 - odd) * low + odd * (n - 1 - low)

    def index_of(pos):
        high = lax.div(pos, n // 2)
        return (1 - high) * 2 * pos + high * (2 * (n - 1 - pos) + 1)

    pos = pos_of(sp)
    toward = pos_of(mate) - pos

    def plane_owner(slot):
        plane = (z, pz, last_z - inner_z, last_z - end_z)[slot % 4]
        return plane * 2 + (x if slot < 4 else 1 - x)

    def ring_slot(side_k, s):
        return n - 1 if s == n // 2 else 1 + side_k * (n // 2 - 1) + s - 1

    def ring_owner(slot):
        if slot == 0:
            return sp
        if slot == n - 1:
            return index_of(lax.rem(pos + n // 2, n))
        side_k, s = divmod(slot - 1, n // 2 - 1)
        way = toward if side_k == 0 else -toward
        return index_of(lax.rem(pos + n + way * (s + 1), n))

    link_device = (mate, beyond)

    class Ring:
        def __init__(self):
            self.rows = kdim // PIECES_C
            self.waited = set()

        def piece(self, slot, q):
            return cbuf.at[slot, pl.ds(q * self.rows, self.rows)]

        def has(self, link, s, q):
            return s < n // 2 - 1 or (q < PIECES_C // 2) == (link == 0)

        def copy(self, link, s, q):
            src = 0 if s == 0 else ring_slot(1 - link, s)
            dst = ring_slot(link, s + 1)
            return remote(
                self.piece(src, q), self.piece(dst, q), cs_sem,
                cr_sem.at[(dst - 1) * PIECES_C + q], {"sp": link_device[link]},
            )

        def arrive(self, slot, q):
            if (slot, q) not in self.waited:
                self.waited.add((slot, q))
                remote(
                    self.piece(slot, q), self.piece(slot, q), cs_sem,
                    cr_sem.at[(slot - 1) * PIECES_C + q], {"sp": mate},
                ).wait_recv()

        def forward(self, link, s, q):
            if s > 0:
                self.arrive(ring_slot(1 - link, s), q)
            self.copy(link, s, q).start()

        def need(self, slot):
            if slot:
                for q in range(PIECES_C):
                    self.arrive(slot, q)

    own_at = pl.multiple_of(HALO + tp * rows, HALO)
    core = lax.rem(tp, CORES)
    chip = lax.div(tp, CORES)
    partner = chip * CORES + 1 - core
    last_tp = tp == T - 1

    def spread_rows(ref, pieces, near_send, near_recv, far_send, far_recv):
        prow = rows // pieces

        def at_rows(block, q):
            return ref.at[pl.ds(pl.multiple_of(HALO + block * rows + q * prow, HALO), prow)]

        def first(d, q):
            device = partner if d == 0 else lax.rem(chip + d, Y) * CORES + core
            return remote(
                at_rows(tp, q), at_rows(tp, q), near_send, near_recv.at[d, q], {"tp": device}
            )

        def second(d, q, at_core):
            block = lax.rem(chip + Y - d, Y) * CORES + at_core
            return remote(
                at_rows(block, q), at_rows(block, q), far_send, far_recv.at[d, q],
                {"tp": partner},
            )

        def start(q):
            for d in range(1, Y):
                first(d, q).start()
            first(0, q).start()

        def relay(q):
            for d in range(1, Y):
                first(d, q).wait_recv()
                second(d, q, core).start()

        def finish():
            for q in range(pieces):
                first(0, q).wait_recv()
                for d in range(1, Y):
                    second(d, q, 1 - core).wait_recv()

        return at_rows, start, relay, finish

    _, t_start, t_relay, t_finish = spread_rows(norm, PIECES_T, ts_sem, tr_sem, us_sem, ur_sem)
    u_rows, u_start, u_relay, u_finish = spread_rows(
        norm2, PIECES_U, t2s_sem, t2r_sem, u2s_sem, u2r_sem
    )

    def v_copy(q):
        prow = rows // PIECES_U
        src = norm.at[pl.ds(pl.multiple_of(own_at + q * prow, HALO), prow)]
        return remote(src, u_rows(tp, q), vs_sem, vr_sem.at[q], {"sp": mate})

    def k_copy():
        cut = pl.ds(0, HALO)
        return remote(norm.at[cut], norm2.at[cut], k_sem.at[0], k_sem.at[1], {"sp": mate})

    def l_copy():
        return remote(spikes, spikes2, l_sem.at[0], l_sem.at[1], {"sp": mate})

    def h_copy():
        return remote(
            norm.at[pl.ds(length, HALO)], norm.at[pl.ds(0, HALO)], h_sem.at[0], h_sem.at[1],
            {"sp": lax.rem(sp + 1, n)},
        )

    def g_copy(d):
        cut = pl.ds(0, HALO)
        return remote(norm.at[cut], norm.at[cut], g_sem.at[0], g_sem.at[1], {"tp": d})

    def halo_relay():
        @pl.when(last_tp & (sp > 0))
        def _():
            h_copy().wait_recv()
            for d in range(T - 1):
                g_copy(d).start()

    def halo_ready():
        @pl.when((tp < T - 1) & (sp > 0))
        def _():
            g_copy(0).wait_recv()

        @pl.when(sp == 0)
        def _():
            norm[0:HALO, :] = jnp.zeros((HALO, width), bf16)

    def project(acc, source, buf, slots, owner, fresh=False):
        for c in range(0, acc.shape[1], 256):
            total = None
            for slot in slots:
                at = pl.multiple_of(owner(slot) * kdim, kdim)
                term = jnp.dot(
                    source[:, pl.ds(at, kdim)], buf[slot, :, c : c + 256],
                    preferred_element_type=f32,
                )
                total = term if total is None else total + term
            if fresh:
                acc[:, c : c + 256] = total
            else:
                acc[:, c : c + 256] += total

    def column(ref):
        index = lax.broadcasted_iota(jnp.int32, (heads, 1), 0)
        full = jnp.full((heads, 1), ref[0], f32)
        for h in range(1, heads):
            full = jnp.where(index == h, ref[h], full)
        return full

    lane = lax.broadcasted_iota(jnp.int32, (1, heads_width), 1)

    def spread(columns):
        full = jnp.broadcast_to(columns[:, 0:1], (columns.shape[0], heads_width))
        for h in range(1, heads):
            full = jnp.where(lane >= h * HEAD_DIM, columns[:, h : h + 1], full)
        return full

    def taps(u, weights):
        k_taps = weights.shape[0]
        w = weights[...].astype(f32)
        total = w[k_taps - 1 : k_taps] * u[8:]
        for k in range(k_taps - 1):
            total = total + w[k : k + 1] * pltpu.roll(u, k_taps - 1 - k, 0)[8:]
        return total

    blocks = length // CHUNK

    def spans(b):
        t0 = b * CHUNK
        return (
            slice(t0, t0 + CHUNK),
            slice(t0 + HALO, t0 + HALO + CHUNK),
            slice(t0 + HALO - 8, t0 + HALO + CHUNK),
        )

    def field(acc, begin, size, span):
        return acc[span, begin : begin + size].astype(bf16).astype(f32)

    def conv_step(ring, s):
        slots = (0,) if s == 0 else (n - 1,) if s == n // 2 else (ring_slot(0, s), ring_slot(1, s))
        for slot in slots:
            ring.need(slot)
        project(acc_c, norm, cbuf, slots, ring_owner, s == 0)

    def conv_mix():
        for b in range(blocks):
            span, own, take = spans(b)
            product = field(acc_c, cdim, cdim, take) * field(acc_c, 2 * cdim, cdim, take)
            mix = field(acc_c, 0, cdim, own) * taps(product, taps_conv)
            apart[span, 0:cdim] = mix.astype(bf16)

    def m_copy(b):
        cut = pl.ds(b * CHUNK, CHUNK)
        return remote(
            mbuf.at[cut], apart.at[cut, pl.ds(cdim, heads_width)], ms_sem, mr_sem.at[b],
            {"sp": mate},
        )

    def x_copy():
        return remote(st_send, st_recv, x_sem.at[0], x_sem.at[1], {"sp": side})

    def e_copy():
        return remote(e_send, e_recv, e_sem.at[0], e_sem.at[1], {"sp": cross})

    def inner_part():
        sl = Slots(sbuf, PIECES_S, sr_sem)
        gl = Slots(gbuf, PIECES_G, gr_sem)
        ol = Slots(obuf, PIECES_O, or_sem)
        ring = Ring()
        forwards = [(link, 1, q) for link in (0, 1) for q in range(PIECES_C)]
        step_two = sorted((q + 2.5 * link, link, q) for link in (0, 1) for q in range(PIECES_C))
        forwards += [(link, 2, q) for _, link, q in step_two]
        for q in range(PIECES_C // 2):
            forwards += [(0, 3, q), (1, 3, PIECES_C // 2 + q)]
        done = [0]

        def pump(count):
            for _ in range(count):
                if done[0] < len(forwards):
                    ring.forward(*forwards[done[0]])
                    done[0] += 1

        r_id = lax.broadcasted_iota(jnp.int32, (CHUNK, CHUNK), 0)
        c_id = lax.broadcasted_iota(jnp.int32, (CHUNK, CHUNK), 1)
        causal = r_id >= c_id
        lower = causal.astype(f32)
        eye = (r_id == c_id).astype(f32)

        for q in range(PIECES_C):
            ring.forward(0, 0, q)
        for q in range(PIECES_S):
            sl.arrive(1, q, ss_sem, mate)
            sl.send(1, 3, q, ss_sem, cross)
            sl.send(1, 5, q, ss_sem, side)
        for q in range(PIECES_S):
            sl.arrive(2, q, ss_sem, mate)
            sl.send(2, 6, q, ss_sem, side)
        for q in range(PIECES_C):
            ring.forward(1, 0, q)
        t_relay(0)
        landed("g")
        for q in range(PIECES_G):
            gl.send(0, 2, q, gs_sem, cross)
        landed("o")
        for q in range(PIECES_O):
            ol.send(0, 2, q, os_sem, cross)
            ol.send(0, 1, q, os_sem, mate)
        for q in range(PIECES_S):
            sl.arrive(3, q, ss_sem, mate)
            sl.send(3, 7, q, ss_sem, side)
        for q in range(PIECES_G):
            gl.send(0, 4, q, gs_sem, side)
        halo_relay()
        for q in range(PIECES_U):
            v_copy(q).wait_recv()
            u_start(q)
            if q == 0:
                for p in range(1, PIECES_T):
                    t_relay(p)
            if q > 0:
                pump(1)
                u_relay(q - 1)
        pump(1)
        t_finish()
        halo_ready()
        for q in range(PIECES_G):
            gl.arrive(1, q, gs_sem, mate)
            gl.send(1, 3, q, gs_sem, cross)
            gl.send(1, 5, q, gs_sem, side)
        u_relay(PIECES_U - 1)
        for slot in range(1, n):
            for q in range(PIECES_S):
                sl.arrive(slot, q, ss_sem, mate)
        project(acc_s.at[0], norm, sbuf, range(0, 4), plane_owner, True)
        project(acc_s.at[0], norm, sbuf, range(4, 8), plane_owner)
        for q in range(PIECES_G):
            gl.arrive(2, q, gs_sem, mate)
            gl.send(2, 6, q, gs_sem, side)
        k_copy().wait_recv()
        u_finish()
        project(acc_s.at[1], norm2, sbuf, range(0, 4), plane_owner, True)
        project(acc_s.at[1], norm2, sbuf, range(4, 8), plane_owner)
        pump(2)
        landed("v")
        l_copy().wait_recv()

        logs_of = []
        for k, (source, spike) in enumerate(((norm, spikes), (norm2, spikes2))):
            step = jax.nn.softplus(nt(step_w[...], source[HALO:, :]) + column(bias))
            logs = -step * jnp.exp(column(rate)) + spike[...]
            logs_of.append(logs)
            running = jnp.zeros((STATE, heads_width), f32)
            before = jnp.zeros((1, heads_width), f32)
            acc = acc_s.at[k]
            for b in range(blocks):
                span, own, take = spans(b)
                xs = silu(taps(field(acc, 0, cdim, take), taps_in))
                wr = silu(taps(field(acc, cdim, STATE, take), taps_wr))
                rd = silu(taps(field(acc, cdim + STATE, STATE, take), taps_rd))
                cum = nt(lower, logs[:, span], highest)
                steps = nt(eye, step[:, span], highest)
                cum_wide = spread(cum)
                weighted = xs * spread(steps)
                xbuf[k, span, :] = xs
                mixbuf[k, span, :] = weighted.astype(bf16)
                wrbuf[k, span, :] = wr.astype(bf16)
                rdbuf[k, span, :] = rd.astype(bf16)
                cumbuf[k, span, :] = cum_wide
                last = cum_wide[CHUNK - 1 : CHUNK]
                scaled = (weighted * jnp.exp(last - cum_wide)).astype(bf16)
                stbuf[k, b] = running
                running = running * jnp.exp(last) + jnp.dot(
                    wr.T.astype(bf16), scaled, preferred_element_type=f32
                )
                before = before + last
                if k == 0 and b % 2 == 1:
                    pump(1)
            runbuf[k] = running
            decbuf[k] = jnp.exp(before)
            st_send[k, 0:STATE, :] = running.astype(bf16)
            st_send[k, STATE:, :] = jnp.broadcast_to(
                jnp.exp(before), (HALO, heads_width)
            ).astype(bf16)
            if k == 0:
                for q in range(PIECES_O):
                    ol.arrive(2, q, os_sem, mate)
                    ol.send(2, 2, q, os_sem, mate)

        x_copy().start()
        for q in range(PIECES_G):
            gl.arrive(3, q, gs_sem, mate)
            gl.send(3, 7, q, gs_sem, side)

        def within(k, b):
            span, _, _ = spans(b)
            scores = nt(rdbuf[k, span, :], wrbuf[k, span, :])
            cum_t = lax.dot_general(
                logs_of[k][:, span], lower, (((1,), (1,)), ((), ())),
                preferred_element_type=f32, precision=highest,
            )
            for pair in range(0, heads_width, 128):
                both = []
                for h in range(pair // HEAD_DIM, (pair + 128) // HEAD_DIM):
                    diff = cumbuf[k, span, h * HEAD_DIM : h * HEAD_DIM + 1] - cum_t[h : h + 1, :]
                    damped = scores * jnp.exp(jnp.where(causal, diff, -1e30))
                    both.append(
                        jnp.dot(
                            damped.astype(bf16), mixbuf[k, span, pair : pair + 128],
                            preferred_element_type=f32,
                        )
                    )
                first = lax.broadcasted_iota(jnp.int32, (1, 128), 1) < HEAD_DIM
                ybuf[k, span, pair : pair + 128] = jnp.where(first, both[0], both[1])

        for b in range(blocks):
            within(1, b)
        pump(1)
        for slot in (0, 2):
            for q in range(PIECES_O):
                ol.send(slot, 4 + slot, q, ox_sem, side)
        for b in range(blocks):
            within(0, b)
        pump(1)
        x_copy().wait_recv()
        second = jnp.broadcast_to(x, (1, heads_width)) == 1
        pair, pair_decay, other, first_decay = [], [], [], []
        for k in range(2):
            theirs = st_recv[k, 0:STATE, :].astype(f32)
            their_decay = st_recv[k, STATE : STATE + 1, :].astype(f32)
            pair.append(
                jnp.where(
                    second, theirs * decbuf[k] + runbuf[k], runbuf[k] * their_decay + theirs
                )
            )
            pair_decay.append(decbuf[k] * their_decay)
            other.append(jnp.where(second, theirs, jnp.zeros_like(theirs)))
            first_decay.append(jnp.where(second, their_decay, jnp.ones_like(their_decay)))

        @pl.when(upper == 0)
        def _():
            e_send[...] = (pair[1] * pair_decay[0] + pair[0]).astype(bf16)
            e_copy().start()
            runbuf[1] = other[1]
            runbuf[0] = other[0] + first_decay[0] * pair[1]

        @pl.when(upper == 1)
        def _():
            runbuf[0] = other[0]
            runbuf[1] = other[1] + first_decay[1] * pair[0]
            decbuf[0] = first_decay[0]
            decbuf[1] = first_decay[1] * pair_decay[0]

        pump(2)
        for q in range(PIECES_O):
            ol.arrive(1, q, os_sem, mate)
            ol.send(1, 3, q, os_sem, cross)
            ol.send(1, 5, q, ox_sem, side)
        pump(1)
        for slot in range(1, n - 1):
            for q in range(PIECES_G):
                gl.arrive(slot, q, gs_sem, mate)
        for k, source in enumerate((norm, norm2)):
            project(acc_g.at[k], source, gbuf, range(n - 1), plane_owner, True)
            pump(1)
        conv_step(ring, 0)
        pump(1)
        for q in range(PIECES_G):
            gl.arrive(n - 1, q, gs_sem, mate)
        for k, source in enumerate((norm, norm2)):
            project(acc_g.at[k], source, gbuf, (n - 1,), plane_owner)

        @pl.when(upper == 1)
        def _():
            e_copy().wait_recv()
            entering = e_recv[...].astype(f32)
            for k in range(2):
                runbuf[k] = runbuf[k] + decbuf[k] * entering

        group = (
            lax.div(lax.broadcasted_iota(jnp.int32, (heads_width, heads_width), 0), HEAD_DIM)
            == lax.div(lax.broadcasted_iota(jnp.int32, (heads_width, heads_width), 1), HEAD_DIM)
        ).astype(bf16)
        direct_wide = jnp.full((1, heads_width), direct[0], f32)
        for h in range(1, heads):
            direct_wide = jnp.where(lane >= h * HEAD_DIM, direct[h], direct_wide)

        for k in (1, 0):
            so_far = jnp.zeros((1, heads_width), f32)
            for b in range(blocks):
                span, own, _ = spans(b)
                cum_wide = cumbuf[k, span, :]
                entering = (stbuf[k, b] + jnp.exp(so_far) * runbuf[k]).astype(bf16)
                so_far = so_far + cum_wide[CHUNK - 1 : CHUNK]
                head_out = (
                    ybuf[k, span, :]
                    + jnp.dot(rdbuf[k, span, :], entering, preferred_element_type=f32)
                    * jnp.exp(cum_wide)
                    + direct_wide * xbuf[k, span, :]
                )
                gated = head_out * silu(field(acc_g.at[k], 0, cdim, own))
                square = jnp.dot((gated * gated).astype(bf16), group, preferred_element_type=f32)
                normalized = gated * lax.rsqrt(square * (1.0 / HEAD_DIM) + epsilon)
                result = (
                    normalized * hscale[...].astype(f32).reshape(1, heads_width)
                ).astype(bf16)
                if k == 1:
                    mbuf[span, :] = result
                    m_copy(b).start()
                else:
                    apart[span, cdim:] = result
        pump(1)
        conv_step(ring, 1)
        pump(1)
        conv_step(ring, 2)
        pump(len(forwards))
        for q in range(PIECES_O):
            ol.arrive(3, q, os_sem, mate)
            ol.send(3, 3, q, os_sem, mate)
            ol.send(3, 7, q, ox_sem, side)
        conv_step(ring, 3)
        conv_step(ring, n // 2)
        conv_mix()

    def blocks_sent(buf, count, sem):
        every = buf.at[pl.ds(0, count)]
        remote(every, every, sem, cr_sem.at[0], {"sp": mate}).wait_send()

    def end_part():
        gl = Slots(gbuf, PIECES_G, gr_sem)
        ol = Slots(obuf, PIECES_O, or_sem)
        ring = Ring()
        for q in range(PIECES_U):
            v_copy(q).start()
        for q in range(PIECES_C):
            ring.forward(1, 0, q)
        landed("v")
        l_copy().start()
        landed("g")
        for q in range(PIECES_G):
            gl.send(0, 1, q, gs_sem, mate)
        t_relay(0)
        for q in range(PIECES_C):
            ring.forward(1, 1, q)
        for q in range(1, PIECES_T):
            t_relay(q)
        halo_relay()
        halo_ready()
        k_copy().start()
        landed("o")
        for q in range(PIECES_C):
            ring.forward(0, 0, q)
        for q in range(PIECES_O):
            ol.send(0, 1, q, os_sem, mate)
        for q in range(PIECES_O):
            ol.send(0, 4, q, ox_sem, side)
        for q in range(PIECES_C):
            ring.forward(0, 1, q)
        for q in range(PIECES_O):
            ol.arrive(1, q, os_sem, mate)
            ol.send(1, 5, q, ox_sem, side)
        for q in range(PIECES_C):
            ring.forward(0, 2, q)
        t_finish()
        conv_step(ring, 0)
        conv_step(ring, 1)
        for q in range(PIECES_C):
            ring.forward(1, 2, q)
        for q in range(PIECES_C // 2):
            ring.forward(0, 3, q)
        conv_step(ring, 2)
        for q in range(PIECES_O):
            ol.arrive(2, q, os_sem, mate)
            ol.send(2, 6, q, ox_sem, side)
        for q in range(PIECES_C // 2, PIECES_C):
            ring.forward(1, 3, q)
        conv_step(ring, 3)
        for q in range(PIECES_O):
            ol.arrive(3, q, os_sem, mate)
            ol.send(3, 7, q, ox_sem, side)
        conv_step(ring, n // 2)
        conv_mix()
        for b in range(blocks):
            m_copy(b).wait_recv()

    landed("s")
    pl.semaphore_wait(barrier, n - 1 + T - 1)
    first_s = Slots(sbuf, PIECES_S, sr_sem)

    @pl.when(is_inner)
    def _():
        for q in range(PIECES_S):
            first_s.send(0, 2, q, ss_sem, cross)
            first_s.send(0, 4, q, ss_sem, side)

    @pl.when(z == end_z)
    def _():
        for q in range(PIECES_S):
            first_s.send(0, 1, q, ss_sem, mate)

    landed("t")
    value = tokens[...].astype(f32)
    value = value * lax.rsqrt(jnp.mean(value * value, axis=1, keepdims=True) + epsilon)
    norm[pl.ds(own_at, rows), :] = (
        value * in_scale[...].astype(f32).reshape(1, width)
    ).astype(bf16)
    for q in range(PIECES_T):
        t_start(q)

    @pl.when(last_tp & (sp < n - 1))
    def _():
        h_copy().start()

    landed("c")

    @pl.when(is_inner)
    def _():
        inner_part()

    @pl.when(z == end_z)
    def _():
        end_part()

    def block_rows(y, c):
        return pl.ds(pl.multiple_of((y * CORES + c) * rows, rows), rows)

    def columns_of(slot):
        return pl.ds(pl.multiple_of(plane_owner(slot) * ocols, ocols), ocols)

    def r1_copy(d, s):
        return remote(
            part.at[s, block_rows(lax.rem(chip + d, Y), 1 - core)], r1.at[s, d], r1s_sem,
            r1r_sem.at[s], {"tp": partner},
        )

    def r2_copy(d, s):
        return remote(
            p2.at[d - 1, s], far.at[d - 1, :, columns_of(s)], r2s_sem, r2r_sem,
            {"tp": lax.rem(chip + d, Y) * CORES + core},
        )

    def near_copy(s):
        return pltpu.make_async_copy(nbuf.at[s], near.at[:, columns_of(s)], near_sem)

    o_last = Slots(obuf, PIECES_O, or_sem)

    def project_out(s):
        if s >= 4:
            for q in range(PIECES_O):
                o_last.arrive(s, q, os_sem, mate)
        part[s] = jnp.dot(apart[...], obuf[s], preferred_element_type=f32).astype(bf16)
        for d in range(1, Y):
            r1_copy(d, s).start()
        r1_copy(0, s).start()

    def reduce(s):
        remote(r1.at[s], r1.at[s], r1s_sem, r1r_sem.at[s], {"tp": partner}).wait_recv()
        for d in range(1, Y):
            mine = part[s, block_rows(lax.rem(chip + d, Y), core), :]
            p2[d - 1, s] = (mine.astype(f32) + r1[s, d].astype(f32)).astype(bf16)
            r2_copy(d, s).start()
        mine = part[s, block_rows(chip, core), :]
        nbuf[s] = (mine.astype(f32) + r1[s, 0].astype(f32)).astype(bf16)
        near_copy(s).start()

    order = [0, 1, 2, 4, 5, 6, 3, 7]
    previous = None
    for slot in order:
        if slot == order[-1]:
            reduce(previous)
        project_out(slot)
        if slot != order[-1] and previous is not None:
            reduce(previous)
        previous = slot
    reduce(previous)

    @pl.when(is_inner)
    def _():
        x_copy().wait_send()

        @pl.when(upper == 0)
        def _():
            e_copy().wait_send()

        blocks_sent(sbuf, 6, ss_sem)
        blocks_sent(gbuf, 6, gs_sem)
        blocks_sent(obuf, 5, os_sem)
        remote(mbuf, mbuf, ms_sem, mr_sem.at[0], {"sp": mate}).wait_send()
        remote(
            norm2.at[pl.ds(0, Y * rows)], norm2.at[pl.ds(0, Y * rows)], t2s_sem,
            t2r_sem.at[0, 0], {"tp": partner},
        ).wait_send()
        remote(
            norm2.at[pl.ds(0, (Y - 1) * rows)], norm2.at[pl.ds(0, (Y - 1) * rows)], u2s_sem,
            u2r_sem.at[0, 0], {"tp": partner},
        ).wait_send()

    @pl.when(z == end_z)
    def _():
        blocks_sent(sbuf, 1, ss_sem)
        blocks_sent(gbuf, 1, gs_sem)
        blocks_sent(obuf, 1, os_sem)
        remote(
            norm.at[pl.ds(0, rows)], norm.at[pl.ds(0, rows)], vs_sem, vr_sem.at[0], {"sp": mate}
        ).wait_send()
        k_copy().wait_send()
        l_copy().wait_send()

    blocks_sent(cbuf, n - 1, cs_sem)
    blocks_sent(obuf, 4, ox_sem)
    remote(
        norm.at[pl.ds(0, Y * rows)], norm.at[pl.ds(0, Y * rows)], ts_sem, tr_sem.at[0, 0],
        {"tp": partner},
    ).wait_send()
    remote(
        norm.at[pl.ds(0, (Y - 1) * rows)], norm.at[pl.ds(0, (Y - 1) * rows)], us_sem,
        ur_sem.at[0, 0], {"tp": partner},
    ).wait_send()

    @pl.when(last_tp & (sp < n - 1))
    def _():
        h_copy().wait_send()

    @pl.when(last_tp & (sp > 0))
    def _():
        cut = pl.ds(0, (T - 1) * HALO)
        remote(norm.at[cut], norm.at[cut], g_sem.at[0], g_sem.at[1], {"tp": partner}).wait_send()

    remote(r1, r1, r1s_sem, r1r_sem.at[0], {"tp": partner}).wait_send()
    remote(p2, p2, r2s_sem, r2r_sem, {"tp": partner}).wait_send()
    pltpu.make_async_copy(far.at[0], near, near_sem).wait()
    remote(far, far, r2s_sem, r2r_sem, {"tp": partner}).wait_recv()


def shifted(shard, axis, by):
    devices = lax.axis_size(axis)
    pairs = [(i, i + by) for i in range(devices) if 0 <= i + by < devices]
    return lax.ppermute(shard, axis, pairs)


def prefix(shard, axis, combine, identity):
    devices, index = (lax.axis_size(axis), lax.axis_index(axis))
    everything = jax.tree.map(
        lambda part, kind: lax.all_gather(part.astype(kind), axis),
        shard,
        (jnp.bfloat16, jnp.bfloat16),
    )
    start = jax.tree.map(
        lambda part, zero: jnp.broadcast_to(jnp.asarray(zero, part.dtype), part.shape),
        shard,
        identity,
    )

    def turn(k, before):
        reached = k < index
        new = combine(
            before, jax.tree.map(lambda part, own: part[k].astype(own.dtype), everything, shard)
        )
        return jax.tree.map(lambda a, b: jnp.where(reached, a, b), new, before)

    return lax.fori_loop(0, devices, turn, start)


def causal_taps(values, rim_rows, tap_weights):
    tap_count = tap_weights.shape[0]
    length = values.shape[0]
    padded = jnp.concatenate([rim_rows, values], axis=0)
    running = tap_weights[0] * padded[0:length]
    for offset in range(1, tap_count):
        running = running + tap_weights[offset] * padded[offset : offset + length]
    return running


def combine_states(earlier, later):
    return (earlier[0] * later[0], earlier[1] * later[0][:, None, None] + later[1])


def plain_path(
    tokens,
    input_norm_scale,
    outer_gate_weight,
    inner_gate_weight,
    value_weight_matrix,
    output_gate_weight,
    state_input_weight,
    write_key_weight,
    read_key_weight,
    step_size_weight,
    gated_conv_weight,
    input_conv_weight,
    write_conv_weight,
    read_conv_weight,
    step_size_bias,
    log_decay_rate,
    decay_spikes,
    direct_path_weight,
    head_norm_scale,
    conv_output_weight,
    state_output_weight,
):
    token_rows = tokens.astype(jnp.float32)
    scaled = token_rows * lax.rsqrt(
        jnp.mean(token_rows * token_rows, axis=1, keepdims=True) + epsilon
    )
    normed_own = (scaled * input_norm_scale.astype(jnp.float32)).astype(jnp.bfloat16)
    normed = lax.all_gather(normed_own, "tp", axis=0, tiled=True)
    length = normed.shape[0]
    pieces = (
        lax.all_gather(outer_gate_weight, "sp", axis=0, tiled=True),
        lax.all_gather(inner_gate_weight, "sp", axis=0, tiled=True),
        lax.all_gather(value_weight_matrix, "sp", axis=0, tiled=True),
        lax.all_gather(output_gate_weight, "sp", axis=0, tiled=True),
        lax.all_gather(state_input_weight, "sp", axis=0, tiled=True),
        lax.all_gather(write_key_weight, "sp", axis=0, tiled=True),
        lax.all_gather(read_key_weight, "sp", axis=0, tiled=True),
    )
    projected = tuple(
        (jnp.dot(normed, weight_rows, preferred_element_type=jnp.float32) for weight_rows in pieces)
    )
    outer_gate, inner_gate, conv_input, out_gate, state_input, write_keys, read_keys = [
        member.astype(jnp.bfloat16) for member in projected
    ]
    step_raw = jnp.dot(normed, step_size_weight, preferred_element_type=jnp.float32)
    short_rim = gated_conv_weight.shape[0] - 1
    state_rim = input_conv_weight.shape[0] - 1
    rim_rows = shifted(
        (
            inner_gate[length - short_rim :],
            conv_input[length - short_rim :],
            state_input[length - state_rim :],
            write_keys[length - state_rim :],
            read_keys[length - state_rim :],
        ),
        "sp",
        1,
    )
    product = inner_gate.astype(jnp.float32) * conv_input.astype(jnp.float32)
    rim_product = rim_rows[0].astype(jnp.float32) * rim_rows[1].astype(jnp.float32)
    mixer_part = (
        outer_gate.astype(jnp.float32)
        * causal_taps(product, rim_product, gated_conv_weight.astype(jnp.float32))
    ).astype(jnp.bfloat16)
    seq_input = jax.nn.silu(
        causal_taps(
            state_input.astype(jnp.float32),
            rim_rows[2].astype(jnp.float32),
            input_conv_weight.astype(jnp.float32),
        )
    )
    seq_write = jax.nn.silu(
        causal_taps(
            write_keys.astype(jnp.float32),
            rim_rows[3].astype(jnp.float32),
            write_conv_weight.astype(jnp.float32),
        )
    )
    seq_read = jax.nn.silu(
        causal_taps(
            read_keys.astype(jnp.float32),
            rim_rows[4].astype(jnp.float32),
            read_conv_weight.astype(jnp.float32),
        )
    )
    discrete_step = jax.nn.softplus(step_raw + step_size_bias[None, :])
    step_logarithm = discrete_step * (-jnp.exp(log_decay_rate))[None, :] + decay_spikes.T
    heads_here = discrete_step.shape[1]
    groups_here = seq_write.shape[1] // STATE
    per_group = heads_here // groups_here
    blocks = length // PLAIN_BLOCK
    input_blocks = seq_input.reshape(blocks, PLAIN_BLOCK, heads_here, HEAD_DIM)
    weighted = input_blocks * discrete_step.reshape(blocks, PLAIN_BLOCK, heads_here, 1)
    write_blocks = jnp.repeat(
        seq_write.reshape(blocks, PLAIN_BLOCK, groups_here, STATE), per_group, axis=2
    )
    read_blocks = jnp.repeat(seq_read.reshape(blocks, PLAIN_BLOCK, groups_here, STATE), per_group, axis=2)
    cumulative = jnp.cumsum(step_logarithm.reshape(blocks, PLAIN_BLOCK, heads_here), axis=1)
    causal = lax.broadcasted_iota(jnp.int32, (PLAIN_BLOCK, PLAIN_BLOCK), 0) >= lax.broadcasted_iota(
        jnp.int32, (PLAIN_BLOCK, PLAIN_BLOCK), 1
    )
    scores = jnp.einsum("clhm,cshm->clsh", read_blocks, write_blocks, precision=highest)
    damping = jnp.exp(
        jnp.where(
            causal[None, :, :, None],
            cumulative[:, :, None, :] - cumulative[:, None, :, :],
            -jnp.inf,
        )
    )
    within_block = jnp.einsum("clsh,cshp->clhp", scores * damping, weighted, precision=highest)
    to_end = jnp.exp(cumulative[:, -1:, :] - cumulative)
    block_states = jnp.einsum(
        "cshm,cshp->chpm", write_blocks * to_end[..., None], weighted, precision=highest
    )
    block_logs = cumulative[:, -1, :]

    def advance(carried_state, inputs):
        contribution, block_log = inputs
        return (carried_state * jnp.exp(block_log)[:, None, None] + contribution, carried_state)

    own_total, own_before = lax.scan(
        advance, jnp.zeros(block_states.shape[1:], jnp.float32), (block_states, block_logs)
    )
    total_log = jnp.sum(block_logs, axis=0)
    arriving = prefix(
        (jnp.exp(total_log), own_total),
        "sp",
        combine_states,
        (jnp.ones_like(total_log), jnp.zeros_like(own_total)),
    )[1]
    before_logs = jnp.cumsum(block_logs, axis=0) - block_logs
    entering = own_before + jnp.exp(before_logs)[:, :, None, None] * arriving[None]
    from_before = (
        jnp.einsum("clhm,chpm->clhp", read_blocks, entering, precision=highest)
        * jnp.exp(cumulative)[..., None]
    )
    head_out = within_block + from_before + direct_path_weight[None, None, :, None] * input_blocks
    head_out = head_out.reshape(length, heads_here * HEAD_DIM)
    gated_heads = (head_out * jax.nn.silu(out_gate.astype(jnp.float32))).reshape(
        length, heads_here, HEAD_DIM
    )
    normalized = gated_heads * lax.rsqrt(
        jnp.mean(gated_heads * gated_heads, axis=2, keepdims=True) + epsilon
    )
    state_part = (
        normalized.reshape(length, heads_here * HEAD_DIM) * head_norm_scale.astype(jnp.float32)
    ).astype(jnp.bfloat16)
    wide_mixer, wide_state = (
        lax.all_gather(conv_output_weight, "sp", axis=1, tiled=True),
        lax.all_gather(state_output_weight, "sp", axis=1, tiled=True),
    )
    return lax.psum_scatter(
        (
            jnp.dot(mixer_part, wide_mixer, preferred_element_type=jnp.float32)
            + jnp.dot(state_part, wide_state, preferred_element_type=jnp.float32)
        ).astype(jnp.bfloat16),
        "tp",
        scatter_dimension=0,
        tiled=True,
    )


def per_device(
    tokens, input_norm_scale, outer_gate_weight, inner_gate_weight, value_weight_matrix,
    output_gate_weight, state_input_weight, write_key_weight, read_key_weight, step_size_weight,
    gated_conv_weight, input_conv_weight, write_conv_weight, read_conv_weight, step_size_bias,
    log_decay_rate, decay_spikes, direct_path_weight, head_norm_scale, conv_output_weight,
    state_output_weight,
):
    n, T = lax.axis_size("sp"), lax.axis_size("tp")
    rows, width = tokens.shape
    kdim, cdim = outer_gate_weight.shape
    heads = step_size_bias.shape[0]
    hw = heads * HEAD_DIM
    length = rows * T
    ocols = conv_output_weight.shape[1]
    if (
        kdim % 128 or ocols % 256 or n % 2 or n != 2 * PLANES or T % CORES
        or T < 2 * CORES
        or write_key_weight.shape[1] != STATE
    ):
        return plain_path(
            tokens, input_norm_scale, outer_gate_weight, inner_gate_weight,
            value_weight_matrix, output_gate_weight, state_input_weight, write_key_weight,
            read_key_weight, step_size_weight, gated_conv_weight, input_conv_weight,
            write_conv_weight, read_conv_weight, step_size_bias, log_decay_rate, decay_spikes,
            direct_path_weight, head_norm_scale, conv_output_weight, state_output_weight,
        )
    Y = T // CORES
    sm = pl.BlockSpec(memory_space=pltpu.SMEM)
    hbm = pl.BlockSpec(memory_space=pl.ANY)
    dma = pltpu.SemaphoreType.DMA
    s_cols, blocks = cdim + 2 * STATE, length // CHUNK

    def like(array):
        return pltpu.VMEM(array.shape, array.dtype)

    step_t = step_size_weight.T
    near, far = pl.pallas_call(
        functools.partial(kernel, n, T),
        out_shape=(
            jax.ShapeDtypeStruct((rows, width), bf16),
            jax.ShapeDtypeStruct((Y - 1, rows, width), bf16),
        ),
        in_specs=[hbm] * 14 + [sm] * 2 + [hbm, sm, hbm] + [hbm] * 2,
        out_specs=(hbm, hbm),
        scratch_shapes=[
            like(tokens),
            like(input_norm_scale),
            like(step_t),
            like(gated_conv_weight),
            like(input_conv_weight),
            like(write_conv_weight),
            like(read_conv_weight),
            like(decay_spikes),
            like(head_norm_scale),
            pltpu.VMEM((n, kdim, s_cols), bf16),
            pltpu.VMEM((n, kdim, cdim), bf16),
            pltpu.VMEM((n, kdim, 3 * cdim), bf16),
            pltpu.VMEM((n, cdim + hw, ocols), bf16),
            pltpu.VMEM((HALO + length, width), bf16),
            pltpu.VMEM((HALO + length, width), bf16),
            like(decay_spikes),
            pltpu.VMEM((2, HALO + length, s_cols), f32),
            pltpu.VMEM((2, HALO + length, cdim), f32),
            pltpu.VMEM((HALO + length, 3 * cdim), f32),
            pltpu.VMEM((2, length, hw), bf16),
            pltpu.VMEM((2, length, hw), f32),
            pltpu.VMEM((2, length, STATE), bf16),
            pltpu.VMEM((2, length, STATE), bf16),
            pltpu.VMEM((2, length, hw), f32),
            pltpu.VMEM((2, length, hw), f32),
            pltpu.VMEM((2, blocks, STATE, hw), f32),
            pltpu.VMEM((2, STATE, hw), f32),
            pltpu.VMEM((2, 1, hw), f32),
            pltpu.VMEM((2, STATE + HALO, hw), bf16),
            pltpu.VMEM((2, STATE + HALO, hw), bf16),
            pltpu.VMEM((STATE, hw), bf16),
            pltpu.VMEM((STATE, hw), bf16),
            pltpu.VMEM((length, hw), bf16),
            pltpu.VMEM((length, cdim + hw), bf16),
            pltpu.VMEM((n, length, ocols), bf16),
            pltpu.VMEM((n, Y, rows, ocols), bf16),
            pltpu.VMEM((Y - 1, n, rows, ocols), bf16),
            pltpu.VMEM((n, rows, ocols), bf16),
            dma((13,)),
            dma,
            dma(((n - 1) * PIECES_S,)),
            dma,
            dma(((n - 1) * PIECES_G,)),
            dma,
            dma(((n - 1) * PIECES_C,)),
            dma,
            dma,
            dma(((n - 1) * PIECES_O,)),
            dma,
            dma((Y, PIECES_T)),
            dma,
            dma((Y, PIECES_T)),
            dma,
            dma((PIECES_U,)),
            dma,
            dma((Y, PIECES_U)),
            dma,
            dma((Y, PIECES_U)),
            dma((2,)),
            dma((2,)),
            dma((2,)),
            dma((2,)),
            dma((2,)),
            dma((2,)),
            dma,
            dma((blocks,)),
            dma,
            dma((n,)),
            dma,
            dma,
            dma,
        ],
        compiler_params=pltpu.CompilerParams(
            collective_id=0, has_side_effects=True, vmem_limit_bytes=62 * 1024 * 1024
        ),
    )(
        tokens, input_norm_scale, outer_gate_weight, inner_gate_weight,
        value_weight_matrix, output_gate_weight, state_input_weight, write_key_weight,
        read_key_weight, step_t, gated_conv_weight, input_conv_weight, write_conv_weight,
        read_conv_weight, step_size_bias, log_decay_rate, decay_spikes, direct_path_weight,
        head_norm_scale,
        conv_output_weight, state_output_weight,
    )
    total = near.astype(f32)
    for d in range(Y - 1):
        total = total + far[d].astype(f32)
    return total.astype(bf16)


def solution(mesh):
    placed = (
        (P(("sp", "tp"), None), P())
        + (P("sp", "tp"),) * 7
        + (P(None, "tp"),) * 5
        + (P("tp"), P("tp"), P("tp", "sp"), P("tp"), P("tp"), P("tp", "sp"), P("tp", "sp"))
    )
    return jax.shard_map(
        per_device, mesh=mesh, in_specs=placed, out_specs=P(("sp", "tp"), None), check_vma=False
    )
```

```python
import functools

import jax
import jax.numpy as jnp
from jax import lax
from jax.experimental import pallas as pl
from jax.experimental.pallas import tpu as pltpu
from jax.sharding import PartitionSpec as P

HEAD_DIM = 64
STATE = 128
PLAIN_BLOCK = 64
CHUNK = 128
HALO = 16
PIECES_S = 2
PIECES_G = 1
PIECES_C = 4
PIECES_O = 2
PIECES_T = 2
PIECES_U = 4
PLANES = 4
CORES = 2
epsilon = 1e-05
highest = lax.Precision.HIGHEST
f32 = jnp.float32
bf16 = jnp.bfloat16
MESH = pl.DeviceIdType.MESH


def nt(a, b, precision=None):
    return lax.dot_general(
        a, b, (((1,), (1,)), ((), ())), preferred_element_type=f32, precision=precision
    )


def silu(v):
    return v / (1.0 + jnp.exp(-v))


def remote(src, dst, send, recv, device):
    return pltpu.make_async_remote_copy(
        src_ref=src, dst_ref=dst, send_sem=send, recv_sem=recv, device_id=device,
        device_id_type=MESH,
    )


class Slots:
    def __init__(self, buf, pieces, recv):
        self.buf, self.pieces, self.recv = buf, pieces, recv
        self.rows = buf.shape[1] // pieces
        self.waited = set()

    def piece(self, slot, q):
        return self.buf.at[slot, pl.ds(q * self.rows, self.rows)]

    def send(self, src, dst, q, sem, device):
        remote(
            self.piece(src, q), self.piece(dst, q), sem,
            self.recv.at[(dst - 1) * self.pieces + q], {"sp": device},
        ).start()

    def arrive(self, slot, q, sem, device):
        if (slot, q) not in self.waited:
            self.waited.add((slot, q))
            remote(
                self.piece(slot, q), self.piece(slot, q), sem,
                self.recv.at[(slot - 1) * self.pieces + q], {"sp": device},
            ).wait_recv()


def kernel(
    n,
    T,
    tokens_h, in_scale_h, w_outer, w_inner, w_value, w_ogate, w_state, w_write, w_read,
    step_w_h, taps_conv_h, taps_in_h, taps_wr_h, taps_rd_h,
    bias_h, rate_h, spikes_h, direct_h, hscale_h, o_conv, o_state,
    near, far,
    tokens, in_scale, step_w, taps_conv, taps_in, taps_wr, taps_rd, spikes, hscale,
    bias, rate, direct, sbuf, gbuf, cbuf, obuf, norm, norm2, spikes2, acc_s, acc_g, acc_c,
    mixbuf, xbuf, wrbuf, rdbuf, ybuf, cumbuf, stbuf, runbuf, decbuf,
    st_send, st_recv, e_send, e_recv, mbuf, apart, part, r1, p2, nbuf,
    loc_sem, ss_sem, sr_sem, gs_sem, gr_sem, cs_sem, cr_sem, os_sem, ox_sem, or_sem,
    ts_sem, tr_sem, us_sem, ur_sem, vs_sem, vr_sem, t2s_sem, t2r_sem, u2s_sem, u2r_sem,
    h_sem, g_sem, k_sem, l_sem, x_sem, e_sem, ms_sem, mr_sem,
    r1s_sem, r1r_sem, r2s_sem, r2r_sem, near_sem,
):
    sp = lax.axis_index("sp")
    tp = lax.axis_index("tp")
    rows, width = tokens.shape
    kdim = w_outer.shape[0]
    cdim = w_outer.shape[1]
    length = rows * T
    heads_width = mbuf.shape[1]
    heads = heads_width // HEAD_DIM
    ocols = obuf.shape[2]
    Y = T // CORES

    barrier = pltpu.get_barrier_semaphore()
    for d in range(1, n):
        pl.semaphore_signal(
            barrier, inc=1, device_id={"sp": lax.rem(sp + d, n)}, device_id_type=MESH
        )
    for d in range(1, T):
        pl.semaphore_signal(
            barrier, inc=1, device_id={"tp": lax.rem(tp + d, T)}, device_id_type=MESH
        )

    def pack(refs, dst, rows_too=False):
        pairs, at = [], 0
        for ref in refs:
            if rows_too:
                pairs.append((ref, dst.at[0, pl.ds(at, ref.shape[0])]))
                at += ref.shape[0]
            else:
                pairs.append((ref, dst.at[0, :, pl.ds(at, ref.shape[1])]))
                at += ref.shape[1]
        return pairs

    groups = {
        "s": pack((w_state, w_write, w_read), sbuf),
        "t": [(tokens_h, tokens), (in_scale_h, in_scale)],
        "c": pack((w_outer, w_inner, w_value), cbuf),
        "g": pack((w_ogate,), gbuf),
        "v": [
            (spikes_h, spikes), (step_w_h, step_w), (taps_conv_h, taps_conv),
            (taps_in_h, taps_in), (taps_wr_h, taps_wr), (taps_rd_h, taps_rd), (hscale_h, hscale),
            (bias_h, bias), (rate_h, rate), (direct_h, direct),
        ],
        "o": pack((o_conv, o_state), obuf, True),
    }
    whole = {"s": sbuf.at[0], "c": cbuf.at[0], "g": gbuf.at[0], "o": obuf.at[0]}
    local, index = {}, 0
    for name, pairs in groups.items():
        local[name] = []
        for src, dst in pairs:
            pltpu.make_async_copy(src, dst, loc_sem.at[index]).start()
            if name not in whole:
                local[name].append(pltpu.make_async_copy(src, dst, loc_sem.at[index]))
                index += 1
        if name in whole:
            local[name].append(
                pltpu.make_async_copy(whole[name], whole[name], loc_sem.at[index])
            )
            index += 1

    def landed(name):
        for copy in local[name]:
            copy.wait()

    z = lax.div(sp, 2)
    x = lax.rem(sp, 2)
    last_z = PLANES - 1
    odd_z = lax.rem(z, 2)
    pz = z + 1 - 2 * odd_z
    upper = lax.div(z, 2)
    inner_z = 1 + upper
    end_z = upper * last_z
    is_inner = z == inner_z
    inner = (1 - upper) * odd_z + upper * (1 - odd_z)
    mate = pz * 2 + x
    side = z * 2 + 1 - x
    cross = (last_z - z) * 2 + x
    beyond = inner * cross + (1 - inner) * side

    def pos_of(index):
        odd = lax.rem(index, 2)
        low = lax.div(index, 2)
        return (1 - odd) * low + odd * (n - 1 - low)

    def index_of(pos):
        high = lax.div(pos, n // 2)
        return (1 - high) * 2 * pos + high * (2 * (n - 1 - pos) + 1)

    pos = pos_of(sp)
    toward = pos_of(mate) - pos

    def plane_owner(slot):
        plane = (z, pz, last_z - inner_z, last_z - end_z)[slot % 4]
        return plane * 2 + (x if slot < 4 else 1 - x)

    def ring_slot(side_k, s):
        return n - 1 if s == n // 2 else 1 + side_k * (n // 2 - 1) + s - 1

    def ring_owner(slot):
        if slot == 0:
            return sp
        if slot == n - 1:
            return index_of(lax.rem(pos + n // 2, n))
        side_k, s = divmod(slot - 1, n // 2 - 1)
        way = toward if side_k == 0 else -toward
        return index_of(lax.rem(pos + n + way * (s + 1), n))

    link_device = (mate, beyond)

    class Ring:
        def __init__(self):
            self.rows = kdim // PIECES_C
            self.waited = set()

        def piece(self, slot, q):
            return cbuf.at[slot, pl.ds(q * self.rows, self.rows)]

        def copy(self, link, s, q):
            src = 0 if s == 0 else ring_slot(1 - link, s)
            dst = ring_slot(link, s + 1)
            return remote(
                self.piece(src, q), self.piece(dst, q), cs_sem.at[s // (n // 2 - 1)],
                cr_sem.at[(dst - 1) * PIECES_C + q], {"sp": link_device[link]},
            )

        def arrive(self, slot, q):
            if (slot, q) not in self.waited:
                self.waited.add((slot, q))
                remote(
                    self.piece(slot, q), self.piece(slot, q), cs_sem.at[0],
                    cr_sem.at[(slot - 1) * PIECES_C + q], {"sp": mate},
                ).wait_recv()

        def forward(self, link, s, q):
            if s > 0:
                self.arrive(ring_slot(1 - link, s), q)
            self.copy(link, s, q).start()

        def need(self, slot):
            if slot:
                for q in range(PIECES_C):
                    self.arrive(slot, q)

    own_at = pl.multiple_of(HALO + tp * rows, HALO)
    core = lax.rem(tp, CORES)
    chip = lax.div(tp, CORES)
    partner = chip * CORES + 1 - core
    last_tp = tp == T - 1

    def spread_rows(ref, pieces, near_send, near_recv, far_send, far_recv):
        prow = rows // pieces

        def at_rows(block, q):
            return ref.at[pl.ds(pl.multiple_of(HALO + block * rows + q * prow, HALO), prow)]

        def first(d, q):
            device = partner if d == 0 else lax.rem(chip + d, Y) * CORES + core
            return remote(
                at_rows(tp, q), at_rows(tp, q), near_send, near_recv.at[d, q], {"tp": device}
            )

        def second(d, q, at_core):
            block = lax.rem(chip + Y - d, Y) * CORES + at_core
            return remote(
                at_rows(block, q), at_rows(block, q), far_send, far_recv.at[d, q],
                {"tp": partner},
            )

        def start(q):
            for d in range(1, Y):
                first(d, q).start()
            first(0, q).start()

        def relay(q):
            for d in range(1, Y):
                first(d, q).wait_recv()
                second(d, q, core).start()

        def finish():
            for q in range(pieces):
                first(0, q).wait_recv()
                for d in range(1, Y):
                    second(d, q, 1 - core).wait_recv()

        return at_rows, start, relay, finish

    _, t_start, t_relay, t_finish = spread_rows(norm, PIECES_T, ts_sem, tr_sem, us_sem, ur_sem)
    u_rows, u_start, u_relay, u_finish = spread_rows(
        norm2, PIECES_U, t2s_sem, t2r_sem, u2s_sem, u2r_sem
    )

    def v_copy(q):
        prow = rows // PIECES_U
        src = norm.at[pl.ds(pl.multiple_of(own_at + q * prow, HALO), prow)]
        return remote(src, u_rows(tp, q), vs_sem, vr_sem.at[q], {"sp": mate})

    def k_copy():
        cut = pl.ds(HALO - 8, 8)
        return remote(norm.at[cut], norm2.at[cut], k_sem.at[0], k_sem.at[1], {"sp": mate})

    def l_copy():
        return remote(spikes, spikes2, l_sem.at[0], l_sem.at[1], {"sp": mate})

    def h_copy():
        return remote(
            norm.at[pl.ds(length, HALO)], norm.at[pl.ds(0, HALO)], h_sem.at[0], h_sem.at[1],
            {"sp": lax.rem(sp + 1, n)},
        )

    def g_copy(d):
        cut = pl.ds(0, HALO)
        return remote(norm.at[cut], norm.at[cut], g_sem.at[0], g_sem.at[1], {"tp": d})

    def halo_relay():
        @pl.when(last_tp & (sp > 0))
        def _():
            h_copy().wait_recv()
            for d in range(T - 1):
                g_copy(d).start()

    def halo_ready():
        @pl.when((tp < T - 1) & (sp > 0))
        def _():
            g_copy(0).wait_recv()

        @pl.when(sp == 0)
        def _():
            norm[0:HALO, :] = jnp.zeros((HALO, width), bf16)

    def project(acc, source, buf, slots, owner, fresh=False):
        for c in range(0, acc.shape[1], 256):
            total = None
            for slot in slots:
                at = pl.multiple_of(owner(slot) * kdim, kdim)
                term = jnp.dot(
                    source[:, pl.ds(at, kdim)], buf[slot, :, c : c + 256],
                    preferred_element_type=f32,
                )
                total = term if total is None else total + term
            if fresh:
                acc[:, c : c + 256] = total
            else:
                acc[:, c : c + 256] += total

    def column(ref):
        index = lax.broadcasted_iota(jnp.int32, (heads, 1), 0)
        full = jnp.full((heads, 1), ref[0], f32)
        for h in range(1, heads):
            full = jnp.where(index == h, ref[h], full)
        return full

    lane = lax.broadcasted_iota(jnp.int32, (1, heads_width), 1)

    def spread(columns):
        full = jnp.broadcast_to(columns[:, 0:1], (columns.shape[0], heads_width))
        for h in range(1, heads):
            full = jnp.where(lane >= h * HEAD_DIM, columns[:, h : h + 1], full)
        return full

    def taps(u, weights):
        k_taps = weights.shape[0]
        w = weights[...].astype(f32)
        total = w[k_taps - 1 : k_taps] * u[8:]
        for k in range(k_taps - 1):
            total = total + w[k : k + 1] * pltpu.roll(u, k_taps - 1 - k, 0)[8:]
        return total

    blocks = length // CHUNK

    def spans(b):
        t0 = b * CHUNK
        return (
            slice(t0, t0 + CHUNK),
            slice(t0 + HALO, t0 + HALO + CHUNK),
            slice(t0 + HALO - 8, t0 + HALO + CHUNK),
        )

    def field(acc, begin, size, span):
        return acc[span, begin : begin + size].astype(bf16).astype(f32)

    def conv_step(ring, s):
        slots = (0,) if s == 0 else (n - 1,) if s == n // 2 else (ring_slot(0, s), ring_slot(1, s))
        for slot in slots:
            ring.need(slot)
        project(acc_c, norm, cbuf, slots, ring_owner, s == 0)

    half_rows = length // Y
    half_blocks = half_rows // CHUNK

    def conv_mix(y):
        for b in range(half_blocks):
            t0 = y * half_rows + b * CHUNK
            span = pl.ds(pl.multiple_of(t0, CHUNK), CHUNK)
            own = pl.ds(pl.multiple_of(t0 + HALO, HALO), CHUNK)
            take = pl.ds(pl.multiple_of(t0 + HALO - 8, 8), CHUNK + 8)
            product = field(acc_c, cdim, cdim, take) * field(acc_c, 2 * cdim, cdim, take)
            mix = field(acc_c, 0, cdim, own) * taps(product, taps_conv)
            apart[span, 0:cdim] = mix.astype(bf16)

    def turned(b):
        return lax.rem(b + (1 - chip) * half_blocks, blocks)

    def m_copy(b):
        cut = pl.ds(pl.multiple_of(turned(b) * CHUNK, CHUNK), CHUNK)
        return remote(
            mbuf.at[cut], apart.at[cut, pl.ds(cdim, heads_width)], ms_sem, mr_sem.at[b],
            {"sp": mate},
        )

    def x_copy():
        return remote(st_send, st_recv, x_sem.at[0], x_sem.at[1], {"sp": side})

    def e_copy():
        return remote(e_send, e_recv, e_sem.at[0], e_sem.at[1], {"sp": cross})

    def inner_part():
        sl = Slots(sbuf, PIECES_S, sr_sem)
        gl = Slots(gbuf, PIECES_G, gr_sem)
        ol = Slots(obuf, PIECES_O, or_sem)
        ring = Ring()
        forwards = [(link, 1, q) for link in (0, 1) for q in range(PIECES_C)]
        step_two = sorted((q + 2.5 * link, link, q) for link in (0, 1) for q in range(PIECES_C))
        forwards += [(link, 2, q) for _, link, q in step_two]
        for q in range(PIECES_C // 2):
            forwards += [(1, 3, PIECES_C // 2 + q)]
        done = [0]

        def pump(count):
            for _ in range(count):
                if done[0] < len(forwards):
                    ring.forward(*forwards[done[0]])
                    done[0] += 1

        r_id = lax.broadcasted_iota(jnp.int32, (CHUNK, CHUNK), 0)
        c_id = lax.broadcasted_iota(jnp.int32, (CHUNK, CHUNK), 1)
        causal = r_id >= c_id
        lower = causal.astype(f32)
        eye = (r_id == c_id).astype(f32)

        for q in range(PIECES_C):
            ring.forward(0, 0, q)
        for q in range(PIECES_S):
            sl.arrive(1, q, ss_sem, mate)
            sl.send(1, 3, q, ss_sem, cross)
            sl.send(1, 5, q, ss_sem, side)
        for q in range(PIECES_S):
            sl.arrive(2, q, ss_sem, mate)
            sl.send(2, 6, q, ss_sem, side)
        for q in range(PIECES_C):
            ring.forward(1, 0, q)
        t_relay(0)
        landed("g")
        for q in range(PIECES_G):
            gl.send(0, 2, q, gs_sem, cross)
        landed("o")
        for q in range(PIECES_O):
            ol.send(0, 2, q, os_sem, cross)
            ol.send(0, 1, q, os_sem, mate)
        for q in range(PIECES_S):
            sl.arrive(3, q, ss_sem, mate)
            sl.send(3, 7, q, ss_sem, side)
        for q in range(PIECES_G):
            gl.send(0, 4, q, gs_sem, side)
        halo_relay()
        for q in range(PIECES_U):
            v_copy(q).wait_recv()
            u_start(q)
            if q == 0:
                for p in range(1, PIECES_T):
                    t_relay(p)
            if q > 0:
                pump(1)
                u_relay(q - 1)
        pump(1)
        t_finish()
        halo_ready()
        for q in range(PIECES_G):
            gl.arrive(1, q, gs_sem, mate)
            gl.send(1, 3, q, gs_sem, cross)
            gl.send(1, 5, q, gs_sem, side)
        u_relay(PIECES_U - 1)
        for slot in range(1, n):
            for q in range(PIECES_S):
                sl.arrive(slot, q, ss_sem, mate)
        project(acc_s.at[0], norm, sbuf, range(0, 4), plane_owner, True)
        project(acc_s.at[0], norm, sbuf, range(4, 8), plane_owner)
        for q in range(PIECES_G):
            gl.arrive(2, q, gs_sem, mate)
            gl.send(2, 6, q, gs_sem, side)
        k_copy().wait_recv()
        u_finish()
        project(acc_s.at[1], norm2, sbuf, range(0, 4), plane_owner, True)
        project(acc_s.at[1], norm2, sbuf, range(4, 8), plane_owner)
        pump(2)
        landed("v")
        l_copy().wait_recv()

        logs_of = []
        for k, (source, spike) in enumerate(((norm, spikes), (norm2, spikes2))):
            step = jax.nn.softplus(nt(step_w[...], source[HALO:, :]) + column(bias))
            logs = -step * jnp.exp(column(rate)) + spike[...]
            logs_of.append(logs)
            running = jnp.zeros((STATE, heads_width), f32)
            before = jnp.zeros((1, heads_width), f32)
            acc = acc_s.at[k]
            for b in range(blocks):
                span, own, take = spans(b)
                xs = silu(taps(field(acc, 0, cdim, take), taps_in))
                wr = silu(taps(field(acc, cdim, STATE, take), taps_wr))
                rd = silu(taps(field(acc, cdim + STATE, STATE, take), taps_rd))
                cum = nt(lower, logs[:, span], highest)
                steps = nt(eye, step[:, span], highest)
                cum_wide = spread(cum)
                weighted = xs * spread(steps)
                xbuf[k, span, :] = xs
                mixbuf[k, span, :] = weighted.astype(bf16)
                wrbuf[k, span, :] = wr.astype(bf16)
                rdbuf[k, span, :] = rd.astype(bf16)
                cumbuf[k, span, :] = cum_wide
                last = cum_wide[CHUNK - 1 : CHUNK]
                scaled = (weighted * jnp.exp(last - cum_wide)).astype(bf16)
                stbuf[k, b] = running
                running = running * jnp.exp(last) + jnp.dot(
                    wr.T.astype(bf16), scaled, preferred_element_type=f32
                )
                before = before + last
                if k == 0 and b % 2 == 1:
                    pump(1)
            runbuf[k] = running
            decbuf[k] = jnp.exp(before)
            st_send[k, 0:STATE, :] = running.astype(bf16)
            st_send[k, STATE:, :] = jnp.broadcast_to(
                jnp.exp(before), (HALO, heads_width)
            ).astype(bf16)
            if k == 0:
                for q in range(PIECES_O):
                    ol.arrive(2, q, os_sem, mate)
                    ol.send(2, 2, q, os_sem, mate)

        x_copy().start()
        for q in range(PIECES_G):
            gl.arrive(3, q, gs_sem, mate)
            gl.send(3, 7, q, gs_sem, side)

        def within(k, b):
            span, _, _ = spans(b)
            scores = nt(rdbuf[k, span, :], wrbuf[k, span, :])
            cum_t = lax.dot_general(
                logs_of[k][:, span], lower, (((1,), (1,)), ((), ())),
                preferred_element_type=f32, precision=highest,
            )
            for pair in range(0, heads_width, 128):
                both = []
                for h in range(pair // HEAD_DIM, (pair + 128) // HEAD_DIM):
                    diff = cumbuf[k, span, h * HEAD_DIM : h * HEAD_DIM + 1] - cum_t[h : h + 1, :]
                    damped = scores * jnp.exp(jnp.where(causal, diff, -1e30))
                    both.append(
                        jnp.dot(
                            damped.astype(bf16), mixbuf[k, span, pair : pair + 128],
                            preferred_element_type=f32,
                        )
                    )
                first = lax.broadcasted_iota(jnp.int32, (1, 128), 1) < HEAD_DIM
                ybuf[k, span, pair : pair + 128] = jnp.where(first, both[0], both[1])

        for b in range(blocks):
            within(1, b)
        pump(1)
        for slot in (0, 2):
            for q in range(PIECES_O):
                ol.send(slot, 4 + slot, q, ox_sem, side)
        for b in range(blocks):
            within(0, b)
        for q in range(PIECES_O):
            ol.arrive(1, q, os_sem, mate)
            ol.send(1, 3, q, os_sem, cross)
            ol.send(1, 5, q, ox_sem, side)
        pump(1)
        x_copy().wait_recv()
        second = jnp.broadcast_to(x, (1, heads_width)) == 1
        pair, pair_decay, other, first_decay = [], [], [], []
        for k in range(2):
            theirs = st_recv[k, 0:STATE, :].astype(f32)
            their_decay = st_recv[k, STATE : STATE + 1, :].astype(f32)
            pair.append(
                jnp.where(
                    second, theirs * decbuf[k] + runbuf[k], runbuf[k] * their_decay + theirs
                )
            )
            pair_decay.append(decbuf[k] * their_decay)
            other.append(jnp.where(second, theirs, jnp.zeros_like(theirs)))
            first_decay.append(jnp.where(second, their_decay, jnp.ones_like(their_decay)))

        @pl.when(upper == 0)
        def _():
            e_send[...] = (pair[1] * pair_decay[0] + pair[0]).astype(bf16)
            e_copy().start()
            runbuf[1] = other[1]
            runbuf[0] = other[0] + first_decay[0] * pair[1]

        @pl.when(upper == 1)
        def _():
            runbuf[0] = other[0]
            runbuf[1] = other[1] + first_decay[1] * pair[0]
            decbuf[0] = first_decay[0]
            decbuf[1] = first_decay[1] * pair_decay[0]

        pump(2)
        pump(1)
        for slot in range(1, n - 1):
            for q in range(PIECES_G):
                gl.arrive(slot, q, gs_sem, mate)
        for k, source in enumerate((norm, norm2)):
            project(acc_g.at[k], source, gbuf, range(n - 1), plane_owner, True)
            pump(1)
        conv_step(ring, 0)
        pump(1)
        for q in range(PIECES_G):
            gl.arrive(n - 1, q, gs_sem, mate)
        for k, source in enumerate((norm, norm2)):
            project(acc_g.at[k], source, gbuf, (n - 1,), plane_owner)

        for q in range(PIECES_O):
            ol.arrive(3, q, os_sem, mate)
            ol.send(3, 3, q, os_sem, mate)
            ol.send(3, 7, q, ox_sem, side)

        @pl.when(upper == 1)
        def _():
            e_copy().wait_recv()
            entering = e_recv[...].astype(f32)
            for k in range(2):
                runbuf[k] = runbuf[k] + decbuf[k] * entering

        group = (
            lax.div(lax.broadcasted_iota(jnp.int32, (heads_width, heads_width), 0), HEAD_DIM)
            == lax.div(lax.broadcasted_iota(jnp.int32, (heads_width, heads_width), 1), HEAD_DIM)
        ).astype(bf16)
        direct_wide = jnp.full((1, heads_width), direct[0], f32)
        for h in range(1, heads):
            direct_wide = jnp.where(lane >= h * HEAD_DIM, direct[h], direct_wide)

        for k in (1, 0):
            so_far = jnp.zeros((1, heads_width), f32)
            for b in range(blocks):
                stbuf[k, b] = stbuf[k, b] + jnp.exp(so_far) * runbuf[k]
                at_end = b * CHUNK + CHUNK - 1
                so_far = so_far + cumbuf[k, at_end : at_end + 1, :]
            for i in range(blocks):
                b = turned(i)
                span = pl.ds(pl.multiple_of(b * CHUNK, CHUNK), CHUNK)
                own = pl.ds(pl.multiple_of(b * CHUNK + HALO, HALO), CHUNK)
                head_out = (
                    ybuf[k, span, :]
                    + jnp.dot(
                        rdbuf[k, span, :], stbuf[k, b].astype(bf16), preferred_element_type=f32
                    )
                    * jnp.exp(cumbuf[k, span, :])
                    + direct_wide * xbuf[k, span, :]
                )
                gated = head_out * silu(field(acc_g.at[k], 0, cdim, own))
                square = jnp.dot((gated * gated).astype(bf16), group, preferred_element_type=f32)
                normalized = gated * lax.rsqrt(square * (1.0 / HEAD_DIM) + epsilon)
                result = (
                    normalized * hscale[...].astype(f32).reshape(1, heads_width)
                ).astype(bf16)
                if k == 1:
                    mbuf[span, :] = result
                    m_copy(i).start()
                else:
                    apart[span, cdim:] = result
        pump(1)
        conv_step(ring, 1)
        pump(1)
        conv_step(ring, 2)
        pump(len(forwards))
        conv_step(ring, 3)
        conv_step(ring, n // 2)
        conv_mix(1 - chip)

    def blocks_sent(buf, count, sem):
        every = buf.at[pl.ds(0, count)]
        remote(every, every, sem, cr_sem.at[0], {"sp": mate}).wait_send()

    def end_part():
        gl = Slots(gbuf, PIECES_G, gr_sem)
        ol = Slots(obuf, PIECES_O, or_sem)
        ring = Ring()
        for q in range(PIECES_U):
            v_copy(q).start()
        for q in range(PIECES_C):
            ring.forward(1, 0, q)
        landed("v")
        l_copy().start()
        landed("g")
        for q in range(PIECES_G):
            gl.send(0, 1, q, gs_sem, mate)
        t_relay(0)
        for q in range(PIECES_C):
            ring.forward(1, 1, q)
        for q in range(1, PIECES_T):
            t_relay(q)
        halo_relay()
        halo_ready()
        k_copy().start()
        landed("o")
        for q in range(PIECES_C):
            ring.forward(0, 0, q)
        for q in range(PIECES_O):
            ol.send(0, 1, q, os_sem, mate)
        for q in range(PIECES_O):
            ol.send(0, 4, q, ox_sem, side)
        for q in range(PIECES_C):
            ring.forward(0, 1, q)
        for q in range(PIECES_O):
            ol.arrive(1, q, os_sem, mate)
            ol.send(1, 5, q, ox_sem, side)
        for q in range(PIECES_C):
            ring.forward(0, 2, q)
        t_finish()
        conv_step(ring, 0)
        conv_step(ring, 1)
        for q in range(PIECES_C):
            ring.forward(1, 2, q)
        for q in range(PIECES_C // 2):
            ring.forward(0, 3, q)
        conv_step(ring, 2)
        for q in range(PIECES_O):
            ol.arrive(2, q, os_sem, mate)
            ol.send(2, 6, q, ox_sem, side)
        for q in range(PIECES_C):
            ring.forward(1, 3, q)
        conv_step(ring, 3)
        conv_step(ring, n // 2)
        conv_mix(1 - chip)
        for q in range(PIECES_O):
            ol.arrive(3, q, os_sem, mate)
            ol.send(3, 7, q, ox_sem, side)
        for b in range(half_blocks):
            m_copy(b).wait_recv()

    landed("s")
    pl.semaphore_wait(barrier, n - 1 + T - 1)
    first_s = Slots(sbuf, PIECES_S, sr_sem)

    @pl.when(is_inner)
    def _():
        for q in range(PIECES_S):
            first_s.send(0, 2, q, ss_sem, cross)
            first_s.send(0, 4, q, ss_sem, side)

    @pl.when(is_inner)
    def _():
        norm2[0 : HALO - 8, :] = jnp.zeros((HALO - 8, width), bf16)

    @pl.when(z == end_z)
    def _():
        for q in range(PIECES_S):
            first_s.send(0, 1, q, ss_sem, mate)

    landed("t")
    value = tokens[...].astype(f32)
    value = value * lax.rsqrt(jnp.mean(value * value, axis=1, keepdims=True) + epsilon)
    norm[pl.ds(own_at, rows), :] = (
        value * in_scale[...].astype(f32).reshape(1, width)
    ).astype(bf16)
    for q in range(PIECES_T):
        t_start(q)

    @pl.when(last_tp & (sp < n - 1))
    def _():
        h_copy().start()

    landed("c")

    @pl.when(is_inner)
    def _():
        inner_part()

    @pl.when(z == end_z)
    def _():
        end_part()

    def block_rows(y, c):
        return pl.ds(pl.multiple_of((y * CORES + c) * rows, rows), rows)

    def columns_of(slot):
        return pl.ds(pl.multiple_of(plane_owner(slot) * ocols, ocols), ocols)

    def r1_copy(d, s):
        return remote(
            part.at[s, block_rows(lax.rem(chip + d, Y), 1 - core)], r1.at[s, d], r1s_sem,
            r1r_sem.at[d, s], {"tp": partner},
        )

    def r2_copy(d, s):
        return remote(
            p2.at[d - 1, s], far.at[d - 1, :, columns_of(s)], r2s_sem, r2r_sem,
            {"tp": lax.rem(chip + d, Y) * CORES + core},
        )

    def near_copy(s):
        return pltpu.make_async_copy(nbuf.at[s], near.at[:, columns_of(s)], near_sem)

    o_last = Slots(obuf, PIECES_O, or_sem)

    def project_out(d, s):
        if s >= 4:
            for q in range(PIECES_O):
                o_last.arrive(s, q, os_sem, mate)
        span = pl.ds(pl.multiple_of(lax.rem(chip + d, Y) * half_rows, half_rows), half_rows)
        part[s, span, :] = jnp.dot(
            apart[span, :], obuf[s], preferred_element_type=f32
        ).astype(bf16)
        r1_copy(d, s).start()

    def reduce(d, s):
        r1_copy(d, s).wait_recv()
        mine = part[s, block_rows(lax.rem(chip + d, Y), core), :]
        total = (mine.astype(f32) + r1[s, d].astype(f32)).astype(bf16)
        if d:
            p2[d - 1, s] = total
            r2_copy(d, s).start()
        else:
            nbuf[s] = total
            near_copy(s).start()

    open_sums = []

    def output(d, s, lag=3):
        project_out(d, s)
        open_sums.append((d, s))
        if len(open_sums) > lag:
            reduce(*open_sums.pop(0))

    for s in (0, 1, 2, 4, 5, 6):
        output(1, s)
    conv_mix(chip)

    @pl.when(z == end_z)
    def _():
        for b in range(half_blocks, blocks):
            m_copy(b).wait_recv()

    while open_sums:
        reduce(*open_sums.pop(0))
    for d, s in ((0, 0), (0, 1), (1, 3), (0, 2), (0, 4), (1, 7), (0, 5), (0, 6), (0, 3), (0, 7)):
        output(d, s, 1 if s == 7 else 2)
    while open_sums:
        reduce(*open_sums.pop(0))

    @pl.when(is_inner)
    def _():
        x_copy().wait_send()

        @pl.when(upper == 0)
        def _():
            e_copy().wait_send()

        half = cbuf.at[pl.ds(0, 1), pl.ds(0, kdim // 2)]
        remote(half, half, cs_sem.at[1], cr_sem.at[0], {"sp": mate}).wait_send()
        blocks_sent(sbuf, 6, ss_sem)
        blocks_sent(gbuf, 6, gs_sem)
        blocks_sent(obuf, 5, os_sem)
        remote(mbuf, mbuf, ms_sem, mr_sem.at[0], {"sp": mate}).wait_send()
        remote(
            norm2.at[pl.ds(0, Y * rows)], norm2.at[pl.ds(0, Y * rows)], t2s_sem,
            t2r_sem.at[0, 0], {"tp": partner},
        ).wait_send()
        remote(
            norm2.at[pl.ds(0, (Y - 1) * rows)], norm2.at[pl.ds(0, (Y - 1) * rows)], u2s_sem,
            u2r_sem.at[0, 0], {"tp": partner},
        ).wait_send()

    @pl.when(z == end_z)
    def _():
        half = cbuf.at[pl.ds(0, 3), pl.ds(0, kdim // 2)]
        remote(half, half, cs_sem.at[1], cr_sem.at[0], {"sp": mate}).wait_send()
        blocks_sent(sbuf, 1, ss_sem)
        blocks_sent(gbuf, 1, gs_sem)
        blocks_sent(obuf, 1, os_sem)
        remote(
            norm.at[pl.ds(0, rows)], norm.at[pl.ds(0, rows)], vs_sem, vr_sem.at[0], {"sp": mate}
        ).wait_send()
        k_copy().wait_send()
        l_copy().wait_send()

    blocks_sent(cbuf, n - 2, cs_sem.at[0])
    blocks_sent(obuf, 4, ox_sem)
    remote(
        norm.at[pl.ds(0, Y * rows)], norm.at[pl.ds(0, Y * rows)], ts_sem, tr_sem.at[0, 0],
        {"tp": partner},
    ).wait_send()
    remote(
        norm.at[pl.ds(0, (Y - 1) * rows)], norm.at[pl.ds(0, (Y - 1) * rows)], us_sem,
        ur_sem.at[0, 0], {"tp": partner},
    ).wait_send()

    @pl.when(last_tp & (sp < n - 1))
    def _():
        h_copy().wait_send()

    @pl.when(last_tp & (sp > 0))
    def _():
        cut = pl.ds(0, (T - 1) * HALO)
        remote(norm.at[cut], norm.at[cut], g_sem.at[0], g_sem.at[1], {"tp": partner}).wait_send()

    remote(r1, r1, r1s_sem, r1r_sem.at[0, 0], {"tp": partner}).wait_send()
    remote(p2, p2, r2s_sem, r2r_sem, {"tp": partner}).wait_send()
    pltpu.make_async_copy(far.at[0], near, near_sem).wait()
    remote(far, far, r2s_sem, r2r_sem, {"tp": partner}).wait_recv()


def shifted(shard, axis, by):
    devices = lax.axis_size(axis)
    pairs = [(i, i + by) for i in range(devices) if 0 <= i + by < devices]
    return lax.ppermute(shard, axis, pairs)


def prefix(shard, axis, combine, identity):
    devices, index = (lax.axis_size(axis), lax.axis_index(axis))
    everything = jax.tree.map(
        lambda part, kind: lax.all_gather(part.astype(kind), axis),
        shard,
        (jnp.bfloat16, jnp.bfloat16),
    )
    start = jax.tree.map(
        lambda part, zero: jnp.broadcast_to(jnp.asarray(zero, part.dtype), part.shape),
        shard,
        identity,
    )

    def turn(k, before):
        reached = k < index
        new = combine(
            before, jax.tree.map(lambda part, own: part[k].astype(own.dtype), everything, shard)
        )
        return jax.tree.map(lambda a, b: jnp.where(reached, a, b), new, before)

    return lax.fori_loop(0, devices, turn, start)


def causal_taps(values, rim_rows, tap_weights):
    tap_count = tap_weights.shape[0]
    length = values.shape[0]
    padded = jnp.concatenate([rim_rows, values], axis=0)
    running = tap_weights[0] * padded[0:length]
    for offset in range(1, tap_count):
        running = running + tap_weights[offset] * padded[offset : offset + length]
    return running


def combine_states(earlier, later):
    return (earlier[0] * later[0], earlier[1] * later[0][:, None, None] + later[1])


def plain_path(
    tokens,
    input_norm_scale,
    outer_gate_weight,
    inner_gate_weight,
    value_weight_matrix,
    output_gate_weight,
    state_input_weight,
    write_key_weight,
    read_key_weight,
    step_size_weight,
    gated_conv_weight,
    input_conv_weight,
    write_conv_weight,
    read_conv_weight,
    step_size_bias,
    log_decay_rate,
    decay_spikes,
    direct_path_weight,
    head_norm_scale,
    conv_output_weight,
    state_output_weight,
):
    token_rows = tokens.astype(jnp.float32)
    scaled = token_rows * lax.rsqrt(
        jnp.mean(token_rows * token_rows, axis=1, keepdims=True) + epsilon
    )
    normed_own = (scaled * input_norm_scale.astype(jnp.float32)).astype(jnp.bfloat16)
    normed = lax.all_gather(normed_own, "tp", axis=0, tiled=True)
    length = normed.shape[0]
    pieces = (
        lax.all_gather(outer_gate_weight, "sp", axis=0, tiled=True),
        lax.all_gather(inner_gate_weight, "sp", axis=0, tiled=True),
        lax.all_gather(value_weight_matrix, "sp", axis=0, tiled=True),
        lax.all_gather(output_gate_weight, "sp", axis=0, tiled=True),
        lax.all_gather(state_input_weight, "sp", axis=0, tiled=True),
        lax.all_gather(write_key_weight, "sp", axis=0, tiled=True),
        lax.all_gather(read_key_weight, "sp", axis=0, tiled=True),
    )
    projected = tuple(
        (jnp.dot(normed, weight_rows, preferred_element_type=jnp.float32) for weight_rows in pieces)
    )
    outer_gate, inner_gate, conv_input, out_gate, state_input, write_keys, read_keys = [
        member.astype(jnp.bfloat16) for member in projected
    ]
    step_raw = jnp.dot(normed, step_size_weight, preferred_element_type=jnp.float32)
    short_rim = gated_conv_weight.shape[0] - 1
    state_rim = input_conv_weight.shape[0] - 1
    rim_rows = shifted(
        (
            inner_gate[length - short_rim :],
            conv_input[length - short_rim :],
            state_input[length - state_rim :],
            write_keys[length - state_rim :],
            read_keys[length - state_rim :],
        ),
        "sp",
        1,
    )
    product = inner_gate.astype(jnp.float32) * conv_input.astype(jnp.float32)
    rim_product = rim_rows[0].astype(jnp.float32) * rim_rows[1].astype(jnp.float32)
    mixer_part = (
        outer_gate.astype(jnp.float32)
        * causal_taps(product, rim_product, gated_conv_weight.astype(jnp.float32))
    ).astype(jnp.bfloat16)
    seq_input = jax.nn.silu(
        causal_taps(
            state_input.astype(jnp.float32),
            rim_rows[2].astype(jnp.float32),
            input_conv_weight.astype(jnp.float32),
        )
    )
    seq_write = jax.nn.silu(
        causal_taps(
            write_keys.astype(jnp.float32),
            rim_rows[3].astype(jnp.float32),
            write_conv_weight.astype(jnp.float32),
        )
    )
    seq_read = jax.nn.silu(
        causal_taps(
            read_keys.astype(jnp.float32),
            rim_rows[4].astype(jnp.float32),
            read_conv_weight.astype(jnp.float32),
        )
    )
    discrete_step = jax.nn.softplus(step_raw + step_size_bias[None, :])
    step_logarithm = discrete_step * (-jnp.exp(log_decay_rate))[None, :] + decay_spikes.T
    heads_here = discrete_step.shape[1]
    groups_here = seq_write.shape[1] // STATE
    per_group = heads_here // groups_here
    blocks = length // PLAIN_BLOCK
    input_blocks = seq_input.reshape(blocks, PLAIN_BLOCK, heads_here, HEAD_DIM)
    weighted = input_blocks * discrete_step.reshape(blocks, PLAIN_BLOCK, heads_here, 1)
    write_blocks = jnp.repeat(
        seq_write.reshape(blocks, PLAIN_BLOCK, groups_here, STATE), per_group, axis=2
    )
    read_blocks = jnp.repeat(seq_read.reshape(blocks, PLAIN_BLOCK, groups_here, STATE), per_group, axis=2)
    cumulative = jnp.cumsum(step_logarithm.reshape(blocks, PLAIN_BLOCK, heads_here), axis=1)
    causal = lax.broadcasted_iota(jnp.int32, (PLAIN_BLOCK, PLAIN_BLOCK), 0) >= lax.broadcasted_iota(
        jnp.int32, (PLAIN_BLOCK, PLAIN_BLOCK), 1
    )
    scores = jnp.einsum("clhm,cshm->clsh", read_blocks, write_blocks, precision=highest)
    damping = jnp.exp(
        jnp.where(
            causal[None, :, :, None],
            cumulative[:, :, None, :] - cumulative[:, None, :, :],
            -jnp.inf,
        )
    )
    within_block = jnp.einsum("clsh,cshp->clhp", scores * damping, weighted, precision=highest)
    to_end = jnp.exp(cumulative[:, -1:, :] - cumulative)
    block_states = jnp.einsum(
        "cshm,cshp->chpm", write_blocks * to_end[..., None], weighted, precision=highest
    )
    block_logs = cumulative[:, -1, :]

    def advance(carried_state, inputs):
        contribution, block_log = inputs
        return (carried_state * jnp.exp(block_log)[:, None, None] + contribution, carried_state)

    own_total, own_before = lax.scan(
        advance, jnp.zeros(block_states.shape[1:], jnp.float32), (block_states, block_logs)
    )
    total_log = jnp.sum(block_logs, axis=0)
    arriving = prefix(
        (jnp.exp(total_log), own_total),
        "sp",
        combine_states,
        (jnp.ones_like(total_log), jnp.zeros_like(own_total)),
    )[1]
    before_logs = jnp.cumsum(block_logs, axis=0) - block_logs
    entering = own_before + jnp.exp(before_logs)[:, :, None, None] * arriving[None]
    from_before = (
        jnp.einsum("clhm,chpm->clhp", read_blocks, entering, precision=highest)
        * jnp.exp(cumulative)[..., None]
    )
    head_out = within_block + from_before + direct_path_weight[None, None, :, None] * input_blocks
    head_out = head_out.reshape(length, heads_here * HEAD_DIM)
    gated_heads = (head_out * jax.nn.silu(out_gate.astype(jnp.float32))).reshape(
        length, heads_here, HEAD_DIM
    )
    normalized = gated_heads * lax.rsqrt(
        jnp.mean(gated_heads * gated_heads, axis=2, keepdims=True) + epsilon
    )
    state_part = (
        normalized.reshape(length, heads_here * HEAD_DIM) * head_norm_scale.astype(jnp.float32)
    ).astype(jnp.bfloat16)
    wide_mixer, wide_state = (
        lax.all_gather(conv_output_weight, "sp", axis=1, tiled=True),
        lax.all_gather(state_output_weight, "sp", axis=1, tiled=True),
    )
    return lax.psum_scatter(
        (
            jnp.dot(mixer_part, wide_mixer, preferred_element_type=jnp.float32)
            + jnp.dot(state_part, wide_state, preferred_element_type=jnp.float32)
        ).astype(jnp.bfloat16),
        "tp",
        scatter_dimension=0,
        tiled=True,
    )


def per_device(
    tokens, input_norm_scale, outer_gate_weight, inner_gate_weight, value_weight_matrix,
    output_gate_weight, state_input_weight, write_key_weight, read_key_weight, step_size_weight,
    gated_conv_weight, input_conv_weight, write_conv_weight, read_conv_weight, step_size_bias,
    log_decay_rate, decay_spikes, direct_path_weight, head_norm_scale, conv_output_weight,
    state_output_weight,
):
    n, T = lax.axis_size("sp"), lax.axis_size("tp")
    rows, width = tokens.shape
    kdim, cdim = outer_gate_weight.shape
    heads = step_size_bias.shape[0]
    hw = heads * HEAD_DIM
    length = rows * T
    ocols = conv_output_weight.shape[1]
    if (
        kdim % 128 or ocols % 256 or n % 2 or n != 2 * PLANES or T % CORES
        or T != 2 * CORES
        or write_key_weight.shape[1] != STATE
    ):
        return plain_path(
            tokens, input_norm_scale, outer_gate_weight, inner_gate_weight,
            value_weight_matrix, output_gate_weight, state_input_weight, write_key_weight,
            read_key_weight, step_size_weight, gated_conv_weight, input_conv_weight,
            write_conv_weight, read_conv_weight, step_size_bias, log_decay_rate, decay_spikes,
            direct_path_weight, head_norm_scale, conv_output_weight, state_output_weight,
        )
    Y = T // CORES
    hbm = pl.BlockSpec(memory_space=pl.ANY)
    dma = pltpu.SemaphoreType.DMA
    s_cols, blocks = cdim + 2 * STATE, length // CHUNK

    def like(array):
        return pltpu.VMEM(array.shape, array.dtype)

    step_t = step_size_weight.T
    near, far = pl.pallas_call(
        functools.partial(kernel, n, T),
        out_shape=(
            jax.ShapeDtypeStruct((rows, width), bf16),
            jax.ShapeDtypeStruct((Y - 1, rows, width), bf16),
        ),
        in_specs=[hbm] * 21,
        out_specs=(hbm, hbm),
        scratch_shapes=[
            like(tokens),
            like(input_norm_scale),
            like(step_t),
            like(gated_conv_weight),
            like(input_conv_weight),
            like(write_conv_weight),
            like(read_conv_weight),
            like(decay_spikes),
            like(head_norm_scale),
            pltpu.SMEM((heads,), f32),
            pltpu.SMEM((heads,), f32),
            pltpu.SMEM((heads,), f32),
            pltpu.VMEM((n, kdim, s_cols), bf16),
            pltpu.VMEM((n, kdim, cdim), bf16),
            pltpu.VMEM((n, kdim, 3 * cdim), bf16),
            pltpu.VMEM((n, cdim + hw, ocols), bf16),
            pltpu.VMEM((HALO + length, width), bf16),
            pltpu.VMEM((HALO + length, width), bf16),
            like(decay_spikes),
            pltpu.VMEM((2, HALO + length, s_cols), f32),
            pltpu.VMEM((2, HALO + length, cdim), f32),
            pltpu.VMEM((HALO + length, 3 * cdim), f32),
            pltpu.VMEM((2, length, hw), bf16),
            pltpu.VMEM((2, length, hw), f32),
            pltpu.VMEM((2, length, STATE), bf16),
            pltpu.VMEM((2, length, STATE), bf16),
            pltpu.VMEM((2, length, hw), f32),
            pltpu.VMEM((2, length, hw), f32),
            pltpu.VMEM((2, blocks, STATE, hw), f32),
            pltpu.VMEM((2, STATE, hw), f32),
            pltpu.VMEM((2, 1, hw), f32),
            pltpu.VMEM((2, STATE + HALO, hw), bf16),
            pltpu.VMEM((2, STATE + HALO, hw), bf16),
            pltpu.VMEM((STATE, hw), bf16),
            pltpu.VMEM((STATE, hw), bf16),
            pltpu.VMEM((length, hw), bf16),
            pltpu.VMEM((length, cdim + hw), bf16),
            pltpu.VMEM((n, length, ocols), bf16),
            pltpu.VMEM((n, Y, rows, ocols), bf16),
            pltpu.VMEM((Y - 1, n, rows, ocols), bf16),
            pltpu.VMEM((n, rows, ocols), bf16),
            dma((16,)),
            dma,
            dma(((n - 1) * PIECES_S,)),
            dma,
            dma(((n - 1) * PIECES_G,)),
            dma((2,)),
            dma(((n - 1) * PIECES_C,)),
            dma,
            dma,
            dma(((n - 1) * PIECES_O,)),
            dma,
            dma((Y, PIECES_T)),
            dma,
            dma((Y, PIECES_T)),
            dma,
            dma((PIECES_U,)),
            dma,
            dma((Y, PIECES_U)),
            dma,
            dma((Y, PIECES_U)),
            dma((2,)),
            dma((2,)),
            dma((2,)),
            dma((2,)),
            dma((2,)),
            dma((2,)),
            dma,
            dma((blocks,)),
            dma,
            dma((Y, n)),
            dma,
            dma,
            dma,
        ],
        compiler_params=pltpu.CompilerParams(
            collective_id=0, has_side_effects=True, vmem_limit_bytes=62 * 1024 * 1024
        ),
    )(
        tokens, input_norm_scale, outer_gate_weight, inner_gate_weight,
        value_weight_matrix, output_gate_weight, state_input_weight, write_key_weight,
        read_key_weight, step_t, gated_conv_weight, input_conv_weight, write_conv_weight,
        read_conv_weight, step_size_bias, log_decay_rate, decay_spikes, direct_path_weight,
        head_norm_scale,
        conv_output_weight, state_output_weight,
    )
    total = near.astype(f32)
    for d in range(Y - 1):
        total = total + far[d].astype(f32)
    return total.astype(bf16)


def solution(mesh):
    placed = (
        (P(("sp", "tp"), None), P())
        + (P("sp", "tp"),) * 7
        + (P(None, "tp"),) * 5
        + (P("tp"), P("tp"), P("tp", "sp"), P("tp"), P("tp"), P("tp", "sp"), P("tp", "sp"))
    )
    return jax.shard_map(
        per_device, mesh=mesh, in_specs=placed, out_specs=P(("sp", "tp"), None), check_vma=False
    )
```

```python
import functools

import jax
import jax.numpy as jnp
from jax import lax
from jax.experimental import pallas as pl
from jax.experimental.pallas import tpu as pltpu
from jax.sharding import PartitionSpec as P

HEAD_DIM = 64
STATE = 128
PLAIN_BLOCK = 64
CHUNK = 128
HALO = 16
PIECES_S = 2
PIECES_G = 1
PIECES_C = 4
PIECES_O = 2
PIECES_T = 2
PIECES_U = 4
PLANES = 4
FAR_PIECES = 1
CORES = 2
epsilon = 1e-05
highest = lax.Precision.HIGHEST
f32 = jnp.float32
bf16 = jnp.bfloat16
MESH = pl.DeviceIdType.MESH


def nt(a, b, precision=None):
    return lax.dot_general(
        a, b, (((1,), (1,)), ((), ())), preferred_element_type=f32, precision=precision
    )


def silu(v):
    return v / (1.0 + jnp.exp(-v))


def remote(src, dst, send, recv, device):
    return pltpu.make_async_remote_copy(
        src_ref=src, dst_ref=dst, send_sem=send, recv_sem=recv, device_id=device,
        device_id_type=MESH,
    )


class Slots:
    def __init__(self, buf, pieces, recv):
        self.buf, self.pieces, self.recv = buf, pieces, recv
        self.rows = buf.shape[1] // pieces
        self.waited = set()

    def piece(self, slot, q):
        return self.buf.at[slot, pl.ds(q * self.rows, self.rows)]

    def send(self, src, dst, q, sem, device):
        remote(
            self.piece(src, q), self.piece(dst, q), sem,
            self.recv.at[(dst - 1) * self.pieces + q], {"sp": device},
        ).start()

    def arrive(self, slot, q, sem, device):
        if (slot, q) not in self.waited:
            self.waited.add((slot, q))
            remote(
                self.piece(slot, q), self.piece(slot, q), sem,
                self.recv.at[(slot - 1) * self.pieces + q], {"sp": device},
            ).wait_recv()


def kernel(
    n,
    T,
    tokens_h, in_scale_h, w_outer, w_inner, w_value, w_ogate, w_state, w_write, w_read,
    step_w_h, taps_conv_h, taps_in_h, taps_wr_h, taps_rd_h,
    bias_h, rate_h, spikes_h, direct_h, hscale_h, o_conv, o_state,
    near, far,
    tokens, in_scale, step_w, taps_conv, taps_in, taps_wr, taps_rd, spikes, hscale,
    bias, rate, direct, sbuf, gbuf, cbuf, obuf, norm, norm2, spikes2, acc_s, acc_g, acc_c,
    mixbuf, xbuf, wrbuf, rdbuf, ybuf, cumbuf, stbuf, runbuf, decbuf,
    st_send, st_recv, e_send, e_recv, mbuf, apart, part, r1, p2, nbuf,
    loc_sem, ss_sem, sr_sem, gs_sem, gr_sem, cs_sem, cr_sem, os_sem, ox_sem, or_sem,
    ts_sem, tr_sem, us_sem, ur_sem, vs_sem, vr_sem, t2s_sem, t2r_sem, u2s_sem, u2r_sem,
    h_sem, g_sem, k_sem, l_sem, x_sem, e_sem, ms_sem, mr_sem,
    r1s_sem, r1r_sem, r2s_sem, r2r_sem, near_sem,
):
    sp = lax.axis_index("sp")
    tp = lax.axis_index("tp")
    rows, width = tokens.shape
    kdim = w_outer.shape[0]
    cdim = w_outer.shape[1]
    length = rows * T
    heads_width = mbuf.shape[1]
    heads = heads_width // HEAD_DIM
    ocols = obuf.shape[2]
    Y = T // CORES

    barrier = pltpu.get_barrier_semaphore()
    for d in range(1, n):
        pl.semaphore_signal(
            barrier, inc=1, device_id={"sp": lax.rem(sp + d, n)}, device_id_type=MESH
        )
    for d in range(1, T):
        pl.semaphore_signal(
            barrier, inc=1, device_id={"tp": lax.rem(tp + d, T)}, device_id_type=MESH
        )

    def pack(refs, dst, rows_too=False):
        pairs, at = [], 0
        for ref in refs:
            if rows_too:
                pairs.append((ref, dst.at[0, pl.ds(at, ref.shape[0])]))
                at += ref.shape[0]
            else:
                pairs.append((ref, dst.at[0, :, pl.ds(at, ref.shape[1])]))
                at += ref.shape[1]
        return pairs

    groups = {
        "s": pack((w_state, w_write, w_read), sbuf),
        "t": [(tokens_h, tokens), (in_scale_h, in_scale)],
        "c": pack((w_outer, w_inner, w_value), cbuf),
        "g": pack((w_ogate,), gbuf),
        "v": [
            (spikes_h, spikes), (step_w_h, step_w), (taps_conv_h, taps_conv),
            (taps_in_h, taps_in), (taps_wr_h, taps_wr), (taps_rd_h, taps_rd), (hscale_h, hscale),
            (bias_h, bias), (rate_h, rate), (direct_h, direct),
        ],
        "o": pack((o_conv, o_state), obuf, True),
    }
    whole = {"s": sbuf.at[0], "c": cbuf.at[0], "g": gbuf.at[0], "o": obuf.at[0]}
    local, index = {}, 0
    for name, pairs in groups.items():
        local[name] = []
        for src, dst in pairs:
            pltpu.make_async_copy(src, dst, loc_sem.at[index]).start()
            if name not in whole:
                local[name].append(pltpu.make_async_copy(src, dst, loc_sem.at[index]))
                index += 1
        if name in whole:
            local[name].append(
                pltpu.make_async_copy(whole[name], whole[name], loc_sem.at[index])
            )
            index += 1

    def landed(name):
        for copy in local[name]:
            copy.wait()

    z = lax.div(sp, 2)
    x = lax.rem(sp, 2)
    last_z = PLANES - 1
    odd_z = lax.rem(z, 2)
    pz = z + 1 - 2 * odd_z
    upper = lax.div(z, 2)
    inner_z = 1 + upper
    end_z = upper * last_z
    is_inner = z == inner_z
    inner = (1 - upper) * odd_z + upper * (1 - odd_z)
    mate = pz * 2 + x
    side = z * 2 + 1 - x
    cross = (last_z - z) * 2 + x
    beyond = inner * cross + (1 - inner) * side

    def pos_of(index):
        odd = lax.rem(index, 2)
        low = lax.div(index, 2)
        return (1 - odd) * low + odd * (n - 1 - low)

    def index_of(pos):
        high = lax.div(pos, n // 2)
        return (1 - high) * 2 * pos + high * (2 * (n - 1 - pos) + 1)

    pos = pos_of(sp)
    toward = pos_of(mate) - pos

    def plane_owner(slot):
        plane = (z, pz, last_z - inner_z, last_z - end_z)[slot % 4]
        return plane * 2 + (x if slot < 4 else 1 - x)

    def ring_slot(side_k, s):
        return n - 1 if s == n // 2 else 1 + side_k * (n // 2 - 1) + s - 1

    def ring_owner(slot):
        if slot == 0:
            return sp
        if slot == n - 1:
            return index_of(lax.rem(pos + n // 2, n))
        side_k, s = divmod(slot - 1, n // 2 - 1)
        way = toward if side_k == 0 else -toward
        return index_of(lax.rem(pos + n + way * (s + 1), n))

    link_device = (mate, beyond)

    class Ring:
        def __init__(self):
            self.rows = kdim // PIECES_C
            self.waited = set()

        def piece(self, slot, q):
            return cbuf.at[slot, pl.ds(q * self.rows, self.rows)]

        def copy(self, link, s, q):
            src = 0 if s == 0 else ring_slot(1 - link, s)
            dst = ring_slot(link, s + 1)
            return remote(
                self.piece(src, q), self.piece(dst, q), cs_sem.at[s // (n // 2 - 1)],
                cr_sem.at[(dst - 1) * PIECES_C + q], {"sp": link_device[link]},
            )

        def arrive(self, slot, q):
            if (slot, q) not in self.waited:
                self.waited.add((slot, q))
                remote(
                    self.piece(slot, q), self.piece(slot, q), cs_sem.at[0],
                    cr_sem.at[(slot - 1) * PIECES_C + q], {"sp": mate},
                ).wait_recv()

        def forward(self, link, s, q):
            if s > 0:
                self.arrive(ring_slot(1 - link, s), q)
            self.copy(link, s, q).start()

        def need(self, slot):
            if slot:
                for q in range(PIECES_C):
                    self.arrive(slot, q)

    own_at = pl.multiple_of(HALO + tp * rows, HALO)
    core = lax.rem(tp, CORES)
    chip = lax.div(tp, CORES)
    partner = chip * CORES + 1 - core
    last_tp = tp == T - 1

    def spread_rows(ref, pieces, near_send, near_recv, far_send, far_recv):
        prow = rows // pieces

        def at_rows(block, q):
            return ref.at[pl.ds(pl.multiple_of(HALO + block * rows + q * prow, HALO), prow)]

        def first(d, q):
            device = partner if d == 0 else lax.rem(chip + d, Y) * CORES + core
            return remote(
                at_rows(tp, q), at_rows(tp, q), near_send, near_recv.at[d, q], {"tp": device}
            )

        def second(d, q, at_core):
            block = lax.rem(chip + Y - d, Y) * CORES + at_core
            return remote(
                at_rows(block, q), at_rows(block, q), far_send, far_recv.at[d, q],
                {"tp": partner},
            )

        def start(q):
            for d in range(1, Y):
                first(d, q).start()
            first(0, q).start()

        def relay(q):
            for d in range(1, Y):
                first(d, q).wait_recv()
                second(d, q, core).start()

        def finish():
            for q in range(pieces):
                first(0, q).wait_recv()
                for d in range(1, Y):
                    second(d, q, 1 - core).wait_recv()

        return at_rows, start, relay, finish

    _, t_start, t_relay, t_finish = spread_rows(norm, PIECES_T, ts_sem, tr_sem, us_sem, ur_sem)
    u_rows, u_start, u_relay, u_finish = spread_rows(
        norm2, PIECES_U, t2s_sem, t2r_sem, u2s_sem, u2r_sem
    )

    def v_copy(q):
        prow = rows // PIECES_U
        src = norm.at[pl.ds(pl.multiple_of(own_at + q * prow, HALO), prow)]
        return remote(src, u_rows(tp, q), vs_sem, vr_sem.at[q], {"sp": mate})

    def k_copy():
        cut = pl.ds(HALO - 8, 8)
        return remote(norm.at[cut], norm2.at[cut], k_sem.at[0], k_sem.at[1], {"sp": mate})

    def l_copy():
        return remote(spikes, spikes2, l_sem.at[0], l_sem.at[1], {"sp": mate})

    def h_copy():
        return remote(
            norm.at[pl.ds(length, HALO)], norm.at[pl.ds(0, HALO)], h_sem.at[0], h_sem.at[1],
            {"sp": lax.rem(sp + 1, n)},
        )

    def g_copy(d):
        cut = pl.ds(0, HALO)
        return remote(norm.at[cut], norm.at[cut], g_sem.at[0], g_sem.at[1], {"tp": d})

    def halo_relay():
        @pl.when(last_tp & (sp > 0))
        def _():
            h_copy().wait_recv()
            for d in range(T - 1):
                g_copy(d).start()

    def halo_ready():
        @pl.when((tp < T - 1) & (sp > 0))
        def _():
            g_copy(0).wait_recv()

        @pl.when(sp == 0)
        def _():
            norm[0:HALO, :] = jnp.zeros((HALO, width), bf16)

    def project(acc, source, buf, slots, owner, fresh=False):
        for c in range(0, acc.shape[1], 256):
            total = None
            for slot in slots:
                at = pl.multiple_of(owner(slot) * kdim, kdim)
                term = jnp.dot(
                    source[:, pl.ds(at, kdim)], buf[slot, :, c : c + 256],
                    preferred_element_type=f32,
                )
                total = term if total is None else total + term
            if fresh:
                acc[:, c : c + 256] = total
            else:
                acc[:, c : c + 256] += total

    def column(ref):
        index = lax.broadcasted_iota(jnp.int32, (heads, 1), 0)
        full = jnp.full((heads, 1), ref[0], f32)
        for h in range(1, heads):
            full = jnp.where(index == h, ref[h], full)
        return full

    lane = lax.broadcasted_iota(jnp.int32, (1, heads_width), 1)

    def spread(columns):
        full = jnp.broadcast_to(columns[:, 0:1], (columns.shape[0], heads_width))
        for h in range(1, heads):
            full = jnp.where(lane >= h * HEAD_DIM, columns[:, h : h + 1], full)
        return full

    def taps(u, weights):
        k_taps = weights.shape[0]
        w = weights[...].astype(f32)
        total = w[k_taps - 1 : k_taps] * u[8:]
        for k in range(k_taps - 1):
            total = total + w[k : k + 1] * pltpu.roll(u, k_taps - 1 - k, 0)[8:]
        return total

    blocks = length // CHUNK

    def spans(b):
        t0 = b * CHUNK
        return (
            slice(t0, t0 + CHUNK),
            slice(t0 + HALO, t0 + HALO + CHUNK),
            slice(t0 + HALO - 8, t0 + HALO + CHUNK),
        )

    def field(acc, begin, size, span):
        return acc[span, begin : begin + size].astype(bf16).astype(f32)

    def conv_step(ring, s):
        slots = (0,) if s == 0 else (n - 1,) if s == n // 2 else (ring_slot(0, s), ring_slot(1, s))
        for slot in slots:
            ring.need(slot)
        project(acc_c, norm, cbuf, slots, ring_owner, s == 0)

    half_rows = length // Y
    half_blocks = half_rows // CHUNK

    def conv_mix(y):
        for b in range(half_blocks):
            t0 = y * half_rows + b * CHUNK
            span = pl.ds(pl.multiple_of(t0, CHUNK), CHUNK)
            own = pl.ds(pl.multiple_of(t0 + HALO, HALO), CHUNK)
            take = pl.ds(pl.multiple_of(t0 + HALO - 8, 8), CHUNK + 8)
            product = field(acc_c, cdim, cdim, take) * field(acc_c, 2 * cdim, cdim, take)
            mix = field(acc_c, 0, cdim, own) * taps(product, taps_conv)
            apart[span, 0:cdim] = mix.astype(bf16)

    def turned(b):
        return lax.rem(b + (1 - chip) * half_blocks, blocks)

    def m_copy(b):
        cut = pl.ds(pl.multiple_of(turned(b) * CHUNK, CHUNK), CHUNK)
        return remote(
            mbuf.at[cut], apart.at[cut, pl.ds(cdim, heads_width)], ms_sem, mr_sem.at[b],
            {"sp": mate},
        )

    def x_copy():
        return remote(st_send, st_recv, x_sem.at[0], x_sem.at[1], {"sp": side})

    def e_copy():
        return remote(e_send, e_recv, e_sem.at[0], e_sem.at[1], {"sp": cross})

    def inner_part():
        sl = Slots(sbuf, PIECES_S, sr_sem)
        gl = Slots(gbuf, PIECES_G, gr_sem)
        ol = Slots(obuf, PIECES_O, or_sem)
        ring = Ring()
        forwards = [(link, 1, q) for link in (0, 1) for q in range(PIECES_C)]
        step_two = sorted((q + 2.5 * link, link, q) for link in (0, 1) for q in range(PIECES_C))
        forwards += [(link, 2, q) for _, link, q in step_two]
        for q in range(PIECES_C // 2):
            if q < FAR_PIECES:
                forwards += [(1, 3, PIECES_C - FAR_PIECES + q)]
        done = [0]

        def pump(count):
            for _ in range(count):
                if done[0] < len(forwards):
                    ring.forward(*forwards[done[0]])
                    done[0] += 1

        r_id = lax.broadcasted_iota(jnp.int32, (CHUNK, CHUNK), 0)
        c_id = lax.broadcasted_iota(jnp.int32, (CHUNK, CHUNK), 1)
        causal = r_id >= c_id
        lower = causal.astype(f32)
        eye = (r_id == c_id).astype(f32)

        for q in range(PIECES_C):
            ring.forward(0, 0, q)
        for q in range(PIECES_S):
            sl.arrive(1, q, ss_sem, mate)
            sl.send(1, 3, q, ss_sem, cross)
            sl.send(1, 5, q, ss_sem, side)
        for q in range(PIECES_S):
            sl.arrive(2, q, ss_sem, mate)
            sl.send(2, 6, q, ss_sem, side)
        for q in range(PIECES_C):
            ring.forward(1, 0, q)
        t_relay(0)
        landed("g")
        for q in range(PIECES_G):
            gl.send(0, 2, q, gs_sem, cross)
        landed("o")
        for q in range(PIECES_O):
            ol.send(0, 2, q, os_sem, cross)
            ol.send(0, 1, q, os_sem, mate)
        for q in range(PIECES_S):
            sl.arrive(3, q, ss_sem, mate)
            sl.send(3, 7, q, ss_sem, side)
        for q in range(PIECES_G):
            gl.send(0, 4, q, gs_sem, side)
        halo_relay()
        for q in range(PIECES_U):
            v_copy(q).wait_recv()
            u_start(q)
            if q == 0:
                for p in range(1, PIECES_T):
                    t_relay(p)
            if q > 0:
                pump(1)
                u_relay(q - 1)
        pump(1)
        t_finish()
        halo_ready()
        for q in range(PIECES_G):
            gl.arrive(1, q, gs_sem, mate)
            gl.send(1, 3, q, gs_sem, cross)
            gl.send(1, 5, q, gs_sem, side)
        u_relay(PIECES_U - 1)
        for slot in range(1, n):
            for q in range(PIECES_S):
                sl.arrive(slot, q, ss_sem, mate)
        project(acc_s.at[0], norm, sbuf, range(0, 4), plane_owner, True)
        project(acc_s.at[0], norm, sbuf, range(4, 8), plane_owner)
        for q in range(PIECES_G):
            gl.arrive(2, q, gs_sem, mate)
            gl.send(2, 6, q, gs_sem, side)
        k_copy().wait_recv()
        u_finish()
        project(acc_s.at[1], norm2, sbuf, range(0, 4), plane_owner, True)
        project(acc_s.at[1], norm2, sbuf, range(4, 8), plane_owner)
        pump(2)
        landed("v")
        l_copy().wait_recv()

        logs_of = []
        for k, (source, spike) in enumerate(((norm, spikes), (norm2, spikes2))):
            step = jax.nn.softplus(nt(step_w[...], source[HALO:, :]) + column(bias))
            logs = -step * jnp.exp(column(rate)) + spike[...]
            logs_of.append(logs)
            running = jnp.zeros((STATE, heads_width), f32)
            before = jnp.zeros((1, heads_width), f32)
            acc = acc_s.at[k]
            for b in range(blocks):
                span, own, take = spans(b)
                xs = silu(taps(field(acc, 0, cdim, take), taps_in))
                wr = silu(taps(field(acc, cdim, STATE, take), taps_wr))
                rd = silu(taps(field(acc, cdim + STATE, STATE, take), taps_rd))
                cum = nt(lower, logs[:, span], highest)
                steps = nt(eye, step[:, span], highest)
                cum_wide = spread(cum)
                weighted = xs * spread(steps)
                xbuf[k, span, :] = xs
                mixbuf[k, span, :] = weighted.astype(bf16)
                wrbuf[k, span, :] = wr.astype(bf16)
                rdbuf[k, span, :] = rd.astype(bf16)
                cumbuf[k, span, :] = cum_wide
                last = cum_wide[CHUNK - 1 : CHUNK]
                scaled = (weighted * jnp.exp(last - cum_wide)).astype(bf16)
                stbuf[k, b] = running
                running = running * jnp.exp(last) + jnp.dot(
                    wr.T.astype(bf16), scaled, preferred_element_type=f32
                )
                before = before + last
                if k == 0 and b % 2 == 1:
                    pump(1)
            runbuf[k] = running
            decbuf[k] = jnp.exp(before)
            st_send[k, 0:STATE, :] = running.astype(bf16)
            st_send[k, STATE:, :] = jnp.broadcast_to(
                jnp.exp(before), (HALO, heads_width)
            ).astype(bf16)
            if k == 0:
                for q in range(PIECES_O):
                    ol.arrive(2, q, os_sem, mate)
                    ol.send(2, 2, q, os_sem, mate)

        x_copy().start()
        for q in range(PIECES_G):
            gl.arrive(3, q, gs_sem, mate)
            gl.send(3, 7, q, gs_sem, side)

        def within(k, b):
            span, _, _ = spans(b)
            scores = nt(rdbuf[k, span, :], wrbuf[k, span, :])
            cum_t = lax.dot_general(
                logs_of[k][:, span], lower, (((1,), (1,)), ((), ())),
                preferred_element_type=f32, precision=highest,
            )
            for pair in range(0, heads_width, 128):
                both = []
                for h in range(pair // HEAD_DIM, (pair + 128) // HEAD_DIM):
                    diff = cumbuf[k, span, h * HEAD_DIM : h * HEAD_DIM + 1] - cum_t[h : h + 1, :]
                    damped = scores * jnp.exp(jnp.where(causal, diff, -1e30))
                    both.append(
                        jnp.dot(
                            damped.astype(bf16), mixbuf[k, span, pair : pair + 128],
                            preferred_element_type=f32,
                        )
                    )
                first = lax.broadcasted_iota(jnp.int32, (1, 128), 1) < HEAD_DIM
                ybuf[k, span, pair : pair + 128] = jnp.where(first, both[0], both[1])

        for b in range(blocks):
            within(1, b)
        pump(1)
        for slot in (0, 2):
            for q in range(PIECES_O):
                ol.send(slot, 4 + slot, q, ox_sem, side)
        for b in range(blocks):
            within(0, b)
        for q in range(PIECES_O):
            ol.arrive(1, q, os_sem, mate)
            ol.send(1, 3, q, os_sem, cross)
            ol.send(1, 5, q, ox_sem, side)
        pump(1)
        x_copy().wait_recv()
        second = jnp.broadcast_to(x, (1, heads_width)) == 1
        pair, pair_decay, other, first_decay = [], [], [], []
        for k in range(2):
            theirs = st_recv[k, 0:STATE, :].astype(f32)
            their_decay = st_recv[k, STATE : STATE + 1, :].astype(f32)
            pair.append(
                jnp.where(
                    second, theirs * decbuf[k] + runbuf[k], runbuf[k] * their_decay + theirs
                )
            )
            pair_decay.append(decbuf[k] * their_decay)
            other.append(jnp.where(second, theirs, jnp.zeros_like(theirs)))
            first_decay.append(jnp.where(second, their_decay, jnp.ones_like(their_decay)))

        @pl.when(upper == 0)
        def _():
            e_send[...] = (pair[1] * pair_decay[0] + pair[0]).astype(bf16)
            e_copy().start()
            runbuf[1] = other[1]
            runbuf[0] = other[0] + first_decay[0] * pair[1]

        @pl.when(upper == 1)
        def _():
            runbuf[0] = other[0]
            runbuf[1] = other[1] + first_decay[1] * pair[0]
            decbuf[0] = first_decay[0]
            decbuf[1] = first_decay[1] * pair_decay[0]

        pump(2)
        pump(1)
        for slot in range(1, n - 1):
            for q in range(PIECES_G):
                gl.arrive(slot, q, gs_sem, mate)
        for k, source in enumerate((norm, norm2)):
            project(acc_g.at[k], source, gbuf, range(n - 1), plane_owner, True)
            pump(1)
        conv_step(ring, 0)
        pump(1)
        for q in range(PIECES_G):
            gl.arrive(n - 1, q, gs_sem, mate)
        for k, source in enumerate((norm, norm2)):
            project(acc_g.at[k], source, gbuf, (n - 1,), plane_owner)

        @pl.when(upper == 1)
        def _():
            e_copy().wait_recv()
            entering = e_recv[...].astype(f32)
            for k in range(2):
                runbuf[k] = runbuf[k] + decbuf[k] * entering

        group = (
            lax.div(lax.broadcasted_iota(jnp.int32, (heads_width, heads_width), 0), HEAD_DIM)
            == lax.div(lax.broadcasted_iota(jnp.int32, (heads_width, heads_width), 1), HEAD_DIM)
        ).astype(bf16)
        direct_wide = jnp.full((1, heads_width), direct[0], f32)
        for h in range(1, heads):
            direct_wide = jnp.where(lane >= h * HEAD_DIM, direct[h], direct_wide)

        for k in (1, 0):
            so_far = jnp.zeros((1, heads_width), f32)
            for b in range(blocks):
                stbuf[k, b] = stbuf[k, b] + jnp.exp(so_far) * runbuf[k]
                at_end = b * CHUNK + CHUNK - 1
                so_far = so_far + cumbuf[k, at_end : at_end + 1, :]
            for i in range(blocks):
                b = turned(i)
                span = pl.ds(pl.multiple_of(b * CHUNK, CHUNK), CHUNK)
                own = pl.ds(pl.multiple_of(b * CHUNK + HALO, HALO), CHUNK)
                head_out = (
                    ybuf[k, span, :]
                    + jnp.dot(
                        rdbuf[k, span, :], stbuf[k, b].astype(bf16), preferred_element_type=f32
                    )
                    * jnp.exp(cumbuf[k, span, :])
                    + direct_wide * xbuf[k, span, :]
                )
                gated = head_out * silu(field(acc_g.at[k], 0, cdim, own))
                square = jnp.dot((gated * gated).astype(bf16), group, preferred_element_type=f32)
                normalized = gated * lax.rsqrt(square * (1.0 / HEAD_DIM) + epsilon)
                result = (
                    normalized * hscale[...].astype(f32).reshape(1, heads_width)
                ).astype(bf16)
                if k == 1:
                    mbuf[span, :] = result
                    m_copy(i).start()
                    if i == half_blocks - 1:
                        for q in range(PIECES_O):
                            ol.arrive(3, q, os_sem, mate)
                            ol.send(3, 3, q, os_sem, mate)
                            ol.send(3, 7, q, ox_sem, side)
                else:
                    apart[span, cdim:] = result
        pump(1)
        conv_step(ring, 1)
        pump(1)
        conv_step(ring, 2)
        pump(len(forwards))
        conv_step(ring, 3)
        conv_step(ring, n // 2)
        conv_mix(1 - chip)

    def blocks_sent(buf, count, sem):
        every = buf.at[pl.ds(0, count)]
        remote(every, every, sem, cr_sem.at[0], {"sp": mate}).wait_send()

    def end_part():
        gl = Slots(gbuf, PIECES_G, gr_sem)
        ol = Slots(obuf, PIECES_O, or_sem)
        ring = Ring()
        for q in range(PIECES_U):
            v_copy(q).start()
        for q in range(PIECES_C):
            ring.forward(1, 0, q)
        landed("v")
        l_copy().start()
        landed("g")
        for q in range(PIECES_G):
            gl.send(0, 1, q, gs_sem, mate)
        t_relay(0)
        for q in range(PIECES_C):
            ring.forward(1, 1, q)
        for q in range(1, PIECES_T):
            t_relay(q)
        halo_relay()
        halo_ready()
        k_copy().start()
        landed("o")
        for q in range(PIECES_C):
            ring.forward(0, 0, q)
        for q in range(PIECES_O):
            ol.send(0, 1, q, os_sem, mate)
        for q in range(PIECES_O):
            ol.send(0, 4, q, ox_sem, side)
        for q in range(PIECES_C):
            ring.forward(0, 1, q)
        for q in range(PIECES_O):
            ol.arrive(1, q, os_sem, mate)
            ol.send(1, 5, q, ox_sem, side)
        for q in range(PIECES_C):
            ring.forward(0, 2, q)
        t_finish()
        conv_step(ring, 0)
        conv_step(ring, 1)
        for q in range(PIECES_C):
            ring.forward(1, 2, q)
        for q in range(PIECES_C - FAR_PIECES):
            ring.forward(0, 3, q)
        conv_step(ring, 2)
        for q in range(PIECES_O):
            ol.arrive(2, q, os_sem, mate)
            ol.send(2, 6, q, ox_sem, side)
        for q in range(PIECES_C):
            ring.forward(1, 3, q)
        conv_step(ring, 3)
        conv_step(ring, n // 2)
        conv_mix(1 - chip)
        for b in range(half_blocks):
            m_copy(b).wait_recv()

    landed("s")
    pl.semaphore_wait(barrier, n - 1 + T - 1)
    first_s = Slots(sbuf, PIECES_S, sr_sem)

    @pl.when(is_inner)
    def _():
        for q in range(PIECES_S):
            first_s.send(0, 2, q, ss_sem, cross)
            first_s.send(0, 4, q, ss_sem, side)

    @pl.when(is_inner)
    def _():
        norm2[0 : HALO - 8, :] = jnp.zeros((HALO - 8, width), bf16)

    @pl.when(z == end_z)
    def _():
        for q in range(PIECES_S):
            first_s.send(0, 1, q, ss_sem, mate)

    landed("t")
    value = tokens[...].astype(f32)
    value = value * lax.rsqrt(jnp.mean(value * value, axis=1, keepdims=True) + epsilon)
    norm[pl.ds(own_at, rows), :] = (
        value * in_scale[...].astype(f32).reshape(1, width)
    ).astype(bf16)
    for q in range(PIECES_T):
        t_start(q)

    @pl.when(last_tp & (sp < n - 1))
    def _():
        h_copy().start()

    landed("c")

    @pl.when(is_inner)
    def _():
        inner_part()

    @pl.when(z == end_z)
    def _():
        end_part()

    def block_rows(y, c):
        return pl.ds(pl.multiple_of((y * CORES + c) * rows, rows), rows)

    def columns_of(slot):
        return pl.ds(pl.multiple_of(plane_owner(slot) * ocols, ocols), ocols)

    def r1_copy(d, s):
        return remote(
            part.at[s, block_rows(lax.rem(chip + d, Y), 1 - core)], r1.at[s, d], r1s_sem,
            r1r_sem.at[d, s], {"tp": partner},
        )

    def r2_copy(d, s):
        return remote(
            p2.at[d - 1, s], far.at[d - 1, :, columns_of(s)], r2s_sem, r2r_sem,
            {"tp": lax.rem(chip + d, Y) * CORES + core},
        )

    def near_copy(s):
        return pltpu.make_async_copy(nbuf.at[s], near.at[:, columns_of(s)], near_sem)

    o_last = Slots(obuf, PIECES_O, or_sem)

    def project_out(d, s):
        if s >= 4:
            for q in range(PIECES_O):
                o_last.arrive(s, q, os_sem, mate)
        span = pl.ds(pl.multiple_of(lax.rem(chip + d, Y) * half_rows, half_rows), half_rows)
        part[s, span, :] = jnp.dot(
            apart[span, :], obuf[s], preferred_element_type=f32
        ).astype(bf16)
        r1_copy(d, s).start()

    def reduce(d, s):
        r1_copy(d, s).wait_recv()
        mine = part[s, block_rows(lax.rem(chip + d, Y), core), :]
        total = (mine.astype(f32) + r1[s, d].astype(f32)).astype(bf16)
        if d:
            p2[d - 1, s] = total
            r2_copy(d, s).start()
        else:
            nbuf[s] = total
            near_copy(s).start()

    open_sums = []

    def output(d, s, lag=3):
        project_out(d, s)
        open_sums.append((d, s))
        if len(open_sums) > lag:
            reduce(*open_sums.pop(0))

    for s in (0, 1, 2, 4, 6, 5):
        output(1, s, 1)
    conv_mix(chip)

    @pl.when(z == end_z)
    def _():
        ol = Slots(obuf, PIECES_O, or_sem)
        for q in range(PIECES_O):
            ol.arrive(3, q, os_sem, mate)
            ol.send(3, 7, q, ox_sem, side)
        for b in range(half_blocks, blocks):
            m_copy(b).wait_recv()

    while open_sums:
        reduce(*open_sums.pop(0))
    for d, s in ((0, 0), (0, 1), (1, 3), (0, 2), (0, 4), (1, 7), (0, 5), (0, 6), (0, 3), (0, 7)):
        output(d, s, 1 if s == 7 else 2)
    while open_sums:
        reduce(*open_sums.pop(0))

    @pl.when(is_inner)
    def _():
        x_copy().wait_send()

        @pl.when(upper == 0)
        def _():
            e_copy().wait_send()

        last_hop = cbuf.at[pl.ds(0, FAR_PIECES), pl.ds(0, kdim // PIECES_C)]
        remote(last_hop, last_hop, cs_sem.at[1], cr_sem.at[0], {"sp": mate}).wait_send()
        blocks_sent(sbuf, 6, ss_sem)
        blocks_sent(gbuf, 6, gs_sem)
        blocks_sent(obuf, 5, os_sem)
        remote(mbuf, mbuf, ms_sem, mr_sem.at[0], {"sp": mate}).wait_send()
        remote(
            norm2.at[pl.ds(0, Y * rows)], norm2.at[pl.ds(0, Y * rows)], t2s_sem,
            t2r_sem.at[0, 0], {"tp": partner},
        ).wait_send()
        remote(
            norm2.at[pl.ds(0, (Y - 1) * rows)], norm2.at[pl.ds(0, (Y - 1) * rows)], u2s_sem,
            u2r_sem.at[0, 0], {"tp": partner},
        ).wait_send()

    @pl.when(z == end_z)
    def _():
        last_hop = cbuf.at[pl.ds(0, 2 * PIECES_C - FAR_PIECES), pl.ds(0, kdim // PIECES_C)]
        remote(last_hop, last_hop, cs_sem.at[1], cr_sem.at[0], {"sp": mate}).wait_send()
        blocks_sent(sbuf, 1, ss_sem)
        blocks_sent(gbuf, 1, gs_sem)
        blocks_sent(obuf, 1, os_sem)
        remote(
            norm.at[pl.ds(0, rows)], norm.at[pl.ds(0, rows)], vs_sem, vr_sem.at[0], {"sp": mate}
        ).wait_send()
        k_copy().wait_send()
        l_copy().wait_send()

    blocks_sent(cbuf, n - 2, cs_sem.at[0])
    blocks_sent(obuf, 4, ox_sem)
    remote(
        norm.at[pl.ds(0, Y * rows)], norm.at[pl.ds(0, Y * rows)], ts_sem, tr_sem.at[0, 0],
        {"tp": partner},
    ).wait_send()
    remote(
        norm.at[pl.ds(0, (Y - 1) * rows)], norm.at[pl.ds(0, (Y - 1) * rows)], us_sem,
        ur_sem.at[0, 0], {"tp": partner},
    ).wait_send()

    @pl.when(last_tp & (sp < n - 1))
    def _():
        h_copy().wait_send()

    @pl.when(last_tp & (sp > 0))
    def _():
        cut = pl.ds(0, (T - 1) * HALO)
        remote(norm.at[cut], norm.at[cut], g_sem.at[0], g_sem.at[1], {"tp": partner}).wait_send()

    remote(r1, r1, r1s_sem, r1r_sem.at[0, 0], {"tp": partner}).wait_send()
    remote(p2, p2, r2s_sem, r2r_sem, {"tp": partner}).wait_send()
    pltpu.make_async_copy(far.at[0], near, near_sem).wait()
    remote(far, far, r2s_sem, r2r_sem, {"tp": partner}).wait_recv()


def shifted(shard, axis, by):
    devices = lax.axis_size(axis)
    pairs = [(i, i + by) for i in range(devices) if 0 <= i + by < devices]
    return lax.ppermute(shard, axis, pairs)


def prefix(shard, axis, combine, identity):
    devices, index = (lax.axis_size(axis), lax.axis_index(axis))
    everything = jax.tree.map(
        lambda part, kind: lax.all_gather(part.astype(kind), axis),
        shard,
        (jnp.bfloat16, jnp.bfloat16),
    )
    start = jax.tree.map(
        lambda part, zero: jnp.broadcast_to(jnp.asarray(zero, part.dtype), part.shape),
        shard,
        identity,
    )

    def turn(k, before):
        reached = k < index
        new = combine(
            before, jax.tree.map(lambda part, own: part[k].astype(own.dtype), everything, shard)
        )
        return jax.tree.map(lambda a, b: jnp.where(reached, a, b), new, before)

    return lax.fori_loop(0, devices, turn, start)


def causal_taps(values, rim_rows, tap_weights):
    tap_count = tap_weights.shape[0]
    length = values.shape[0]
    padded = jnp.concatenate([rim_rows, values], axis=0)
    running = tap_weights[0] * padded[0:length]
    for offset in range(1, tap_count):
        running = running + tap_weights[offset] * padded[offset : offset + length]
    return running


def combine_states(earlier, later):
    return (earlier[0] * later[0], earlier[1] * later[0][:, None, None] + later[1])


def plain_path(
    tokens,
    input_norm_scale,
    outer_gate_weight,
    inner_gate_weight,
    value_weight_matrix,
    output_gate_weight,
    state_input_weight,
    write_key_weight,
    read_key_weight,
    step_size_weight,
    gated_conv_weight,
    input_conv_weight,
    write_conv_weight,
    read_conv_weight,
    step_size_bias,
    log_decay_rate,
    decay_spikes,
    direct_path_weight,
    head_norm_scale,
    conv_output_weight,
    state_output_weight,
):
    token_rows = tokens.astype(jnp.float32)
    scaled = token_rows * lax.rsqrt(
        jnp.mean(token_rows * token_rows, axis=1, keepdims=True) + epsilon
    )
    normed_own = (scaled * input_norm_scale.astype(jnp.float32)).astype(jnp.bfloat16)
    normed = lax.all_gather(normed_own, "tp", axis=0, tiled=True)
    length = normed.shape[0]
    pieces = (
        lax.all_gather(outer_gate_weight, "sp", axis=0, tiled=True),
        lax.all_gather(inner_gate_weight, "sp", axis=0, tiled=True),
        lax.all_gather(value_weight_matrix, "sp", axis=0, tiled=True),
        lax.all_gather(output_gate_weight, "sp", axis=0, tiled=True),
        lax.all_gather(state_input_weight, "sp", axis=0, tiled=True),
        lax.all_gather(write_key_weight, "sp", axis=0, tiled=True),
        lax.all_gather(read_key_weight, "sp", axis=0, tiled=True),
    )
    projected = tuple(
        (jnp.dot(normed, weight_rows, preferred_element_type=jnp.float32) for weight_rows in pieces)
    )
    outer_gate, inner_gate, conv_input, out_gate, state_input, write_keys, read_keys = [
        member.astype(jnp.bfloat16) for member in projected
    ]
    step_raw = jnp.dot(normed, step_size_weight, preferred_element_type=jnp.float32)
    short_rim = gated_conv_weight.shape[0] - 1
    state_rim = input_conv_weight.shape[0] - 1
    rim_rows = shifted(
        (
            inner_gate[length - short_rim :],
            conv_input[length - short_rim :],
            state_input[length - state_rim :],
            write_keys[length - state_rim :],
            read_keys[length - state_rim :],
        ),
        "sp",
        1,
    )
    product = inner_gate.astype(jnp.float32) * conv_input.astype(jnp.float32)
    rim_product = rim_rows[0].astype(jnp.float32) * rim_rows[1].astype(jnp.float32)
    mixer_part = (
        outer_gate.astype(jnp.float32)
        * causal_taps(product, rim_product, gated_conv_weight.astype(jnp.float32))
    ).astype(jnp.bfloat16)
    seq_input = jax.nn.silu(
        causal_taps(
            state_input.astype(jnp.float32),
            rim_rows[2].astype(jnp.float32),
            input_conv_weight.astype(jnp.float32),
        )
    )
    seq_write = jax.nn.silu(
        causal_taps(
            write_keys.astype(jnp.float32),
            rim_rows[3].astype(jnp.float32),
            write_conv_weight.astype(jnp.float32),
        )
    )
    seq_read = jax.nn.silu(
        causal_taps(
            read_keys.astype(jnp.float32),
            rim_rows[4].astype(jnp.float32),
            read_conv_weight.astype(jnp.float32),
        )
    )
    discrete_step = jax.nn.softplus(step_raw + step_size_bias[None, :])
    step_logarithm = discrete_step * (-jnp.exp(log_decay_rate))[None, :] + decay_spikes.T
    heads_here = discrete_step.shape[1]
    groups_here = seq_write.shape[1] // STATE
    per_group = heads_here // groups_here
    blocks = length // PLAIN_BLOCK
    input_blocks = seq_input.reshape(blocks, PLAIN_BLOCK, heads_here, HEAD_DIM)
    weighted = input_blocks * discrete_step.reshape(blocks, PLAIN_BLOCK, heads_here, 1)
    write_blocks = jnp.repeat(
        seq_write.reshape(blocks, PLAIN_BLOCK, groups_here, STATE), per_group, axis=2
    )
    read_blocks = jnp.repeat(seq_read.reshape(blocks, PLAIN_BLOCK, groups_here, STATE), per_group, axis=2)
    cumulative = jnp.cumsum(step_logarithm.reshape(blocks, PLAIN_BLOCK, heads_here), axis=1)
    causal = lax.broadcasted_iota(jnp.int32, (PLAIN_BLOCK, PLAIN_BLOCK), 0) >= lax.broadcasted_iota(
        jnp.int32, (PLAIN_BLOCK, PLAIN_BLOCK), 1
    )
    scores = jnp.einsum("clhm,cshm->clsh", read_blocks, write_blocks, precision=highest)
    damping = jnp.exp(
        jnp.where(
            causal[None, :, :, None],
            cumulative[:, :, None, :] - cumulative[:, None, :, :],
            -jnp.inf,
        )
    )
    within_block = jnp.einsum("clsh,cshp->clhp", scores * damping, weighted, precision=highest)
    to_end = jnp.exp(cumulative[:, -1:, :] - cumulative)
    block_states = jnp.einsum(
        "cshm,cshp->chpm", write_blocks * to_end[..., None], weighted, precision=highest
    )
    block_logs = cumulative[:, -1, :]

    def advance(carried_state, inputs):
        contribution, block_log = inputs
        return (carried_state * jnp.exp(block_log)[:, None, None] + contribution, carried_state)

    own_total, own_before = lax.scan(
        advance, jnp.zeros(block_states.shape[1:], jnp.float32), (block_states, block_logs)
    )
    total_log = jnp.sum(block_logs, axis=0)
    arriving = prefix(
        (jnp.exp(total_log), own_total),
        "sp",
        combine_states,
        (jnp.ones_like(total_log), jnp.zeros_like(own_total)),
    )[1]
    before_logs = jnp.cumsum(block_logs, axis=0) - block_logs
    entering = own_before + jnp.exp(before_logs)[:, :, None, None] * arriving[None]
    from_before = (
        jnp.einsum("clhm,chpm->clhp", read_blocks, entering, precision=highest)
        * jnp.exp(cumulative)[..., None]
    )
    head_out = within_block + from_before + direct_path_weight[None, None, :, None] * input_blocks
    head_out = head_out.reshape(length, heads_here * HEAD_DIM)
    gated_heads = (head_out * jax.nn.silu(out_gate.astype(jnp.float32))).reshape(
        length, heads_here, HEAD_DIM
    )
    normalized = gated_heads * lax.rsqrt(
        jnp.mean(gated_heads * gated_heads, axis=2, keepdims=True) + epsilon
    )
    state_part = (
        normalized.reshape(length, heads_here * HEAD_DIM) * head_norm_scale.astype(jnp.float32)
    ).astype(jnp.bfloat16)
    wide_mixer, wide_state = (
        lax.all_gather(conv_output_weight, "sp", axis=1, tiled=True),
        lax.all_gather(state_output_weight, "sp", axis=1, tiled=True),
    )
    return lax.psum_scatter(
        (
            jnp.dot(mixer_part, wide_mixer, preferred_element_type=jnp.float32)
            + jnp.dot(state_part, wide_state, preferred_element_type=jnp.float32)
        ).astype(jnp.bfloat16),
        "tp",
        scatter_dimension=0,
        tiled=True,
    )


def per_device(
    tokens, input_norm_scale, outer_gate_weight, inner_gate_weight, value_weight_matrix,
    output_gate_weight, state_input_weight, write_key_weight, read_key_weight, step_size_weight,
    gated_conv_weight, input_conv_weight, write_conv_weight, read_conv_weight, step_size_bias,
    log_decay_rate, decay_spikes, direct_path_weight, head_norm_scale, conv_output_weight,
    state_output_weight,
):
    n, T = lax.axis_size("sp"), lax.axis_size("tp")
    rows, width = tokens.shape
    kdim, cdim = outer_gate_weight.shape
    heads = step_size_bias.shape[0]
    hw = heads * HEAD_DIM
    length = rows * T
    ocols = conv_output_weight.shape[1]
    if (
        kdim % 128 or ocols % 256 or n % 2 or n != 2 * PLANES or T % CORES
        or T != 2 * CORES
        or write_key_weight.shape[1] != STATE
    ):
        return plain_path(
            tokens, input_norm_scale, outer_gate_weight, inner_gate_weight,
            value_weight_matrix, output_gate_weight, state_input_weight, write_key_weight,
            read_key_weight, step_size_weight, gated_conv_weight, input_conv_weight,
            write_conv_weight, read_conv_weight, step_size_bias, log_decay_rate, decay_spikes,
            direct_path_weight, head_norm_scale, conv_output_weight, state_output_weight,
        )
    Y = T // CORES
    hbm = pl.BlockSpec(memory_space=pl.ANY)
    dma = pltpu.SemaphoreType.DMA
    s_cols, blocks = cdim + 2 * STATE, length // CHUNK

    def like(array):
        return pltpu.VMEM(array.shape, array.dtype)

    step_t = step_size_weight.T
    near, far = pl.pallas_call(
        functools.partial(kernel, n, T),
        out_shape=(
            jax.ShapeDtypeStruct((rows, width), bf16),
            jax.ShapeDtypeStruct((Y - 1, rows, width), bf16),
        ),
        in_specs=[hbm] * 21,
        out_specs=(hbm, hbm),
        scratch_shapes=[
            like(tokens),
            like(input_norm_scale),
            like(step_t),
            like(gated_conv_weight),
            like(input_conv_weight),
            like(write_conv_weight),
            like(read_conv_weight),
            like(decay_spikes),
            like(head_norm_scale),
            pltpu.SMEM((heads,), f32),
            pltpu.SMEM((heads,), f32),
            pltpu.SMEM((heads,), f32),
            pltpu.VMEM((n, kdim, s_cols), bf16),
            pltpu.VMEM((n, kdim, cdim), bf16),
            pltpu.VMEM((n, kdim, 3 * cdim), bf16),
            pltpu.VMEM((n, cdim + hw, ocols), bf16),
            pltpu.VMEM((HALO + length, width), bf16),
            pltpu.VMEM((HALO + length, width), bf16),
            like(decay_spikes),
            pltpu.VMEM((2, HALO + length, s_cols), f32),
            pltpu.VMEM((2, HALO + length, cdim), f32),
            pltpu.VMEM((HALO + length, 3 * cdim), f32),
            pltpu.VMEM((2, length, hw), bf16),
            pltpu.VMEM((2, length, hw), f32),
            pltpu.VMEM((2, length, STATE), bf16),
            pltpu.VMEM((2, length, STATE), bf16),
            pltpu.VMEM((2, length, hw), f32),
            pltpu.VMEM((2, length, hw), f32),
            pltpu.VMEM((2, blocks, STATE, hw), f32),
            pltpu.VMEM((2, STATE, hw), f32),
            pltpu.VMEM((2, 1, hw), f32),
            pltpu.VMEM((2, STATE + HALO, hw), bf16),
            pltpu.VMEM((2, STATE + HALO, hw), bf16),
            pltpu.VMEM((STATE, hw), bf16),
            pltpu.VMEM((STATE, hw), bf16),
            pltpu.VMEM((length, hw), bf16),
            pltpu.VMEM((length, cdim + hw), bf16),
            pltpu.VMEM((n, length, ocols), bf16),
            pltpu.VMEM((n, Y, rows, ocols), bf16),
            pltpu.VMEM((Y - 1, n, rows, ocols), bf16),
            pltpu.VMEM((n, rows, ocols), bf16),
            dma((16,)),
            dma,
            dma(((n - 1) * PIECES_S,)),
            dma,
            dma(((n - 1) * PIECES_G,)),
            dma((2,)),
            dma(((n - 1) * PIECES_C,)),
            dma,
            dma,
            dma(((n - 1) * PIECES_O,)),
            dma,
            dma((Y, PIECES_T)),
            dma,
            dma((Y, PIECES_T)),
            dma,
            dma((PIECES_U,)),
            dma,
            dma((Y, PIECES_U)),
            dma,
            dma((Y, PIECES_U)),
            dma((2,)),
            dma((2,)),
            dma((2,)),
            dma((2,)),
            dma((2,)),
            dma((2,)),
            dma,
            dma((blocks,)),
            dma,
            dma((Y, n)),
            dma,
            dma,
            dma,
        ],
        compiler_params=pltpu.CompilerParams(
            collective_id=0, has_side_effects=True, vmem_limit_bytes=62 * 1024 * 1024
        ),
    )(
        tokens, input_norm_scale, outer_gate_weight, inner_gate_weight,
        value_weight_matrix, output_gate_weight, state_input_weight, write_key_weight,
        read_key_weight, step_t, gated_conv_weight, input_conv_weight, write_conv_weight,
        read_conv_weight, step_size_bias, log_decay_rate, decay_spikes, direct_path_weight,
        head_norm_scale,
        conv_output_weight, state_output_weight,
    )
    total = near.astype(f32)
    for d in range(Y - 1):
        total = total + far[d].astype(f32)
    return total.astype(bf16)


def solution(mesh):
    placed = (
        (P(("sp", "tp"), None), P())
        + (P("sp", "tp"),) * 7
        + (P(None, "tp"),) * 5
        + (P("tp"), P("tp"), P("tp", "sp"), P("tp"), P("tp"), P("tp", "sp"), P("tp", "sp"))
    )
    return jax.shard_map(
        per_device, mesh=mesh, in_specs=placed, out_specs=P(("sp", "tp"), None), check_vma=False
    )
```
